512 devices in a mesh: sp: 256 (over z, y, x), tp: 2 (over core).
Axes of the slice: x: 4, y: 4, z: 16, core: 2. Of those that a mesh axis runs over, the one named last changes fastest.
Arguments:
- query_rows: bfloat16 [65536, 1024], P('sp', 'tp'), may hold values from -6 to 6
- key_rows: bfloat16 [65536, 1024], P('sp', 'tp'), may hold values from -6 to 6
- value_rows: bfloat16 [65536, 1024], P('sp', 'tp'), may hold values from -6 to 6
- out_weight: bfloat16 [1024, 2048], P('tp'), may hold values from -0.75 to 0.75
Outputs:
- layer_out: bfloat16 [65536, 2048], P(('sp', 'tp'))
The draws below stay inside these ranges and needn't reach their ends.
All inputs are finite; a program needn't handle non-finite values.
Results may differ from the reference program's by a relative error of at most 0.012.
Values may be sent and summed in bfloat16 or wider, within the bound.
No kernel may reach another device: no remote copies, remote signals or barrier semaphores. Data moves between devices by JAX's collectives and lax.ppermute only.
A program may use at most 64 MiB of HBM per device.

```python
import math
import jax
import jax.numpy as jnp
from jax import lax

D = 2048
H = 16
HD = 64
BACK = 128
SEQ = 65536


def planted_pair(key):
    base = jax.random.fold_in(key, 11)
    width = H * HD
    first = jnp.clip(jax.random.normal(jax.random.fold_in(base, 1), (SEQ, width), jnp.float32), -6.0, 6.0)
    second = jnp.clip(jax.random.normal(jax.random.fold_in(base, 2), (SEQ, width), jnp.float32), -6.0, 6.0)
    return (first, second)


def draw_query_rows(key, part):
    return planted_pair(key)[0].astype(jnp.bfloat16)


def draw_key_rows(key, part):
    return planted_pair(key)[1].astype(jnp.bfloat16)


def shard_levels(rng, dims, shards, smallest, high):
    factor_of, own = 1.0, jax.random.fold_in(rng, 6)
    for position, blocks in shards:
        heights = jnp.exp(jax.random.uniform(jax.random.fold_in(own, position), (blocks,), jnp.float32, smallest / len(shards), high / len(shards)))
        factor_of = factor_of * jnp.repeat(heights, dims[position] // blocks).reshape([-1 if axis == position else 1 for axis in range(len(dims))])
    return factor_of


def noise(rng, dims, scale, reach, pieces=(), kind=jnp.bfloat16):
    values = jax.random.normal(rng, dims, jnp.float32) * scale
    if len(pieces) > 0:
        values = shard_levels(rng, dims, pieces, -0.22, 0.18) * values
    return jnp.clip(values, min=-reach, max=reach).astype(kind)


def setup_inputs(seed: int = 0) -> dict:
    seeds = jax.random.split(jax.random.key(seed), 5)
    query_rows = draw_query_rows(jax.random.fold_in(seeds[4], 71), 0)
    key_rows = draw_key_rows(jax.random.fold_in(seeds[4], 71), 0)
    value_rows = noise(seeds[2], (SEQ, H * HD), 1.0, 6.0, ((0, 256), (1, 2)))
    out_weight = noise(seeds[3], (H * HD, D), HD ** -0.5, 0.75, ((0, 2),))
    return {"query_rows": query_rows, "key_rows": key_rows, "value_rows": value_rows, "out_weight": out_weight}


THETA = 500000.0
DILATIONS = (1, 4, 16)

def rotate(rows, positions, head_count, head_dim):
    half_dim = head_dim // 2
    inverse = jnp.power(jnp.float32(THETA), -jnp.arange(half_dim, dtype=jnp.float32) / half_dim)
    angles = positions.astype(jnp.float32)[:, None] * inverse[None, :]
    cosine = jnp.cos(angles)[:, None, :]
    sine = jnp.sin(angles)[:, None, :]
    whole = rows.astype(jnp.float32).reshape(rows.shape[0], head_count, head_dim)
    lower = whole[..., :half_dim]
    upper = whole[..., half_dim:]
    turned = jnp.concatenate([lower * cosine - upper * sine, upper * cosine + lower * sine], axis=-1)
    return turned.reshape(rows.shape[0], head_count * head_dim).astype(jnp.bfloat16)

def one_pattern(queries, key_seq, value_seq, dilation):
    head_dim = queries.shape[1]
    length = queries.shape[0] // dilation
    blocks = -(-length // BACK)
    padded = blocks * BACK

    def residue(rows):
        return rows.reshape(length, dilation, head_dim).transpose(1, 0, 2)
    query_sub = jnp.pad(residue(queries), ((0, 0), (0, padded - length), (0, 0)))
    query_sub = query_sub.reshape(dilation, blocks, BACK, head_dim)

    def with_prior(rows):
        extended = jnp.pad(residue(rows), ((0, 0), (BACK, padded - length), (0, 0)))
        prior = extended[:, :padded].reshape(dilation, blocks, BACK, head_dim)
        current = extended[:, BACK:].reshape(dilation, blocks, BACK, head_dim)
        return jnp.concatenate([prior, current], axis=2)
    key_sub = with_prior(key_seq)
    value_sub = with_prior(value_seq)
    scores = jnp.einsum('rnqc,rnkc->rnqk', query_sub.astype(jnp.float32), key_sub.astype(jnp.float32))
    scores = scores * (1.0 / math.sqrt(head_dim))
    query_index = jnp.arange(BACK)[:, None]
    key_index = jnp.arange(2 * BACK)[None, :]
    distance = query_index + BACK - key_index
    key_place = jnp.arange(blocks)[:, None, None] * BACK + key_index[None] - BACK
    allowed = (distance >= 0) & (distance <= BACK) & (key_place >= 0)
    scores = jnp.where(allowed[None], scores, -jnp.inf)
    row_max = lax.optimization_barrier(jnp.max(scores, axis=-1))
    weights = jnp.exp(scores - row_max[..., None])
    row_sum = lax.optimization_barrier(jnp.sum(weights, axis=-1))
    rounded = weights.astype(jnp.bfloat16)
    weighted = jnp.einsum('rnqk,rnkc->rnqc', rounded.astype(jnp.float32), value_sub.astype(jnp.float32))
    result = (weighted / row_sum[..., None]).astype(jnp.bfloat16)
    result = result.reshape(dilation, padded, head_dim)[:, :length].transpose(1, 0, 2)
    result = result.reshape(length * dilation, head_dim)
    row_max = row_max.reshape(dilation, padded)[:, :length].transpose(1, 0).reshape(-1)
    row_sum = row_sum.reshape(dilation, padded)[:, :length].transpose(1, 0).reshape(-1)
    return (result, row_max, row_sum)

def reference(query_rows, key_rows, value_rows, out_weight):
    positions = jnp.arange(SEQ, dtype=jnp.int32)
    turned_q = rotate(query_rows, positions, H, HD)
    turned_k = rotate(key_rows, positions, H, HD)

    def split(rows):
        return rows.reshape(SEQ, H, HD).transpose(1, 0, 2)

    def per_head(stacked):
        query_head, key_head, value_head = stacked
        results, maxima, sums = ([], [], [])
        for dilation in DILATIONS:
            result, row_max, row_sum = one_pattern(query_head, key_head, value_head, dilation)
            results.append(result)
            maxima.append(row_max)
            sums.append(row_sum)
        return (tuple(results), tuple(maxima), tuple(sums))
    results, maxima, sums = lax.map(per_head, (split(turned_q), split(turned_k), split(value_rows)))
    top = jnp.maximum(jnp.maximum(maxima[0], maxima[1]), maxima[2])
    scales = [sums[i] * jnp.exp(maxima[i] - top) for i in range(3)]
    weighted = scales[0][..., None] * results[0].astype(jnp.float32)
    weighted = weighted + scales[1][..., None] * results[1].astype(jnp.float32)
    weighted = weighted + scales[2][..., None] * results[2].astype(jnp.float32)
    denominator = scales[0] + scales[1] + scales[2]
    mixed = weighted / denominator[..., None]
    mixed = mixed.transpose(1, 0, 2).reshape(SEQ, H * HD).astype(jnp.bfloat16)
    return jnp.dot(mixed, out_weight, preferred_element_type=jnp.float32).astype(jnp.bfloat16)
```

```python
import functools
import math

import jax
import jax.numpy as jnp
import numpy as np
from jax import lax
from jax.experimental import pallas as pl
from jax.experimental.pallas import tpu as pltpu
from jax.sharding import Mesh, PartitionSpec as P

HD = 64
BACK = 128
THETA = 500000.0
TOK = 256
GROUP = 8
SP = ("z", "g", "b", "x")
NEG = -1e30
BF = jnp.bfloat16
F32 = jnp.float32


def row_tokens():
    p = np.arange(TOK)
    residue4, a, n = p // 64, (p % 64) // 16, p % 16
    return 16 * n + residue4 + 4 * a


def make_tables(blocks):
    t = row_tokens()
    inverse = np.float64(THETA) ** (-np.arange(32, dtype=np.float64) / 32)
    lanes = inverse[np.arange(128) % 32]
    sign = np.where(np.arange(128) % 64 < 32, -1.0, 1.0)
    inner = t[:, None] * lanes[None, :]
    anchor = (np.arange(blocks) * TOK)[:, None] * lanes[None, :]
    cos_a, sin_a = np.cos(anchor), np.sin(anchor)
    zero = np.zeros_like(cos_a)
    anchors = np.stack([cos_a, sin_a, cos_a * sign, sin_a * sign, zero, zero, zero, zero], axis=1)
    perm = np.zeros((TOK, TOK), np.float32)
    perm[np.arange(TOK), t] = 1.0

    def band(query, key):
        distance = query[:, None] - key[None, :]
        return np.where((distance >= 0) & (distance <= BACK), 0.0, NEG).astype(np.float32)

    mask1 = band(t, np.concatenate([t - TOK, t]))
    row = np.arange(64)
    sub = 4 * (row % 16) + row // 16
    query4 = np.concatenate([sub, sub + 64])
    mask4 = band(query4, np.concatenate([query4 - 128, query4]))
    query16 = np.arange(128)
    mask16 = band(query16, np.concatenate([query16 - 128, query16]))
    return dict(
        cos=np.cos(inner).astype(np.float32),
        sin=np.sin(inner).astype(np.float32),
        anchors=anchors.astype(np.float32),
        perm=perm,
        mask1=mask1,
        mask4=mask4,
        mask16=mask16,
    )


def dot(a, b):
    return lax.dot_general(a, b, (((1,), (0,)), ((), ())), preferred_element_type=F32)


def dot_t(a, b):
    return lax.dot_general(a, b, (((1,), (1,)), ((), ())), preferred_element_type=F32)


def half(rows):
    return lax.broadcasted_iota(jnp.int32, (rows, 128), 1) < 64


def pack_kernel(index_ref, q_ref, k_ref, v_ref, perm_ref, cos_ref, sin_ref, anchor_ref, out_ref):
    cos_a, sin_a = anchor_ref[0, 0:1], anchor_ref[0, 1:2]
    cos_s, sin_s = anchor_ref[0, 2:3], anchor_ref[0, 3:4]
    cosine = cos_a * cos_ref[...] - sin_a * sin_ref[...]
    sine = sin_s * cos_ref[...] + cos_s * sin_ref[...]
    lane = lax.broadcasted_iota(jnp.int32, (TOK, 128), 1)
    low64 = lane < 64
    low32 = (lane & 63) < 32

    def turn(rows):
        other = jnp.where(low32, pltpu.roll(rows, 96, 1), pltpu.roll(rows, 32, 1))
        return rows * cosine + other * sine

    perm = perm_ref[...]
    for j in range(4):
        cols = slice(128 * j, 128 * j + 128)
        query = turn(dot(perm, q_ref[:, cols])) * (1.0 / math.sqrt(HD))
        key = turn(dot(perm, k_ref[:, cols]))
        value = dot(perm, v_ref[:, cols])
        out_ref[2 * j, 0:TOK] = jnp.where(low64, key, pltpu.roll(value, 64, 1)).astype(BF)
        out_ref[2 * j + 1, 0:TOK] = jnp.where(low64, pltpu.roll(key, 64, 1), value).astype(BF)
        first, second = query[:128], query[128:]
        out_ref[2 * j, TOK : TOK + 128] = jnp.where(low64[:128], first, pltpu.roll(second, 64, 1)).astype(BF)
        out_ref[2 * j + 1, TOK : TOK + 128] = jnp.where(low64[:128], pltpu.roll(first, 64, 1), second).astype(BF)


def attend_kernel(
    index_ref, own_ref, halo_ref, perm_ref, mask1_ref, mask4_ref, mask16_ref, out_ref, qs, vown, vhalo, acc, top
):
    bias = jnp.where(index_ref[0] < GROUP, NEG, 0.0).astype(F32)
    low = half(128)
    low_bf = jnp.where(low, 1.0, 0.0).astype(BF)
    high_bf = jnp.where(low, 0.0, 1.0).astype(BF)
    low256 = jnp.concatenate([low_bf, low_bf], axis=0)
    high256 = jnp.concatenate([high_bf, high_bf], axis=0)
    for i in range(GROUP):
        packed = own_ref[i, TOK : TOK + 128]
        qs[i, 0:128] = packed * low_bf
        qs[i, 128:256] = pltpu.roll(packed.astype(F32), 64, 1).astype(BF) * low_bf
        vown[i] = own_ref[i, 0:TOK] * high256 + low256
        vhalo[i] = halo_ref[i] * high256 + low256

    def wide(x, n):
        return jnp.concatenate([x] * n, axis=1) if n > 1 else x

    lead16 = mask16_ref[:, 0:128] + bias
    mask16 = jnp.concatenate([lead16, mask16_ref[:, 128:256]], axis=1)
    for r in range(16):
        rows = slice(16 * r, 16 * r + 16)
        query = qs[:, rows].reshape(128, 128)
        keys = jnp.concatenate([halo_ref[:, rows].reshape(128, 128), own_ref[:, rows].reshape(128, 128)], axis=0)
        values = jnp.concatenate([vhalo[:, rows].reshape(128, 128), vown[:, rows].reshape(128, 128)], axis=0)
        scores = dot_t(query, keys) + mask16
        peak = jnp.broadcast_to(jnp.max(scores, axis=1, keepdims=True), (128, 128))
        probs = jnp.exp(scores - wide(peak, 2)).astype(BF)
        acc[:, rows] = dot(probs, values).reshape(8, 16, 128)
        top[:, rows] = peak.reshape(8, 16, 128)

    lead4 = jnp.concatenate([mask4_ref[:, 0:128] + bias, mask4_ref[:, 128:256]], axis=1)
    for b in range(4):
        for r in range(4):
            rows = slice(64 * r, 64 * r + 64)
            at = slice(2 * b, 2 * b + 2)
            query = qs[at, rows].reshape(128, 128)
            if b == 0:
                keys = jnp.concatenate([halo_ref[6:8, rows].reshape(128, 128), own_ref[at, rows].reshape(128, 128)], axis=0)
                values = jnp.concatenate([vhalo[6:8, rows].reshape(128, 128), vown[at, rows].reshape(128, 128)], axis=0)
                mask = lead4
            else:
                keys = own_ref[2 * b - 2 : 2 * b + 2, rows].reshape(256, 128)
                values = vown[2 * b - 2 : 2 * b + 2, rows].reshape(256, 128)
                mask = mask4_ref[...]
            scores = dot_t(query, keys) + mask
            before = top[at, rows].reshape(128, 128)
            peak = jnp.maximum(before, jnp.max(scores, axis=1, keepdims=True))
            probs = jnp.exp(scores - wide(peak, 2)).astype(BF)
            total = acc[at, rows].reshape(128, 128) * jnp.exp(before - peak) + dot(probs, values)
            acc[at, rows] = total.reshape(2, 64, 128)
            top[at, rows] = peak.reshape(2, 64, 128)

    lead1 = jnp.concatenate([mask1_ref[:, 0:256] + bias, mask1_ref[:, 256:512]], axis=1)
    low_rows = half(64)
    for i in range(GROUP):
        if i == 0:
            keys = jnp.concatenate([halo_ref[7], own_ref[0, 0:TOK]], axis=0)
            values = jnp.concatenate([vhalo[7], vown[0]], axis=0)
            mask = lead1
        else:
            keys = jnp.concatenate([own_ref[i - 1, 0:TOK], own_ref[i, 0:TOK]], axis=0)
            values = vown[i - 1 : i + 1].reshape(512, 128)
            mask = mask1_ref[...]
        scores = dot_t(qs[i], keys) + mask
        before = top[i]
        peak = jnp.maximum(before, jnp.max(scores, axis=1, keepdims=True))
        probs = jnp.exp(scores - wide(peak, 4)).astype(BF)
        total = acc[i] * jnp.exp(before - peak) + dot(probs, values)
        mixed = (total / pltpu.roll(total, 64, 1)).astype(BF) * high256
        natural = dot(perm_ref[...], mixed)
        out_ref[2 * i] = jnp.where(low_rows, pltpu.roll(natural[0:64], 64, 1), natural[64:128]).astype(BF)
        out_ref[2 * i + 1] = jnp.where(low_rows, pltpu.roll(natural[128:192], 64, 1), natural[192:256]).astype(BF)


def project_kernel(core_ref, rows_ref, own_ref, other_ref, out_ref, mixed):
    low = half(64)
    for side in range(2):
        core = core_ref[0] if side == 0 else 1 - core_ref[0]
        for j in range(4):
            first = rows_ref[4 * j + core].astype(F32)
            second = rows_ref[4 * j + 2 + core].astype(F32)
            cols = slice(128 * j, 128 * j + 128)
            mixed[side, 0:64, cols] = jnp.where(low, first, pltpu.roll(second, 64, 1)).astype(BF)
            mixed[side, 64:128, cols] = jnp.where(low, pltpu.roll(first, 64, 1), second).astype(BF)
    for n in range(4):
        cols = slice(512 * n, 512 * n + 512)
        out_ref[:, cols] = (dot(mixed[0], own_ref[:, cols]) + dot(mixed[1], other_ref[:, cols])).astype(BF)


def vmem():
    return pl.BlockSpec(memory_space=pltpu.VMEM)


def per_device(query_rows, key_rows, value_rows, out_weight, blocks):
    tables = make_tables(blocks)
    index = lax.axis_index(SP).astype(jnp.int32).reshape(1)
    core = lax.axis_index("tp").astype(jnp.int32).reshape(1)
    other_weight = lax.ppermute(out_weight, "tp", [(0, 1), (1, 0)])

    def full(shape):
        return pl.BlockSpec(shape, lambda i, s: (0,) * len(shape))

    send = pl.pallas_call(
        pack_kernel,
        grid_spec=pltpu.PrefetchScalarGridSpec(
            num_scalar_prefetch=1,
            grid=(1,),
            in_specs=[
                full((TOK, 512)),
                full((TOK, 512)),
                full((TOK, 512)),
                full((TOK, TOK)),
                full((TOK, 128)),
                full((TOK, 128)),
                pl.BlockSpec((1, 8, 128), lambda i, s: (s[0], 0, 0)),
            ],
            out_specs=full((GROUP, TOK + 128, 128)),
        ),
        out_shape=jax.ShapeDtypeStruct((GROUP, TOK + 128, 128), BF),
        name="pack",
    )(
        index,
        query_rows,
        key_rows,
        value_rows,
        jnp.asarray(tables["perm"], BF),
        jnp.asarray(tables["cos"]),
        jnp.asarray(tables["sin"]),
        jnp.asarray(tables["anchors"]),
    )
    own = lax.all_to_all(send, ("b", "x"), 0, 0, tiled=True)
    halo = lax.ppermute(own[:, :TOK], SP, [(s, s + GROUP) for s in range(blocks - GROUP)])
    back = pl.pallas_call(
        attend_kernel,
        in_specs=[pl.BlockSpec(memory_space=pltpu.SMEM)] + [vmem()] * 6,
        out_specs=vmem(),
        out_shape=jax.ShapeDtypeStruct((2 * GROUP, 64, 128), BF),
        scratch_shapes=[
            pltpu.VMEM((GROUP, TOK, 128), BF),
            pltpu.VMEM((GROUP, TOK, 128), BF),
            pltpu.VMEM((GROUP, TOK, 128), BF),
            pltpu.VMEM((GROUP, TOK, 128), F32),
            pltpu.VMEM((GROUP, TOK, 128), F32),
        ],
        name="attend",
    )(
        index,
        own,
        halo,
        jnp.asarray(tables["perm"].T, BF),
        jnp.asarray(tables["mask1"]),
        jnp.asarray(tables["mask4"]),
        jnp.asarray(tables["mask16"]),
    )
    rows = lax.all_to_all(back, ("b", "x", "tp"), 0, 0, tiled=True)
    return pl.pallas_call(
        project_kernel,
        in_specs=[pl.BlockSpec(memory_space=pltpu.SMEM)] + [vmem()] * 3,
        out_specs=vmem(),
        out_shape=jax.ShapeDtypeStruct((TOK // 2, 2048), BF),
        scratch_shapes=[pltpu.VMEM((2, TOK // 2, 512), BF)],
        name="project",
    )(core, rows, out_weight, other_weight)


def solution(mesh):
    blocks = mesh.shape["sp"]
    fine = Mesh(mesh.devices.reshape(blocks // 16, 2, 2, 4, 2), SP + ("tp",))
    return jax.shard_map(
        functools.partial(per_device, blocks=blocks),
        mesh=fine,
        in_specs=(P(SP, "tp"), P(SP, "tp"), P(SP, "tp"), P("tp", None)),
        out_specs=P(SP + ("tp",), None),
        check_vma=False,
    )
```

```python
import functools
import math

import jax
import jax.numpy as jnp
import numpy as np
from jax import lax
from jax.experimental import pallas as pl
from jax.experimental.pallas import tpu as pltpu
from jax.sharding import Mesh, PartitionSpec as P


HD = 64
BACK = 128
THETA = 500000.0
TOK = 256
GROUP = 8
SP = ("z", "g", "b", "x")
NEG = -1e30
BF = jnp.bfloat16
F32 = jnp.float32


def row_tokens():
    p = np.arange(TOK)
    residue4, a, n = p // 64, (p % 64) // 16, p % 16
    return 16 * n + residue4 + 4 * a


def make_tables(blocks):
    t = row_tokens()
    inverse = np.float64(THETA) ** (-np.arange(32, dtype=np.float64) / 32)
    lanes = inverse[np.arange(128) % 32]
    inner = t[:, None] * lanes[None, :]
    fine = np.arange(16) * TOK
    coarse = np.arange(blocks // 16) * (16 * TOK)
    anchor = np.concatenate([fine, coarse])[:, None] * lanes[None, :]
    anchors = np.concatenate([np.cos(anchor), np.sin(anchor)], axis=1)
    perm = np.zeros((TOK, TOK), np.float32)
    perm[np.arange(TOK), t] = 1.0

    def band(query, key):
        distance = query[:, None] - key[None, :]
        return np.where((distance >= 0) & (distance <= BACK), 0.0, NEG).astype(np.float32)

    mask1 = band(t, np.concatenate([t - TOK, t]))
    row = np.arange(64)
    sub = 4 * (row % 16) + row // 16
    query4 = np.concatenate([sub, sub + 64])
    mask4 = band(query4, np.concatenate([query4 - 128, query4]))
    query16 = np.arange(128)
    mask16 = band(query16, np.concatenate([query16 - 128, query16]))
    return dict(
        cos=np.cos(inner).astype(np.float32),
        sin=np.sin(inner).astype(np.float32),
        anchors=anchors.astype(np.float32),
        perm=perm,
        mask1=mask1,
        mask4=mask4,
        mask16=mask16,
    )


def dot(a, b):
    return lax.dot_general(a, b, (((1,), (0,)), ((), ())), preferred_element_type=F32)


def dot_t(a, b):
    return lax.dot_general(a, b, (((1,), (1,)), ((), ())), preferred_element_type=F32)


def half(rows):
    return lax.broadcasted_iota(jnp.int32, (rows, 128), 1) < 64


def pack_kernel(index_ref, q_ref, k_ref, v_ref, perm_ref, cos_ref, sin_ref, anchor_ref, out_ref):
    block = index_ref[0]
    fine = anchor_ref[pl.ds(block % 16, 1), :]
    coarse = anchor_ref[pl.ds(16 + block // 16, 1), :]
    cos_a = fine[:, :128] * coarse[:, :128] - fine[:, 128:] * coarse[:, 128:]
    sin_a = fine[:, 128:] * coarse[:, :128] + fine[:, :128] * coarse[:, 128:]
    lane = lax.broadcasted_iota(jnp.int32, (TOK, 128), 1)
    low64 = lane < 64
    low32 = (lane & 63) < 32
    sign = jnp.where(low32[:1], -1.0, 1.0).astype(F32)
    cosine = cos_a * cos_ref[...] - sin_a * sin_ref[...]
    sine = (sin_a * sign) * cos_ref[...] + (cos_a * sign) * sin_ref[...]

    def turn(rows):
        other = jnp.where(low32, pltpu.roll(rows, 96, 1), pltpu.roll(rows, 32, 1))
        return rows * cosine + other * sine

    perm = perm_ref[...]
    for j in range(4):
        cols = slice(128 * j, 128 * j + 128)
        query = turn(dot(perm, q_ref[:, cols])) * (1.0 / math.sqrt(HD))
        key = turn(dot(perm, k_ref[:, cols]))
        value = dot(perm, v_ref[:, cols])
        out_ref[2 * j, 0:TOK] = jnp.where(low64, key, pltpu.roll(value, 64, 1)).astype(BF)
        out_ref[2 * j + 1, 0:TOK] = jnp.where(low64, pltpu.roll(key, 64, 1), value).astype(BF)
        first, second = query[:128], query[128:]
        out_ref[2 * j, TOK : TOK + 128] = jnp.where(low64[:128], first, pltpu.roll(second, 64, 1)).astype(BF)
        out_ref[2 * j + 1, TOK : TOK + 128] = jnp.where(low64[:128], pltpu.roll(first, 64, 1), second).astype(BF)


def wide(x, n):
    return jnp.concatenate([x] * n, axis=1) if n > 1 else x


def lane_of(x, lane):
    return jnp.broadcast_to(x[:, lane : lane + 1], x.shape)


def value_masks(rows):
    low = half(rows)
    return jnp.where(low, 1.0, 0.0).astype(BF), jnp.where(low, 0.0, 1.0).astype(BF)


def stamp(total, peak):
    lane = lax.broadcasted_iota(jnp.int32, total.shape, 1)
    return jnp.where((lane >= 32) & (lane < 64), peak, total)


def fresh(query, keys, values, mask):
    scores = dot_t(query, keys) + mask
    peak = jnp.broadcast_to(jnp.max(scores, axis=1, keepdims=True), (scores.shape[0], 128))
    probs = jnp.exp(scores - wide(peak, scores.shape[1] // 128)).astype(BF)
    return dot(probs, values), peak


def merge(state, query, keys, values, mask):
    scores = dot_t(query, keys) + mask
    before = lane_of(state, 32)
    peak = jnp.maximum(before, jnp.max(scores, axis=1, keepdims=True))
    probs = jnp.exp(scores - wide(peak, scores.shape[1] // 128)).astype(BF)
    return state * jnp.exp(before - peak) + dot(probs, values), peak


def own_kernel(own_ref, mask1_ref, mask4_ref, mask16_ref, acc_ref, qs_ref, vown):
    low256, high256 = value_masks(TOK)
    low_bf = low256[:128]
    for i in range(GROUP):
        packed = own_ref[i, TOK : TOK + 128]
        qs_ref[i, 0:128] = packed * low_bf
        qs_ref[i, 128:256] = pltpu.roll(packed.astype(F32), 64, 1).astype(BF) * low_bf
        vown[i] = own_ref[i, 0:TOK] * high256 + low256
    for r in range(16):
        rows = slice(16 * r, 16 * r + 16)
        total, peak = fresh(
            qs_ref[:, rows].reshape(128, 128),
            own_ref[:, rows].reshape(128, 128),
            vown[:, rows].reshape(128, 128),
            mask16_ref[:, 128:256],
        )
        acc_ref[:, rows] = stamp(total, peak).reshape(8, 16, 128)
    for b in range(4):
        for r in range(4):
            rows = slice(64 * r, 64 * r + 64)
            at = slice(2 * b, 2 * b + 2)
            seen = slice(max(0, 2 * b - 2), 2 * b + 2)
            n = 64 * (seen.stop - seen.start)
            total, peak = merge(
                acc_ref[at, rows].reshape(128, 128),
                qs_ref[at, rows].reshape(128, 128),
                own_ref[seen, rows].reshape(n, 128),
                vown[seen, rows].reshape(n, 128),
                mask4_ref[:, 256 - n : 256],
            )
            acc_ref[at, rows] = stamp(total, peak).reshape(2, 64, 128)
    for i in range(GROUP):
        first = max(0, i - 1)
        n = TOK * (i + 1 - first)
        total, peak = merge(
            acc_ref[i],
            qs_ref[i],
            own_ref[first : i + 1, 0:TOK].reshape(n, 128),
            vown[first : i + 1].reshape(n, 128),
            mask1_ref[:, 2 * TOK - n : 2 * TOK],
        )
        acc_ref[i] = stamp(total, peak)


def halo_rows(index_ref, acc_ref, qs_ref, halo_ref, vhalo, mask4_ref, mask16_ref, new_ref, base):
    bias = jnp.where(index_ref[0] < GROUP, NEG, 0.0).astype(F32)
    low, high = value_masks(128)
    for i in range(GROUP):
        vhalo[i] = halo_ref[i] * high + low
    mask16 = mask16_ref[:, 0:128] + bias
    for r in range(8):
        rows = slice(16 * r, 16 * r + 16)
        full = slice(base + 16 * r, base + 16 * r + 16)
        total, peak = merge(
            acc_ref[:, full].reshape(128, 128),
            qs_ref[:, full].reshape(128, 128),
            halo_ref[:, rows].reshape(128, 128),
            vhalo[:, rows].reshape(128, 128),
            mask16,
        )
        new_ref[:, rows] = stamp(total, peak).reshape(8, 16, 128)
    mask4 = mask4_ref[:, 0:128] + bias
    for r in range(2):
        rows = slice(64 * r, 64 * r + 64)
        full = slice(base + 64 * r, base + 64 * r + 64)
        total, peak = merge(
            new_ref[0:2, rows].reshape(128, 128),
            qs_ref[0:2, full].reshape(128, 128),
            halo_ref[6:8, rows].reshape(128, 128),
            vhalo[6:8, rows].reshape(128, 128),
            mask4,
        )
        new_ref[0:2, rows] = stamp(total, peak).reshape(2, 64, 128)


def first_kernel(index_ref, acc_ref, qs_ref, halo_ref, mask4_ref, mask16_ref, new_ref, vhalo):
    halo_rows(index_ref, acc_ref, qs_ref, halo_ref, vhalo, mask4_ref, mask16_ref, new_ref, 0)


def last_kernel(
    index_ref, acc_ref, qs_ref, done_ref, before_ref, halo_ref, perm_ref, mask1_ref, mask4_ref, mask16_ref, out_ref, vhalo, new
):
    halo_rows(index_ref, acc_ref, qs_ref, halo_ref, vhalo, mask4_ref, mask16_ref, new, 128)
    bias = jnp.where(index_ref[0] < GROUP, NEG, 0.0).astype(F32)
    low256, high256 = value_masks(TOK)
    low_rows = half(64)
    for i in range(GROUP):
        total = jnp.concatenate([done_ref[i], new[i]], axis=0)
        if i == 0:
            keys = jnp.concatenate([before_ref[7], halo_ref[7]], axis=0)
            total, _ = merge(total, qs_ref[0], keys, keys * high256 + low256, mask1_ref[:, 0:TOK] + bias)
        mixed = (total / lane_of(total, 0)).astype(BF) * high256
        natural = dot(perm_ref[...], mixed)
        out_ref[2 * i] = jnp.where(low_rows, pltpu.roll(natural[0:64], 64, 1), natural[64:128]).astype(BF)
        out_ref[2 * i + 1] = jnp.where(low_rows, pltpu.roll(natural[128:192], 64, 1), natural[192:256]).astype(BF)


def project_kernel(core_ref, rows_ref, own_ref, other_ref, out_ref, mixed):
    low = half(64)
    for side in range(2):
        core = core_ref[0] if side == 0 else 1 - core_ref[0]
        for j in range(4):
            first = rows_ref[4 * j + core].astype(F32)
            second = rows_ref[4 * j + 2 + core].astype(F32)
            cols = slice(128 * j, 128 * j + 128)
            mixed[side, 0:64, cols] = jnp.where(low, first, pltpu.roll(second, 64, 1)).astype(BF)
            mixed[side, 64:128, cols] = jnp.where(low, pltpu.roll(first, 64, 1), second).astype(BF)
    for n in range(4):
        cols = slice(512 * n, 512 * n + 512)
        out_ref[:, cols] = (dot(mixed[0], own_ref[:, cols]) + dot(mixed[1], other_ref[:, cols])).astype(BF)


def vmem():
    return pl.BlockSpec(memory_space=pltpu.VMEM)


def limit(mib):
    return pltpu.CompilerParams(vmem_limit_bytes=mib * 2**20)


def per_device(query_rows, key_rows, value_rows, out_weight, blocks):
    tables = make_tables(blocks)
    index = lax.axis_index(SP).astype(jnp.int32).reshape(1)
    core = lax.axis_index("tp").astype(jnp.int32).reshape(1)

    def full(shape):
        return pl.BlockSpec(shape, lambda i, s: (0,) * len(shape))

    send = pl.pallas_call(
        pack_kernel,
        grid_spec=pltpu.PrefetchScalarGridSpec(
            num_scalar_prefetch=1,
            grid=(1,),
            in_specs=[
                full((TOK, 512)),
                full((TOK, 512)),
                full((TOK, 512)),
                full((TOK, TOK)),
                full((TOK, 128)),
                full((TOK, 128)),
                full((16 + blocks // 16, 256)),
            ],
            out_specs=full((GROUP, TOK + 128, 128)),
        ),
        out_shape=jax.ShapeDtypeStruct((GROUP, TOK + 128, 128), BF),
        compiler_params=limit(12),
        name="pack",
    )(
        index,
        query_rows,
        key_rows,
        value_rows,
        jnp.asarray(tables["perm"], BF),
        jnp.asarray(tables["cos"]),
        jnp.asarray(tables["sin"]),
        jnp.asarray(tables["anchors"]),
    )
    own = lax.all_to_all(send, ("b", "x"), 0, 0, tiled=True)
    following = [(s, s + GROUP) for s in range(blocks - GROUP)]
    halo_a = lax.ppermute(own[:, 0:128], SP, following)
    halo_b = lax.ppermute(own[:, 128:256], SP, following)
    weight, _ = lax.optimization_barrier((out_weight, own))
    other_weight = lax.ppermute(weight, "tp", [(0, 1), (1, 0)])
    mask1, mask4, mask16 = (jnp.asarray(tables[name]) for name in ("mask1", "mask4", "mask16"))
    smem = pl.BlockSpec(memory_space=pltpu.SMEM)
    acc, qs = pl.pallas_call(
        own_kernel,
        in_specs=[vmem()] * 4,
        out_specs=[vmem()] * 2,
        out_shape=[
            jax.ShapeDtypeStruct((GROUP, TOK, 128), F32),
            jax.ShapeDtypeStruct((GROUP, TOK, 128), BF),
        ],
        scratch_shapes=[pltpu.VMEM((GROUP, TOK, 128), BF)],
        compiler_params=limit(16),
        cost_estimate=pl.CostEstimate(flops=20 * 10**9, bytes_accessed=2 * 2**20, transcendentals=0),
        name="attend_own",
    )(own, mask1, mask4, mask16)
    done = pl.pallas_call(
        first_kernel,
        in_specs=[smem] + [vmem()] * 5,
        out_specs=vmem(),
        out_shape=jax.ShapeDtypeStruct((GROUP, 128, 128), F32),
        scratch_shapes=[pltpu.VMEM((GROUP, 128, 128), BF)],
        compiler_params=limit(16),
        cost_estimate=pl.CostEstimate(flops=4 * 10**9, bytes_accessed=2 * 2**20, transcendentals=0),
        name="attend_first",
    )(index, acc, qs, halo_a, mask4, mask16)
    back = pl.pallas_call(
        last_kernel,
        in_specs=[smem] + [vmem()] * 9,
        out_specs=vmem(),
        out_shape=jax.ShapeDtypeStruct((2 * GROUP, 64, 128), BF),
        scratch_shapes=[
            pltpu.VMEM((GROUP, 128, 128), BF),
            pltpu.VMEM((GROUP, 128, 128), F32),
        ],
        compiler_params=limit(16),
        cost_estimate=pl.CostEstimate(flops=4 * 10**9, bytes_accessed=2 * 2**20, transcendentals=0),
        name="attend_last",
    )(index, acc, qs, done, halo_a, halo_b, jnp.asarray(tables["perm"].T, BF), mask1, mask4, mask16)
    rows = lax.all_to_all(back, ("b", "x", "tp"), 0, 0, tiled=True)
    return pl.pallas_call(
        project_kernel,
        in_specs=[pl.BlockSpec(memory_space=pltpu.SMEM)] + [vmem()] * 3,
        out_specs=vmem(),
        out_shape=jax.ShapeDtypeStruct((TOK // 2, 2048), BF),
        scratch_shapes=[pltpu.VMEM((2, TOK // 2, 512), BF)],
        compiler_params=limit(16),
        name="project",
    )(core, rows, out_weight, other_weight)


def solution(mesh):
    blocks = mesh.shape["sp"]
    fine = Mesh(mesh.devices.reshape(blocks // 16, 2, 2, 4, 2), SP + ("tp",))
    return jax.shard_map(
        functools.partial(per_device, blocks=blocks),
        mesh=fine,
        in_specs=(P(SP, "tp"), P(SP, "tp"), P(SP, "tp"), P("tp", None)),
        out_specs=P(SP + ("tp",), None),
        check_vma=False,
    )
```

```python
import functools
import math

import jax
import jax.numpy as jnp
import numpy as np
from jax import lax
from jax.experimental import pallas as pl
from jax.experimental.pallas import tpu as pltpu
from jax.sharding import Mesh, PartitionSpec as P


HD = 64
BACK = 128
THETA = 500000.0
TOK = 256
GROUP = 8
SP = ("z", "g", "b", "x")
NEG = -1e30
BF = jnp.bfloat16
F32 = jnp.float32


def row_tokens():
    p = np.arange(TOK)
    residue4, a, n = p // 64, (p % 64) // 16, p % 16
    return 16 * n + residue4 + 4 * a


def make_tables(blocks):
    t = row_tokens()
    inverse = np.float64(THETA) ** (-np.arange(32, dtype=np.float64) / 32)
    lanes = inverse[np.arange(128) % 32]
    inner = t[:, None] * lanes[None, :]
    fine = np.arange(16) * TOK
    coarse = np.arange(blocks // 16) * (16 * TOK)
    anchor = np.concatenate([fine, coarse])[:, None] * lanes[None, :]
    anchors = np.concatenate([np.cos(anchor), np.sin(anchor)], axis=1)
    perm = np.zeros((TOK, TOK), np.float32)
    perm[np.arange(TOK), t] = 1.0

    def band(query, key):
        distance = query[:, None] - key[None, :]
        return np.where((distance >= 0) & (distance <= BACK), 0.0, NEG).astype(np.float32)

    mask1 = band(t, np.concatenate([t - TOK, t]))
    row = np.arange(64)
    sub = 4 * (row % 16) + row // 16
    query4 = np.concatenate([sub, sub + 64])
    mask4 = band(query4, np.concatenate([query4 - 128, query4]))
    query16 = np.arange(128)
    mask16 = band(query16, np.concatenate([query16 - 128, query16]))
    return dict(
        cos=np.cos(inner).astype(np.float32),
        sin=np.sin(inner).astype(np.float32),
        anchors=anchors.astype(np.float32),
        perm=perm,
        mask1=mask1,
        mask4=mask4,
        mask16=mask16,
    )


def dot(a, b):
    return lax.dot_general(a, b, (((1,), (0,)), ((), ())), preferred_element_type=F32)


def dot_t(a, b):
    return lax.dot_general(a, b, (((1,), (1,)), ((), ())), preferred_element_type=F32)


def half(rows):
    return lax.broadcasted_iota(jnp.int32, (rows, 128), 1) < 64


def pack_kernel(
    index_ref, core_ref, q_hbm, k_hbm, v_hbm, perm_hbm, cos_hbm, sin_hbm, anchor_hbm, out_ref,
    q_ref, k_ref, v_ref, perm_ref, cos_ref, sin_ref, anchor_ref, sems,
):
    pairs = (
        (anchor_hbm, anchor_ref), (cos_hbm, cos_ref), (sin_hbm, sin_ref), (perm_hbm, perm_ref),
        (q_hbm, q_ref), (k_hbm, k_ref), (v_hbm, v_ref),
    )
    copies = [pltpu.make_async_copy(source, target, sems.at[n]) for n, (source, target) in enumerate(pairs)]
    for copy in copies:
        copy.start()
    for copy in copies:
        copy.wait()
    block = index_ref[0]
    flip = 4 * ((block // GROUP) % 2)
    fine = anchor_ref[pl.ds(block % 16, 1), :]
    coarse = anchor_ref[pl.ds(16 + block // 16, 1), :]
    cos_a = fine[:, :128] * coarse[:, :128] - fine[:, 128:] * coarse[:, 128:]
    sin_a = fine[:, 128:] * coarse[:, :128] + fine[:, :128] * coarse[:, 128:]
    lane = lax.broadcasted_iota(jnp.int32, (TOK, 128), 1)
    low64 = lane < 64
    low32 = (lane & 63) < 32
    sign = jnp.where(low32[:1], -1.0, 1.0).astype(F32)
    cosine = cos_a * cos_ref[...] - sin_a * sin_ref[...]
    sine = (sin_a * sign) * cos_ref[...] + (cos_a * sign) * sin_ref[...]

    def turn(rows):
        other = jnp.where(low32, pltpu.roll(rows, 96, 1), pltpu.roll(rows, 32, 1))
        return rows * cosine + other * sine

    perm = perm_ref[...]
    for j in range(4):
        cols = slice(128 * j, 128 * j + 128)
        query = turn(dot(perm, q_ref[:, cols])) * (1.0 / math.sqrt(HD))
        key = turn(dot(perm, k_ref[:, cols]))
        value = dot(perm, v_ref[:, cols])
        even = (2 * j) ^ flip
        odd = even + 1
        out_ref[even, 0:TOK] = jnp.where(low64, key, pltpu.roll(value, 64, 1)).astype(BF)
        out_ref[odd, 0:TOK] = jnp.where(low64, pltpu.roll(key, 64, 1), value).astype(BF)
        first, second = query[:128], query[128:]
        out_ref[even, TOK : TOK + 128] = jnp.where(low64[:128], first, pltpu.roll(second, 64, 1)).astype(BF)
        out_ref[odd, TOK : TOK + 128] = jnp.where(low64[:128], pltpu.roll(first, 64, 1), second).astype(BF)


def wide(x, n):
    return jnp.concatenate([x] * n, axis=1) if n > 1 else x


def value_masks(rows):
    low = half(rows)
    return jnp.where(low, 1.0, 0.0).astype(BF), jnp.where(low, 0.0, 1.0).astype(BF)


def merge(total, before, query, keys, values, mask):
    scores = dot_t(query, keys) + mask
    peak = jnp.maximum(before, jnp.max(scores, axis=1, keepdims=True))
    probs = jnp.exp(scores - wide(peak, scores.shape[1] // 128)).astype(BF)
    return total * jnp.exp(before - peak) + dot(probs, values), peak


def normal(total):
    return total / pltpu.roll(total, 64, 1)


def own_kernel(own_ref, mask1_ref, mask4_ref, mask16_ref, acc_ref, top_ref, qs_ref, ks, vs):
    low256, high256 = value_masks(TOK)
    low_bf = low256[:128]
    for i in range(GROUP):
        packed = own_ref[i, TOK : TOK + 128]
        qs_ref[i, 0:128] = packed * low_bf
        qs_ref[i, 128:256] = pltpu.roll(packed.astype(F32), 64, 1).astype(BF) * low_bf
        key = own_ref[i, 0:TOK]
        ks[i, 0:TOK] = key
        vs[i, 0:TOK] = key * high256 + low256
    for r in range(16):
        rows = slice(16 * r, 16 * r + 16)
        scores = dot_t(qs_ref[:, rows].reshape(128, 128), ks[:, rows].reshape(128, 128)) + mask16_ref[:, 128:256]
        peak = jnp.broadcast_to(jnp.max(scores, axis=1, keepdims=True), (128, 128))
        probs = jnp.exp(scores - peak).astype(BF)
        acc_ref[:, rows] = dot(probs, vs[:, rows].reshape(128, 128)).reshape(8, 16, 128)
        top_ref[:, rows] = peak.reshape(8, 16, 128)
    for b in range(4):
        for r in range(4):
            rows = slice(64 * r, 64 * r + 64)
            at = slice(2 * b, 2 * b + 2)
            seen = slice(max(0, 2 * b - 2), 2 * b + 2)
            n = 64 * (seen.stop - seen.start)
            total, peak = merge(
                acc_ref[at, rows].reshape(128, 128),
                top_ref[at, rows].reshape(128, 128),
                qs_ref[at, rows].reshape(128, 128),
                ks[seen, rows].reshape(n, 128),
                vs[seen, rows].reshape(n, 128),
                mask4_ref[:, 256 - n : 256],
            )
            acc_ref[at, rows] = total.reshape(2, 64, 128)
            top_ref[at, rows] = peak.reshape(2, 64, 128)
    for i in range(GROUP):
        first = max(0, i - 1)
        n = TOK * (i + 1 - first)
        total, peak = merge(
            acc_ref[i, 0:TOK],
            top_ref[i, 0:TOK],
            qs_ref[i, 0:TOK],
            ks[first : i + 1, 0:TOK].reshape(n, 128),
            vs[first : i + 1, 0:TOK].reshape(n, 128),
            mask1_ref[:, 2 * TOK - n : 2 * TOK],
        )
        acc_ref[i, 0:TOK] = total
        top_ref[i, 0:TOK] = peak


def halo_rows(acc_ref, top_ref, qs_ref, ks, vs, mask4, mask16, new, head, base, store):
    for r in range(2):
        rows = slice(64 * r, 64 * r + 64)
        full = slice(base + 64 * r, base + 64 * r + 64)
        total, peak = merge(
            acc_ref[0:2, full].reshape(128, 128),
            top_ref[0:2, full].reshape(128, 128),
            qs_ref[0:2, full].reshape(128, 128),
            ks[6:8, rows].reshape(128, 128),
            vs[6:8, rows].reshape(128, 128),
            mask4,
        )
        new[0:2, rows] = total.reshape(2, 64, 128)
        head[0:2, rows] = peak.reshape(2, 64, 128)
    for r in range(8):
        rows = slice(16 * r, 16 * r + 16)
        full = slice(base + 16 * r, base + 16 * r + 16)
        total, _ = merge(
            jnp.concatenate([new[0:2, rows], acc_ref[2:8, full]], axis=0).reshape(128, 128),
            jnp.concatenate([head[0:2, rows], top_ref[2:8, full]], axis=0).reshape(128, 128),
            qs_ref[:, full].reshape(128, 128),
            ks[0:8, rows].reshape(128, 128),
            vs[0:8, rows].reshape(128, 128),
            mask16,
        )
        store(rows, normal(total).reshape(8, 16, 128).astype(BF))


def spread(halo_ref, ks, vs, n):
    low, high = value_masks(128)
    for i in range(n):
        key = halo_ref[i]
        ks[i, 0:128] = key
        vs[i, 0:128] = key * high + low


def first_kernel(
    index_ref, acc_ref, top_ref, qs_ref, halo_ref, mask1_ref, mask4_ref, mask16_ref,
    lo_ref, acc0_ref, top0_ref, ks, vs, new, head, state, peaks,
):
    bias = jnp.where(index_ref[0] < GROUP, NEG, 0.0).astype(F32)
    spread(halo_ref, ks, vs, GROUP + 1)
    total, peak = merge(
        acc_ref[0, 0:TOK],
        top_ref[0, 0:TOK],
        qs_ref[0, 0:TOK],
        ks[7:9, 0:128].reshape(TOK, 128),
        vs[7:9, 0:128].reshape(TOK, 128),
        mask1_ref[:, 0:TOK] + bias,
    )
    acc0_ref[...] = total[128:]
    top0_ref[...] = peak[128:]
    state[0, 0:128] = total[:128]
    peaks[0, 0:128] = peak[:128]
    state[1, 0:128] = acc_ref[1, 0:128]
    peaks[1, 0:128] = top_ref[1, 0:128]

    def store(rows, value):
        lo_ref[:, rows] = value

    halo_rows(
        Stacked(state, acc_ref), Stacked(peaks, top_ref), qs_ref, ks, vs,
        mask4_ref[:, 0:128] + bias, mask16_ref[:, 0:128] + bias, new, head, 0, store,
    )


def last_kernel(
    index_ref, acc_ref, top_ref, acc0_ref, top0_ref, qs_ref, lo_ref, halo_ref, perm_ref, mask4_ref, mask16_ref,
    out_ref, ks, vs, new, head, state, peaks, hi,
):
    bias = jnp.where(index_ref[0] < GROUP, NEG, 0.0).astype(F32)
    spread(halo_ref, ks, vs, GROUP)
    state[0, 128:256] = acc0_ref[...]
    peaks[0, 128:256] = top0_ref[...]
    state[1, 128:256] = acc_ref[1, 128:256]
    peaks[1, 128:256] = top_ref[1, 128:256]

    def store(rows, value):
        hi[:, rows] = value

    halo_rows(
        Stacked(state, acc_ref), Stacked(peaks, top_ref), qs_ref, ks, vs,
        mask4_ref[:, 0:128] + bias, mask16_ref[:, 0:128] + bias, new, head, 128, store,
    )
    _, high = value_masks(TOK)
    low_rows = half(64)
    for i in range(GROUP):
        mixed = jnp.concatenate([lo_ref[i, 0:128], hi[i, 0:128]], axis=0) * high
        natural = dot(perm_ref[...], mixed)
        out_ref[2 * i] = jnp.where(low_rows, pltpu.roll(natural[0:64], 64, 1), natural[64:128]).astype(BF)
        out_ref[2 * i + 1] = jnp.where(low_rows, pltpu.roll(natural[128:192], 64, 1), natural[192:256]).astype(BF)


class Stacked:

    def __init__(self, start, rest):
        self.start, self.rest = start, rest

    def __getitem__(self, at):
        blocks, rows = at
        return (self.start if blocks.stop <= 2 else self.rest)[blocks, rows]


def project_kernel(index_ref, core_ref, rows_ref, own_ref, other_ref, out_ref, mixed):
    low = half(64)
    flip = 4 * ((index_ref[0] // GROUP) % 2)
    for side in range(2):
        core = core_ref[0] if side == 0 else 1 - core_ref[0]
        for j in range(4):
            first = rows_ref[2 * ((2 * j) ^ flip) + core].astype(F32)
            second = rows_ref[2 * ((2 * j) ^ flip) + 2 + core].astype(F32)
            cols = slice(128 * j, 128 * j + 128)
            mixed[side, 0:64, cols] = jnp.where(low, first, pltpu.roll(second, 64, 1)).astype(BF)
            mixed[side, 64:128, cols] = jnp.where(low, pltpu.roll(first, 64, 1), second).astype(BF)
    for n in range(4):
        cols = slice(512 * n, 512 * n + 512)
        out_ref[:, cols] = (dot(mixed[0], own_ref[:, cols]) + dot(mixed[1], other_ref[:, cols])).astype(BF)


def vmem():
    return pl.BlockSpec(memory_space=pltpu.VMEM)


def limit(mib):
    return pltpu.CompilerParams(vmem_limit_bytes=mib * 2**20)


def per_device(query_rows, key_rows, value_rows, out_weight, blocks):
    tables = make_tables(blocks)
    index = lax.axis_index(SP).astype(jnp.int32).reshape(1)
    core = lax.axis_index("tp").astype(jnp.int32).reshape(1)

    smem = pl.BlockSpec(memory_space=pltpu.SMEM)
    hbm = pl.BlockSpec(memory_space=pltpu.HBM)
    send = pl.pallas_call(
        pack_kernel,
        in_specs=[smem] * 2 + [hbm] * 7,
        out_specs=vmem(),
        out_shape=jax.ShapeDtypeStruct((GROUP, TOK + 128, 128), BF),
        scratch_shapes=[
            pltpu.VMEM((TOK, 512), BF),
            pltpu.VMEM((TOK, 512), BF),
            pltpu.VMEM((TOK, 512), BF),
            pltpu.VMEM((TOK, TOK), BF),
            pltpu.VMEM((TOK, 128), F32),
            pltpu.VMEM((TOK, 128), F32),
            pltpu.VMEM((16 + blocks // 16, 256), F32),
            pltpu.SemaphoreType.DMA((7,)),
        ],
        compiler_params=limit(12),
        name="pack",
    )(
        index,
        core,
        *(
            pltpu.with_memory_space_constraint(array, pltpu.HBM)
            for array in (
                query_rows,
                key_rows,
                value_rows,
                jnp.asarray(tables["perm"], BF),
                jnp.asarray(tables["cos"]),
                jnp.asarray(tables["sin"]),
                jnp.asarray(tables["anchors"]),
            )
        ),
    )
    own = lax.all_to_all(send, ("b", "x"), 0, 0, tiled=True)
    following = [(s, (s // GROUP + 1) * GROUP + ((s % GROUP) ^ 4)) for s in range(blocks - GROUP)]
    halo_a = lax.ppermute(jnp.concatenate([own[:, 0:128], own[7:8, 128:256]], axis=0), SP, following)
    halo_b = lax.ppermute(own[:, 128:256], SP, following)
    weight, _ = lax.optimization_barrier((out_weight, own))
    other_weight = lax.ppermute(weight, "tp", [(0, 1), (1, 0)])
    mask1, mask4, mask16 = (jnp.asarray(tables[name]) for name in ("mask1", "mask4", "mask16"))
    state = jax.ShapeDtypeStruct((GROUP, TOK + 8, 128), F32)
    acc, top, qs = pl.pallas_call(
        own_kernel,
        in_specs=[vmem()] * 4,
        out_specs=[vmem()] * 3,
        out_shape=[state, state, jax.ShapeDtypeStruct((GROUP, TOK + 16, 128), BF)],
        scratch_shapes=[pltpu.VMEM((GROUP, TOK + 16, 128), BF)] * 2,
        compiler_params=limit(16),
        cost_estimate=pl.CostEstimate(flops=20 * 10**9, bytes_accessed=2 * 2**20, transcendentals=0),
        name="attend_own",
    )(own, mask1, mask4, mask16)
    part = jax.ShapeDtypeStruct((128, 128), F32)
    lo, acc0, top0 = pl.pallas_call(
        first_kernel,
        in_specs=[smem] + [vmem()] * 7,
        out_specs=[vmem()] * 3,
        out_shape=[jax.ShapeDtypeStruct((GROUP, 144, 128), BF), part, part],
        scratch_shapes=[pltpu.VMEM((GROUP + 1, 144, 128), BF)] * 2
        + [pltpu.VMEM((2, 136, 128), F32)] * 2
        + [pltpu.VMEM((2, TOK + 8, 128), F32)] * 2,
        compiler_params=limit(16),
        cost_estimate=pl.CostEstimate(flops=4 * 10**9, bytes_accessed=2 * 2**20, transcendentals=0),
        name="attend_first",
    )(index, acc, top, qs, halo_a, mask1, mask4, mask16)
    back = pl.pallas_call(
        last_kernel,
        in_specs=[smem] + [vmem()] * 10,
        out_specs=vmem(),
        out_shape=jax.ShapeDtypeStruct((2 * GROUP, 64, 128), BF),
        scratch_shapes=[pltpu.VMEM((GROUP, 144, 128), BF)] * 2
        + [pltpu.VMEM((2, 136, 128), F32)] * 2
        + [pltpu.VMEM((2, TOK + 8, 128), F32)] * 2
        + [pltpu.VMEM((GROUP, 144, 128), BF)],
        compiler_params=limit(16),
        cost_estimate=pl.CostEstimate(flops=4 * 10**9, bytes_accessed=2 * 2**20, transcendentals=0),
        name="attend_last",
    )(index, acc, top, acc0, top0, qs, lo, halo_b, jnp.asarray(tables["perm"].T, BF), mask4, mask16)
    back, other_weight = lax.optimization_barrier((back, other_weight))
    rows = lax.all_to_all(back, ("b", "x", "tp"), 0, 0, tiled=True)
    return pl.pallas_call(
        project_kernel,
        in_specs=[smem] * 2 + [vmem()] * 3,
        out_specs=vmem(),
        out_shape=jax.ShapeDtypeStruct((TOK // 2, 2048), BF),
        scratch_shapes=[pltpu.VMEM((2, TOK // 2, 512), BF)],
        compiler_params=limit(16),
        name="project",
    )(index, core, rows, out_weight, other_weight)


def solution(mesh):
    blocks = mesh.shape["sp"]
    fine = Mesh(mesh.devices.reshape(blocks // 16, 2, 2, 4, 2), SP + ("tp",))
    return jax.shard_map(
        functools.partial(per_device, blocks=blocks),
        mesh=fine,
        in_specs=(P(SP, "tp"), P(SP, "tp"), P(SP, "tp"), P("tp", None)),
        out_specs=P(SP + ("tp",), None),
        check_vma=False,
    )
```

```python
import functools
import math

import jax
import jax.numpy as jnp
import numpy as np
from jax import lax
from jax.experimental import pallas as pl
from jax.experimental.pallas import tpu as pltpu
from jax.sharding import Mesh, PartitionSpec as P


HD = 64
BACK = 128
THETA = 500000.0
TOK = 256
GROUP = 8
SP = ("z", "g", "b", "x")
NEG = -1e30
BF = jnp.bfloat16
F32 = jnp.float32


def row_tokens():
    p = np.arange(TOK)
    residue4, a, n = p // 64, (p % 64) // 16, p % 16
    return 16 * n + residue4 + 4 * a


def make_tables(blocks):
    t = row_tokens()
    inverse = np.float64(THETA) ** (-np.arange(32, dtype=np.float64) / 32)
    lanes = inverse[np.arange(128) % 32]
    inner = t[:, None] * lanes[None, :]
    fine = np.arange(16) * TOK
    coarse = np.arange(blocks // 16) * (16 * TOK)
    anchor = np.concatenate([fine, coarse])[:, None] * lanes[None, :]
    anchors = np.concatenate([np.cos(anchor), np.sin(anchor)], axis=1)
    perm = np.zeros((TOK, TOK), np.float32)
    perm[np.arange(TOK), t] = 1.0

    def band(query, key):
        distance = query[:, None] - key[None, :]
        return np.where((distance >= 0) & (distance <= BACK), 0.0, NEG).astype(np.float32)

    mask1 = band(t, np.concatenate([t - TOK, t]))
    row = np.arange(64)
    sub = 4 * (row % 16) + row // 16
    query4 = np.concatenate([sub, sub + 64])
    mask4 = band(query4, np.concatenate([query4 - 128, query4]))
    query16 = np.arange(128)
    mask16 = band(query16, np.concatenate([query16 - 128, query16]))
    return dict(
        cos=np.cos(inner).astype(np.float32),
        sin=np.sin(inner).astype(np.float32),
        anchors=anchors.astype(np.float32),
        perm=perm,
        mask1=mask1,
        mask4=mask4,
        mask16=mask16,
    )


def dot(a, b):
    return lax.dot_general(a, b, (((1,), (0,)), ((), ())), preferred_element_type=F32)


def dot_t(a, b):
    return lax.dot_general(a, b, (((1,), (1,)), ((), ())), preferred_element_type=F32)


def half(rows):
    return lax.broadcasted_iota(jnp.int32, (rows, 128), 1) < 64


def pack_kernel(
    index_ref, core_ref, q_hbm, k_hbm, v_hbm, perm_hbm, cos_hbm, sin_hbm, anchor_hbm, out_ref,
    q_ref, k_ref, v_ref, perm_ref, cos_ref, sin_ref, anchor_ref, sems,
):
    pairs = (
        (anchor_hbm, anchor_ref), (cos_hbm, cos_ref), (sin_hbm, sin_ref), (perm_hbm, perm_ref),
        (q_hbm, q_ref), (k_hbm, k_ref), (v_hbm, v_ref),
    )
    copies = [pltpu.make_async_copy(source, target, sems.at[n]) for n, (source, target) in enumerate(pairs)]
    for copy in copies:
        copy.start()
    for copy in copies:
        copy.wait()
    block = index_ref[0]
    flip = 4 * ((block // GROUP) % 2)
    fine = anchor_ref[pl.ds(block % 16, 1), :]
    coarse = anchor_ref[pl.ds(16 + block // 16, 1), :]
    cos_a = fine[:, :128] * coarse[:, :128] - fine[:, 128:] * coarse[:, 128:]
    sin_a = fine[:, 128:] * coarse[:, :128] + fine[:, :128] * coarse[:, 128:]
    lane = lax.broadcasted_iota(jnp.int32, (TOK, 128), 1)
    low64 = lane < 64
    low32 = (lane & 63) < 32
    sign = jnp.where(low32[:1], -1.0, 1.0).astype(F32)
    cosine = cos_a * cos_ref[...] - sin_a * sin_ref[...]
    sine = (sin_a * sign) * cos_ref[...] + (cos_a * sign) * sin_ref[...]

    def turn(rows):
        other = jnp.where(low32, pltpu.roll(rows, 96, 1), pltpu.roll(rows, 32, 1))
        return rows * cosine + other * sine

    perm = perm_ref[...]
    for j in range(4):
        cols = slice(128 * j, 128 * j + 128)
        query = turn(dot(perm, q_ref[:, cols])) * (1.0 / math.sqrt(HD))
        key = turn(dot(perm, k_ref[:, cols]))
        value = dot(perm, v_ref[:, cols])
        even = (2 * j) ^ flip
        odd = even + 1
        out_ref[even, 0:TOK] = jnp.where(low64, key, pltpu.roll(value, 64, 1)).astype(BF)
        out_ref[odd, 0:TOK] = jnp.where(low64, pltpu.roll(key, 64, 1), value).astype(BF)
        first, second = query[:128], query[128:]
        out_ref[even, TOK : TOK + 128] = jnp.where(low64[:128], first, pltpu.roll(second, 64, 1)).astype(BF)
        out_ref[odd, TOK : TOK + 128] = jnp.where(low64[:128], pltpu.roll(first, 64, 1), second).astype(BF)


def wide(x, n):
    return jnp.concatenate([x] * n, axis=1) if n > 1 else x


def value_masks(rows):
    low = half(rows)
    return jnp.where(low, 1.0, 0.0).astype(BF), jnp.where(low, 0.0, 1.0).astype(BF)


def normal(total):
    return total / pltpu.roll(total, 64, 1)


def row_max(scores):
    return jnp.max(scores, axis=1, keepdims=True)


def weights(scores, peak):
    return jnp.exp(scores - wide(peak, scores.shape[1] // 128)).astype(BF)


def own_kernel(own_ref, mask1_ref, mask4_ref, mask16_ref, acc_ref, top_ref, qs_ref, ks, vs, s16, s4, s1, p16, p4, p1):
    low256, high256 = value_masks(TOK)
    low_bf = low256[:128]
    for i in range(GROUP):
        packed = own_ref[i, TOK : TOK + 128]
        qs_ref[i, 0:128] = packed * low_bf
        qs_ref[i, 128:256] = pltpu.roll(packed.astype(F32), 64, 1).astype(BF) * low_bf
        key = own_ref[i, 0:TOK]
        ks[i, 0:TOK] = key
        vs[i, 0:TOK] = key * high256 + low256

    def at4(n):
        b, r = n // 4, n % 4
        seen = slice(max(0, 2 * b - 2), 2 * b + 2)
        return slice(2 * b, 2 * b + 2), slice(64 * r, 64 * r + 64), seen, 64 * (seen.stop - seen.start)

    def at1(i):
        seen = slice(max(0, i - 1), i + 1)
        return seen, TOK * (seen.stop - seen.start)

    for r in range(16):
        rows = slice(16 * r, 16 * r + 16)
        scores = dot_t(qs_ref[:, rows].reshape(128, 128), ks[:, rows].reshape(128, 128)) + mask16_ref[:, 128:256]
        s16[r] = scores
        top_ref[:, rows] = jnp.broadcast_to(row_max(scores), (128, 128)).reshape(8, 16, 128)
    for n in range(16):
        at, rows, seen, width = at4(n)
        scores = dot_t(qs_ref[at, rows].reshape(128, 128), ks[seen, rows].reshape(width, 128))
        scores = scores + mask4_ref[:, 256 - width : 256]
        s4[n, :, 0:width] = scores
        top_ref[at, rows] = jnp.maximum(top_ref[at, rows].reshape(128, 128), row_max(scores)).reshape(2, 64, 128)
    for i in range(GROUP):
        seen, width = at1(i)
        scores = dot_t(qs_ref[i, 0:TOK], ks[seen, 0:TOK].reshape(width, 128)) + mask1_ref[:, 512 - width : 512]
        s1[i, :, 0:width] = scores
        top_ref[i, 0:TOK] = jnp.maximum(top_ref[i, 0:TOK], row_max(scores))
    for r in range(16):
        p16[r] = weights(s16[r], top_ref[:, 16 * r : 16 * r + 16].reshape(128, 128))
    for n in range(16):
        at, rows, seen, width = at4(n)
        p4[n, :, 0:width] = weights(s4[n, :, 0:width], top_ref[at, rows].reshape(128, 128))
    for i in range(GROUP):
        seen, width = at1(i)
        p1[i, :, 0:width] = weights(s1[i, :, 0:width], top_ref[i, 0:TOK])
    for r in range(16):
        rows = slice(16 * r, 16 * r + 16)
        acc_ref[:, rows] = dot(p16[r], vs[:, rows].reshape(128, 128)).reshape(8, 16, 128)
    for n in range(16):
        at, rows, seen, width = at4(n)
        acc_ref[at, rows] += dot(p4[n, :, 0:width], vs[seen, rows].reshape(width, 128)).reshape(2, 64, 128)
    for i in range(GROUP):
        seen, width = at1(i)
        acc_ref[i, 0:TOK] += dot(p1[i, :, 0:width], vs[seen, 0:TOK].reshape(width, 128))


def halo_rows(index_ref, acc_ref, top_ref, qs_ref, masks, scratch, base):
    mask1_ref, mask4_ref, mask16_ref = masks
    ks, vs, new, peak, s16, s4, s1, p16, p4, p1 = scratch
    bias = jnp.where(index_ref[0] < GROUP, NEG, 0.0).astype(F32)
    half_rows = slice(base, base + 128)
    order = (7, 8) if base == 0 else (8, 7)

    def both(ref):
        return jnp.concatenate([ref[order[0], 0:128], ref[order[1], 0:128]], axis=0)

    mask16 = mask16_ref[:, 0:128] + bias
    for r in range(8):
        rows = slice(16 * r, 16 * r + 16)
        full = slice(base + 16 * r, base + 16 * r + 16)
        scores = dot_t(qs_ref[:, full].reshape(128, 128), ks[0:8, rows].reshape(128, 128)) + mask16
        s16[r] = scores
        peak[:, rows] = jnp.maximum(top_ref[:, full].reshape(128, 128), row_max(scores)).reshape(8, 16, 128)
    mask4 = mask4_ref[:, 0:128] + bias
    for r in range(2):
        rows = slice(64 * r, 64 * r + 64)
        full = slice(base + 64 * r, base + 64 * r + 64)
        scores = dot_t(qs_ref[0:2, full].reshape(128, 128), ks[6:8, rows].reshape(128, 128)) + mask4
        s4[r] = scores
        peak[0:2, rows] = jnp.maximum(peak[0:2, rows].reshape(128, 128), row_max(scores)).reshape(2, 64, 128)
    scores = dot_t(qs_ref[0, half_rows], both(ks)) + (mask1_ref[half_rows, 0:TOK] + bias)
    s1[...] = scores
    peak[0, 0:128] = jnp.maximum(peak[0, 0:128], row_max(scores))
    for r in range(8):
        p16[r] = weights(s16[r], peak[:, 16 * r : 16 * r + 16].reshape(128, 128))
    for r in range(2):
        p4[r] = weights(s4[r], peak[0:2, 64 * r : 64 * r + 64].reshape(128, 128))
    p1[...] = weights(s1[...], peak[0, 0:128])
    for i in range(GROUP):
        new[i, 0:128] = acc_ref[i, half_rows] * jnp.exp(top_ref[i, half_rows] - peak[i, 0:128])
    for r in range(8):
        rows = slice(16 * r, 16 * r + 16)
        new[:, rows] += dot(p16[r], vs[0:8, rows].reshape(128, 128)).reshape(8, 16, 128)
    for r in range(2):
        rows = slice(64 * r, 64 * r + 64)
        new[0:2, rows] += dot(p4[r], vs[6:8, rows].reshape(128, 128)).reshape(2, 64, 128)
    new[0, 0:128] += dot(p1[...], both(vs))


def spread(halo_ref, ks, vs, n):
    low, high = value_masks(128)
    for i in range(n):
        key = halo_ref[i]
        ks[i, 0:128] = key
        vs[i, 0:128] = key * high + low


def first_kernel(index_ref, acc_ref, top_ref, qs_ref, halo_ref, mask1_ref, mask4_ref, mask16_ref, lo_ref, *scratch):
    ks, vs, new = scratch[:3]
    spread(halo_ref, ks, vs, GROUP + 1)
    halo_rows(index_ref, acc_ref, top_ref, qs_ref, (mask1_ref, mask4_ref, mask16_ref), scratch, 0)
    _, high = value_masks(128)
    for i in range(GROUP):
        lo_ref[i, 0:128] = normal(new[i, 0:128]).astype(BF) * high


def last_kernel(
    index_ref, acc_ref, top_ref, qs_ref, lo_ref, before_ref, halo_ref, perm_ref, mask1_ref, mask4_ref, mask16_ref,
    out_ref, *scratch,
):
    ks, vs, new = scratch[:3]
    spread(halo_ref, ks, vs, GROUP)
    low, high = value_masks(128)
    key = before_ref[7]
    ks[GROUP, 0:128] = key
    vs[GROUP, 0:128] = key * high + low
    halo_rows(index_ref, acc_ref, top_ref, qs_ref, (mask1_ref, mask4_ref, mask16_ref), scratch, 128)
    low_rows = half(64)
    for i in range(GROUP):
        mixed = jnp.concatenate([lo_ref[i, 0:128], normal(new[i, 0:128]).astype(BF) * high], axis=0)
        natural = dot(perm_ref[...], mixed)
        out_ref[2 * i] = jnp.where(low_rows, pltpu.roll(natural[0:64], 64, 1), natural[64:128]).astype(BF)
        out_ref[2 * i + 1] = jnp.where(low_rows, pltpu.roll(natural[128:192], 64, 1), natural[192:256]).astype(BF)


def project_kernel(index_ref, core_ref, rows_ref, own_ref, other_ref, out_ref, mixed):
    low = half(64)
    flip = 4 * ((index_ref[0] // GROUP) % 2)
    for side in range(2):
        core = core_ref[0] if side == 0 else 1 - core_ref[0]
        for j in range(4):
            first = rows_ref[2 * ((2 * j) ^ flip) + core].astype(F32)
            second = rows_ref[2 * ((2 * j) ^ flip) + 2 + core].astype(F32)
            cols = slice(128 * j, 128 * j + 128)
            mixed[side, 0:64, cols] = jnp.where(low, first, pltpu.roll(second, 64, 1)).astype(BF)
            mixed[side, 64:128, cols] = jnp.where(low, pltpu.roll(first, 64, 1), second).astype(BF)
    for n in range(4):
        cols = slice(512 * n, 512 * n + 512)
        out_ref[:, cols] = (dot(mixed[0], own_ref[:, cols]) + dot(mixed[1], other_ref[:, cols])).astype(BF)


def vmem():
    return pl.BlockSpec(memory_space=pltpu.VMEM)


def limit(mib):
    return pltpu.CompilerParams(vmem_limit_bytes=mib * 2**20)


def per_device(query_rows, key_rows, value_rows, out_weight, blocks):
    tables = make_tables(blocks)
    index = lax.axis_index(SP).astype(jnp.int32).reshape(1)
    core = lax.axis_index("tp").astype(jnp.int32).reshape(1)

    smem = pl.BlockSpec(memory_space=pltpu.SMEM)
    hbm = pl.BlockSpec(memory_space=pltpu.HBM)
    send = pl.pallas_call(
        pack_kernel,
        in_specs=[smem] * 2 + [hbm] * 7,
        out_specs=vmem(),
        out_shape=jax.ShapeDtypeStruct((GROUP, TOK + 128, 128), BF),
        scratch_shapes=[
            pltpu.VMEM((TOK, 512), BF),
            pltpu.VMEM((TOK, 512), BF),
            pltpu.VMEM((TOK, 512), BF),
            pltpu.VMEM((TOK, TOK), BF),
            pltpu.VMEM((TOK, 128), F32),
            pltpu.VMEM((TOK, 128), F32),
            pltpu.VMEM((16 + blocks // 16, 256), F32),
            pltpu.SemaphoreType.DMA((7,)),
        ],
        compiler_params=limit(12),
        name="pack",
    )(
        index,
        core,
        *(
            pltpu.with_memory_space_constraint(array, pltpu.HBM)
            for array in (
                query_rows,
                key_rows,
                value_rows,
                jnp.asarray(tables["perm"], BF),
                jnp.asarray(tables["cos"]),
                jnp.asarray(tables["sin"]),
                jnp.asarray(tables["anchors"]),
            )
        ),
    )
    own = lax.all_to_all(send, ("b", "x"), 0, 0, tiled=True)
    following = [(s, (s // GROUP + 1) * GROUP + ((s % GROUP) ^ 4)) for s in range(blocks - GROUP)]
    halo_a = lax.ppermute(jnp.concatenate([own[:, 0:128], own[7:8, 128:256]], axis=0), SP, following)
    halo_b = lax.ppermute(own[:, 128:256], SP, following)
    weight, _ = lax.optimization_barrier((out_weight, own))
    other_weight = lax.ppermute(weight, "tp", [(0, 1), (1, 0)])
    mask1, mask4, mask16 = (jnp.asarray(tables[name]) for name in ("mask1", "mask4", "mask16"))
    state = jax.ShapeDtypeStruct((GROUP, TOK + 8, 128), F32)
    acc, top, qs = pl.pallas_call(
        own_kernel,
        in_specs=[vmem()] * 4,
        out_specs=[vmem()] * 3,
        out_shape=[state, state, jax.ShapeDtypeStruct((GROUP, TOK + 16, 128), BF)],
        scratch_shapes=[
            pltpu.VMEM((GROUP, TOK + 16, 128), BF),
            pltpu.VMEM((GROUP, TOK + 16, 128), BF),
            pltpu.VMEM((16, 128, 128), F32),
            pltpu.VMEM((16, 128, 256), F32),
            pltpu.VMEM((GROUP, TOK, 512), F32),
            pltpu.VMEM((16, 128, 128), BF),
            pltpu.VMEM((16, 128, 256), BF),
            pltpu.VMEM((GROUP, TOK, 512), BF),
        ],
        compiler_params=limit(24),
        cost_estimate=pl.CostEstimate(flops=20 * 10**9, bytes_accessed=2 * 2**20, transcendentals=0),
        name="attend_own",
    )(own, mask1, mask4, mask16)
    scratch = [
        pltpu.VMEM((GROUP + 1, 144, 128), BF),
        pltpu.VMEM((GROUP + 1, 144, 128), BF),
        pltpu.VMEM((GROUP, 136, 128), F32),
        pltpu.VMEM((GROUP, 136, 128), F32),
        pltpu.VMEM((8, 128, 128), F32),
        pltpu.VMEM((2, 128, 128), F32),
        pltpu.VMEM((128, TOK), F32),
        pltpu.VMEM((8, 128, 128), BF),
        pltpu.VMEM((2, 128, 128), BF),
        pltpu.VMEM((128, TOK), BF),
    ]
    lo = pl.pallas_call(
        first_kernel,
        in_specs=[smem] + [vmem()] * 7,
        out_specs=vmem(),
        out_shape=jax.ShapeDtypeStruct((GROUP, 144, 128), BF),
        scratch_shapes=scratch,
        compiler_params=limit(16),
        cost_estimate=pl.CostEstimate(flops=4 * 10**9, bytes_accessed=2 * 2**20, transcendentals=0),
        name="attend_first",
    )(index, acc, top, qs, halo_a, mask1, mask4, mask16)
    back = pl.pallas_call(
        last_kernel,
        in_specs=[smem] + [vmem()] * 10,
        out_specs=vmem(),
        out_shape=jax.ShapeDtypeStruct((2 * GROUP, 64, 128), BF),
        scratch_shapes=scratch,
        compiler_params=limit(16),
        cost_estimate=pl.CostEstimate(flops=4 * 10**9, bytes_accessed=2 * 2**20, transcendentals=0),
        name="attend_last",
    )(index, acc, top, qs, lo, halo_a, halo_b, jnp.asarray(tables["perm"].T, BF), mask1, mask4, mask16)
    back, other_weight = lax.optimization_barrier((back, other_weight))
    rows = lax.all_to_all(back, ("b", "x", "tp"), 0, 0, tiled=True)
    return pl.pallas_call(
        project_kernel,
        in_specs=[smem] * 2 + [vmem()] * 3,
        out_specs=vmem(),
        out_shape=jax.ShapeDtypeStruct((TOK // 2, 2048), BF),
        scratch_shapes=[pltpu.VMEM((2, TOK // 2, 512), BF)],
        compiler_params=limit(16),
        name="project",
    )(index, core, rows, out_weight, other_weight)


def solution(mesh):
    blocks = mesh.shape["sp"]
    fine = Mesh(mesh.devices.reshape(blocks // 16, 2, 2, 4, 2), SP + ("tp",))
    return jax.shard_map(
        functools.partial(per_device, blocks=blocks),
        mesh=fine,
        in_specs=(P(SP, "tp"), P(SP, "tp"), P(SP, "tp"), P("tp", None)),
        out_specs=P(SP + ("tp",), None),
        check_vma=False,
    )
```

```python
import functools
import math

import jax
import jax.numpy as jnp
import numpy as np
from jax import lax
from jax.experimental import pallas as pl
from jax.experimental.pallas import tpu as pltpu
from jax.sharding import Mesh, PartitionSpec as P


HD = 64
BACK = 128
THETA = 500000.0
TOK = 256
GROUP = 8
SP = ("z", "g", "b", "x")
NEG = -1e30
BF = jnp.bfloat16
F32 = jnp.float32


def row_tokens():
    p = np.arange(TOK)
    residue4, a, n = p // 64, (p % 64) // 16, p % 16
    return 16 * n + residue4 + 4 * a


def make_tables(blocks):
    t = row_tokens()
    inverse = np.float64(THETA) ** (-np.arange(32, dtype=np.float64) / 32)
    lanes = inverse[np.arange(128) % 32]
    inner = t[:, None] * lanes[None, :]
    fine = np.arange(16) * TOK
    coarse = np.arange(blocks // 16) * (16 * TOK)
    anchor = np.concatenate([fine, coarse])[:, None] * lanes[None, :]
    anchors = np.concatenate([np.cos(anchor), np.sin(anchor)], axis=1)
    perm = np.zeros((TOK, TOK), np.float32)
    perm[np.arange(TOK), t] = 1.0

    def band(query, key):
        distance = query[:, None] - key[None, :]
        return np.where((distance >= 0) & (distance <= BACK), 0.0, NEG).astype(np.float32)

    mask1 = band(t, np.concatenate([t - TOK, t]))
    row = np.arange(64)
    sub = 4 * (row % 16) + row // 16
    query4 = np.concatenate([sub, sub + 64])
    mask4 = band(query4, np.concatenate([query4 - 128, query4]))
    query16 = np.arange(128)
    mask16 = band(query16, np.concatenate([query16 - 128, query16]))
    return dict(
        cos=np.cos(inner).astype(np.float32),
        sin=np.sin(inner).astype(np.float32),
        anchors=anchors.astype(np.float32),
        perm=perm,
        mask1=mask1,
        mask4=mask4,
        mask16=mask16,
    )


def dot(a, b):
    return lax.dot_general(a, b, (((1,), (0,)), ((), ())), preferred_element_type=F32)


def dot_t(a, b):
    return lax.dot_general(a, b, (((1,), (1,)), ((), ())), preferred_element_type=F32)


def half(rows):
    return lax.broadcasted_iota(jnp.int32, (rows, 128), 1) < 64


def pack_kernel(
    index_ref, core_ref, q_hbm, k_hbm, v_hbm, perm_hbm, cos_hbm, sin_hbm, anchor_hbm, out_hbm, halo_ref,
    q_ref, k_ref, v_ref, perm_ref, cos_ref, sin_ref, anchor_ref, out_ref, sems, out_sems,
):
    pairs = (
        (anchor_hbm, anchor_ref), (cos_hbm, cos_ref), (sin_hbm, sin_ref), (perm_hbm, perm_ref),
        (q_hbm, q_ref), (k_hbm, k_ref), (v_hbm, v_ref),
    )
    copies = [pltpu.make_async_copy(source, target, sems.at[n]) for n, (source, target) in enumerate(pairs)]
    for copy in copies:
        copy.start()
    for copy in copies:
        copy.wait()
    block = index_ref[0]
    fine = anchor_ref[pl.ds(block % 16, 1), :]
    coarse = anchor_ref[pl.ds(16 + block // 16, 1), :]
    cos_a = fine[:, :128] * coarse[:, :128] - fine[:, 128:] * coarse[:, 128:]
    sin_a = fine[:, 128:] * coarse[:, :128] + fine[:, :128] * coarse[:, 128:]
    lane = lax.broadcasted_iota(jnp.int32, (TOK, 128), 1)
    low64 = lane < 64
    low32 = (lane & 63) < 32
    sign = jnp.where(low32[:1], -1.0, 1.0).astype(F32)
    cosine = cos_a * cos_ref[...] - sin_a * sin_ref[...]
    sine = (sin_a * sign) * cos_ref[...] + (cos_a * sign) * sin_ref[...]

    def turn(rows):
        other = jnp.where(low32, pltpu.roll(rows, 96, 1), pltpu.roll(rows, 32, 1))
        return rows * cosine + other * sine

    perm = perm_ref[...]
    outgoing = []
    for j in range(4):
        cols = slice(128 * j, 128 * j + 128)
        query = turn(dot(perm, q_ref[:, cols])) * (1.0 / math.sqrt(HD))
        key = turn(dot(perm, k_ref[:, cols]))
        value = dot(perm, v_ref[:, cols])
        even, odd = 2 * j, 2 * j + 1
        packed = jnp.where(low64, key, pltpu.roll(value, 64, 1)).astype(BF)
        out_ref[even, 0:TOK] = packed
        halo_ref[even] = packed
        packed = jnp.where(low64, pltpu.roll(key, 64, 1), value).astype(BF)
        out_ref[odd, 0:TOK] = packed
        halo_ref[odd] = packed
        first, second = query[:128], query[128:]
        out_ref[even, TOK : TOK + 128] = jnp.where(low64[:128], first, pltpu.roll(second, 64, 1)).astype(BF)
        out_ref[odd, TOK : TOK + 128] = jnp.where(low64[:128], pltpu.roll(first, 64, 1), second).astype(BF)
        copy = pltpu.make_async_copy(out_ref.at[pl.ds(2 * j, 2)], out_hbm.at[pl.ds(2 * j, 2)], out_sems.at[j])
        copy.start()
        outgoing.append(copy)
    for copy in outgoing:
        copy.wait()


def wide(x, n):
    return jnp.concatenate([x] * n, axis=1) if n > 1 else x


def value_masks(rows):
    low = half(rows)
    return jnp.where(low, 1.0, 0.0).astype(BF), jnp.where(low, 0.0, 1.0).astype(BF)


def normal(total):
    return total / pltpu.roll(total, 64, 1)


def start_all(pairs, sems):
    copies = [pltpu.make_async_copy(source, target, sems.at[n]) for n, (source, target) in enumerate(pairs)]
    for copy in copies:
        copy.start()
    return copies


def row_max(scores):
    return jnp.max(scores, axis=1, keepdims=True)


def weights(scores, peak):
    return jnp.exp(scores - wide(peak, scores.shape[1] // 128)).astype(BF)


def own_kernel(
    own_ref, mask1_hbm, mask4_hbm, mask16_hbm, acc_hbm, top_hbm, qs_hbm,
    acc_ref, top_ref, qs_ref, mask1_ref, mask4_ref, mask16_ref, vs, s16, s4, s1, p16, p4, p1, mask_sems, sems,
):
    loads = start_all(((mask16_hbm, mask16_ref), (mask4_hbm, mask4_ref), (mask1_hbm, mask1_ref)), mask_sems)
    low256, high256 = value_masks(TOK)
    low_bf = low256[:128]
    for i in range(GROUP):
        packed = own_ref[i, TOK : TOK + 128]
        qs_ref[i, 0:128] = packed * low_bf
        qs_ref[i, 128:256] = pltpu.roll(packed.astype(F32), 64, 1).astype(BF) * low_bf
        vs[i, 0:TOK] = own_ref[i, 0:TOK] * high256 + low256

    def at4(n):
        b, r = n // 4, n % 4
        seen = slice(max(0, 2 * b - 2), 2 * b + 2)
        return slice(2 * b, 2 * b + 2), slice(64 * r, 64 * r + 64), seen, 64 * (seen.stop - seen.start)

    def at1(i):
        seen = slice(max(0, i - 1), i + 1)
        return seen, TOK * (seen.stop - seen.start)

    for load in loads:
        load.wait()
    for r in range(16):
        rows = slice(16 * r, 16 * r + 16)
        scores = dot_t(qs_ref[:, rows].reshape(128, 128), own_ref[:, rows].reshape(128, 128)) + mask16_ref[:, 128:256]
        s16[r] = scores
        top_ref[:, rows] = jnp.broadcast_to(row_max(scores), (128, 128)).reshape(8, 16, 128)
    for n in range(16):
        at, rows, seen, width = at4(n)
        scores = dot_t(qs_ref[at, rows].reshape(128, 128), own_ref[seen, rows].reshape(width, 128))
        scores = scores + mask4_ref[:, 256 - width : 256]
        s4[n, :, 0:width] = scores
        top_ref[at, rows] = jnp.maximum(top_ref[at, rows].reshape(128, 128), row_max(scores)).reshape(2, 64, 128)
    for i in range(GROUP):
        seen, width = at1(i)
        scores = dot_t(qs_ref[i, 0:TOK], own_ref[seen, 0:TOK].reshape(width, 128)) + mask1_ref[:, 512 - width : 512]
        s1[i, :, 0:width] = scores
        top_ref[i, 0:TOK] = jnp.maximum(top_ref[i, 0:TOK], row_max(scores))
    copies = [
        pltpu.make_async_copy(source, target, sems.at[n])
        for n, (source, target) in enumerate(((qs_ref, qs_hbm), (top_ref, top_hbm), (acc_ref, acc_hbm)))
    ]
    copies[0].start()
    copies[1].start()
    for r in range(16):
        p16[r] = weights(s16[r], top_ref[:, 16 * r : 16 * r + 16].reshape(128, 128))
    for n in range(16):
        at, rows, seen, width = at4(n)
        p4[n, :, 0:width] = weights(s4[n, :, 0:width], top_ref[at, rows].reshape(128, 128))
    for i in range(GROUP):
        seen, width = at1(i)
        p1[i, :, 0:width] = weights(s1[i, :, 0:width], top_ref[i, 0:TOK])
    for r in range(16):
        rows = slice(16 * r, 16 * r + 16)
        acc_ref[:, rows] = dot(p16[r], vs[:, rows].reshape(128, 128)).reshape(8, 16, 128)
    for n in range(16):
        at, rows, seen, width = at4(n)
        acc_ref[at, rows] += dot(p4[n, :, 0:width], vs[seen, rows].reshape(width, 128)).reshape(2, 64, 128)
    for i in range(GROUP):
        seen, width = at1(i)
        acc_ref[i, 0:TOK] += dot(p1[i, :, 0:width], vs[seen, 0:TOK].reshape(width, 128))
    copies[2].start()
    for copy in copies:
        copy.wait()


def halo_kernel(
    index_ref, halo_ref, qs_hbm, top_hbm, mask16_hbm, mask4_hbm, mask1_hbm, acc_hbm, perm_hbm,
    out_ref, qs_ref, top_ref, mask16_ref, mask4_ref, mask1_ref, acc_ref, perm_ref,
    vs, peak, s16, s4, s1, p16, p4, p1, sems,
):
    copies = start_all(
        (
            (qs_hbm, qs_ref), (top_hbm, top_ref), (mask16_hbm, mask16_ref), (mask4_hbm, mask4_ref),
            (mask1_hbm, mask1_ref), (acc_hbm, acc_ref), (perm_hbm, perm_ref),
        ),
        sems,
    )
    bias = jnp.where(index_ref[0] < GROUP, NEG, 0.0).astype(F32)
    low256, high256 = value_masks(TOK)
    for i in range(GROUP):
        vs[i, 0:TOK] = halo_ref[i] * high256 + low256

    def blocks(ref, rows):
        return jnp.concatenate([ref[4:8, rows], ref[0:4, rows]], axis=0).reshape(128, 128)

    def last_two(ref, rows):
        return ref[2:4, rows].reshape(128, 128)

    for copy in copies[:5]:
        copy.wait()
    mask16 = mask16_ref[:, 0:128] + bias
    for r in range(16):
        rows = slice(16 * r, 16 * r + 16)
        scores = dot_t(qs_ref[:, rows].reshape(128, 128), blocks(halo_ref, rows)) + mask16
        s16[r] = scores
        peak[:, rows] = jnp.maximum(top_ref[:, rows].reshape(128, 128), row_max(scores)).reshape(8, 16, 128)
    mask4 = mask4_ref[:, 0:128] + bias
    for r in range(4):
        rows = slice(64 * r, 64 * r + 64)
        scores = dot_t(qs_ref[0:2, rows].reshape(128, 128), last_two(halo_ref, rows)) + mask4
        s4[r] = scores
        peak[0:2, rows] = jnp.maximum(peak[0:2, rows].reshape(128, 128), row_max(scores)).reshape(2, 64, 128)
    scores = dot_t(qs_ref[0, 0:TOK], halo_ref[3]) + (mask1_ref[:, 0:TOK] + bias)
    s1[...] = scores
    peak[0, 0:TOK] = jnp.maximum(peak[0, 0:TOK], row_max(scores))
    for r in range(16):
        p16[r] = weights(s16[r], peak[:, 16 * r : 16 * r + 16].reshape(128, 128))
    for r in range(4):
        p4[r] = weights(s4[r], peak[0:2, 64 * r : 64 * r + 64].reshape(128, 128))
    p1[...] = weights(s1[...], peak[0, 0:TOK])
    copies[5].wait()
    copies[6].wait()
    for i in range(GROUP):
        peak[i, 0:TOK] = acc_ref[i, 0:TOK] * jnp.exp(top_ref[i, 0:TOK] - peak[i, 0:TOK])
    new = peak
    for r in range(16):
        rows = slice(16 * r, 16 * r + 16)
        new[:, rows] += dot(p16[r], blocks(vs, rows)).reshape(8, 16, 128)
    for r in range(4):
        rows = slice(64 * r, 64 * r + 64)
        new[0:2, rows] += dot(p4[r], last_two(vs, rows)).reshape(2, 64, 128)
    new[0, 0:TOK] += dot(p1[...], vs[3, 0:TOK])
    low_rows = half(64)
    for i in range(GROUP):
        mixed = normal(new[i, 0:TOK]).astype(BF) * high256
        natural = dot(perm_ref[...], mixed)
        out_ref[2 * i] = jnp.where(low_rows, pltpu.roll(natural[0:64], 64, 1), natural[64:128]).astype(BF)
        out_ref[2 * i + 1] = jnp.where(low_rows, pltpu.roll(natural[128:192], 64, 1), natural[192:256]).astype(BF)


def project_kernel(core_ref, rows_ref, own_ref, other_ref, out_ref, mixed):
    low = half(64)
    for side in range(2):
        core = core_ref[0] if side == 0 else 1 - core_ref[0]
        for j in range(4):
            first = rows_ref[4 * j + core].astype(F32)
            second = rows_ref[4 * j + 2 + core].astype(F32)
            cols = slice(128 * j, 128 * j + 128)
            mixed[side, 0:64, cols] = jnp.where(low, first, pltpu.roll(second, 64, 1)).astype(BF)
            mixed[side, 64:128, cols] = jnp.where(low, pltpu.roll(first, 64, 1), second).astype(BF)
    for n in range(4):
        cols = slice(512 * n, 512 * n + 512)
        out_ref[:, cols] = (dot(mixed[0], own_ref[:, cols]) + dot(mixed[1], other_ref[:, cols])).astype(BF)


def vmem():
    return pl.BlockSpec(memory_space=pltpu.VMEM)


def limit(mib):
    return pltpu.CompilerParams(vmem_limit_bytes=mib * 2**20)


def per_device(query_rows, key_rows, value_rows, out_weight, blocks):
    tables = make_tables(blocks)
    index = lax.axis_index(SP).astype(jnp.int32).reshape(1)
    core = lax.axis_index("tp").astype(jnp.int32).reshape(1)

    smem = pl.BlockSpec(memory_space=pltpu.SMEM)
    hbm = pl.BlockSpec(memory_space=pltpu.HBM)
    send, keys_values = pl.pallas_call(
        pack_kernel,
        in_specs=[smem] * 2 + [hbm] * 7,
        out_specs=[hbm, vmem()],
        out_shape=[
            pltpu.HBM((GROUP, TOK + 128, 128), BF),
            jax.ShapeDtypeStruct((GROUP, TOK, 128), BF),
        ],
        scratch_shapes=[
            pltpu.VMEM((TOK, 512), BF),
            pltpu.VMEM((TOK, 512), BF),
            pltpu.VMEM((TOK, 512), BF),
            pltpu.VMEM((TOK, TOK), BF),
            pltpu.VMEM((TOK, 128), F32),
            pltpu.VMEM((TOK, 128), F32),
            pltpu.VMEM((16 + blocks // 16, 256), F32),
            pltpu.VMEM((GROUP, TOK + 128, 128), BF),
            pltpu.SemaphoreType.DMA((7,)),
            pltpu.SemaphoreType.DMA((4,)),
        ],
        compiler_params=limit(12),
        name="pack",
    )(
        index,
        core,
        *(
            pltpu.with_memory_space_constraint(array, pltpu.HBM)
            for array in (
                query_rows,
                key_rows,
                value_rows,
                jnp.asarray(tables["perm"], BF),
                jnp.asarray(tables["cos"]),
                jnp.asarray(tables["sin"]),
                jnp.asarray(tables["anchors"]),
            )
        ),
    )
    following = [(s, (s // GROUP + 1) * GROUP + ((s % GROUP) ^ 4)) for s in range(blocks - GROUP)]
    shifted = lax.ppermute(keys_values, SP, following)
    own = lax.all_to_all(send, ("b", "x"), 0, 0, tiled=True)
    shifted, _ = lax.optimization_barrier((shifted, own))
    halo = lax.all_to_all(shifted, ("b", "x"), 0, 0, tiled=True)
    weight, _ = lax.optimization_barrier((out_weight, keys_values))
    other_weight = lax.ppermute(weight, "tp", [(0, 1), (1, 0)])
    mask1, mask4, mask16 = (jnp.asarray(tables[name]) for name in ("mask1", "mask4", "mask16"))
    mask1, mask4, mask16 = (pltpu.with_memory_space_constraint(x, pltpu.HBM) for x in (mask1, mask4, mask16))
    acc, top, qs = pl.pallas_call(
        own_kernel,
        in_specs=[vmem()] + [hbm] * 3,
        out_specs=[hbm] * 3,
        out_shape=[
            pltpu.HBM((GROUP, TOK + 8, 128), F32),
            pltpu.HBM((GROUP, TOK + 8, 128), F32),
            pltpu.HBM((GROUP, TOK + 16, 128), BF),
        ],
        scratch_shapes=[
            pltpu.VMEM((GROUP, TOK + 8, 128), F32),
            pltpu.VMEM((GROUP, TOK + 8, 128), F32),
            pltpu.VMEM((GROUP, TOK + 16, 128), BF),
            pltpu.VMEM((TOK, 2 * TOK), F32),
            pltpu.VMEM((128, 256), F32),
            pltpu.VMEM((128, 256), F32),
            pltpu.VMEM((GROUP, TOK + 16, 128), BF),
            pltpu.VMEM((16, 128, 128), F32),
            pltpu.VMEM((16, 128, 256), F32),
            pltpu.VMEM((GROUP, TOK, 512), F32),
            pltpu.VMEM((16, 128, 128), BF),
            pltpu.VMEM((16, 128, 256), BF),
            pltpu.VMEM((GROUP, TOK, 512), BF),
            pltpu.SemaphoreType.DMA((3,)),
            pltpu.SemaphoreType.DMA((3,)),
        ],
        compiler_params=limit(24),
        cost_estimate=pl.CostEstimate(flops=20 * 10**9, bytes_accessed=2 * 2**20, transcendentals=0),
        name="attend_own",
    )(own, mask1, mask4, mask16)
    back = pl.pallas_call(
        halo_kernel,
        in_specs=[smem, vmem()] + [hbm] * 7,
        out_specs=vmem(),
        out_shape=jax.ShapeDtypeStruct((2 * GROUP, 64, 128), BF),
        scratch_shapes=[
            pltpu.VMEM((GROUP, TOK + 16, 128), BF),
            pltpu.VMEM((GROUP, TOK + 8, 128), F32),
            pltpu.VMEM((128, 256), F32),
            pltpu.VMEM((128, 256), F32),
            pltpu.VMEM((TOK, 2 * TOK), F32),
            pltpu.VMEM((GROUP, TOK + 8, 128), F32),
            pltpu.VMEM((TOK, TOK), BF),
            pltpu.VMEM((GROUP, TOK + 16, 128), BF),
            pltpu.VMEM((GROUP, TOK + 8, 128), F32),
            pltpu.VMEM((16, 128, 128), F32),
            pltpu.VMEM((4, 128, 128), F32),
            pltpu.VMEM((TOK, TOK), F32),
            pltpu.VMEM((16, 128, 128), BF),
            pltpu.VMEM((4, 128, 128), BF),
            pltpu.VMEM((TOK, TOK), BF),
            pltpu.SemaphoreType.DMA((7,)),
        ],
        compiler_params=limit(16),
        cost_estimate=pl.CostEstimate(flops=4 * 10**9, bytes_accessed=2 * 2**20, transcendentals=0),
        name="attend_halo",
    )(
        index,
        halo,
        *(
            pltpu.with_memory_space_constraint(x, pltpu.HBM)
            for x in (qs, top, mask16, mask4, mask1, acc, jnp.asarray(tables["perm"].T, BF))
        ),
    )
    back, other_weight = lax.optimization_barrier((back, other_weight))
    rows = lax.all_to_all(back, ("b", "x", "tp"), 0, 0, tiled=True)
    return pl.pallas_call(
        project_kernel,
        in_specs=[smem] + [vmem()] * 3,
        out_specs=vmem(),
        out_shape=jax.ShapeDtypeStruct((TOK // 2, 2048), BF),
        scratch_shapes=[pltpu.VMEM((2, TOK // 2, 512), BF)],
        compiler_params=limit(16),
        name="project",
    )(core, rows, out_weight, other_weight)


def solution(mesh):
    blocks = mesh.shape["sp"]
    fine = Mesh(mesh.devices.reshape(blocks // 16, 2, 2, 4, 2), SP + ("tp",))
    return jax.shard_map(
        functools.partial(per_device, blocks=blocks),
        mesh=fine,
        in_specs=(P(SP, "tp"), P(SP, "tp"), P(SP, "tp"), P("tp", None)),
        out_specs=P(SP + ("tp",), None),
        check_vma=False,
    )
```

```python
import functools
import math

import jax
import jax.numpy as jnp
import numpy as np
from jax import lax
from jax.experimental import pallas as pl
from jax.experimental.pallas import tpu as pltpu
from jax.sharding import Mesh, PartitionSpec as P


HD = 64
BACK = 128
THETA = 500000.0
TOK = 256
GROUP = 8
SP = ("z", "g", "b", "x")
NEG = -1e30
FIRST = 192
BF = jnp.bfloat16
F32 = jnp.float32


def row_tokens():
    p = np.arange(TOK)
    residue4, a, n = p // 64, (p % 64) // 16, p % 16
    return 16 * n + residue4 + 4 * a


def make_tables(blocks):
    t = row_tokens()
    inverse = np.float64(THETA) ** (-np.arange(32, dtype=np.float64) / 32)
    lanes = inverse[np.arange(128) % 32]
    inner = t[:, None] * lanes[None, :]
    fine = np.arange(16) * TOK
    coarse = np.arange(blocks // 16) * (16 * TOK)
    anchor = np.concatenate([fine, coarse])[:, None] * lanes[None, :]
    anchors = np.concatenate([np.cos(anchor), np.sin(anchor)], axis=1)
    perm = np.zeros((TOK, TOK), np.float32)
    perm[np.arange(TOK), t] = 1.0

    def band(query, key):
        distance = query[:, None] - key[None, :]
        return np.where((distance >= 0) & (distance <= BACK), 0.0, NEG).astype(np.float32)

    mask1 = band(t, np.concatenate([t - TOK, t]))
    row = np.arange(64)
    sub = 4 * (row % 16) + row // 16
    query4 = np.concatenate([sub, sub + 64])
    mask4 = band(query4, np.concatenate([query4 - 128, query4]))
    query16 = np.arange(128)
    mask16 = band(query16, np.concatenate([query16 - 128, query16]))
    return dict(
        cos=np.cos(inner).astype(np.float32),
        sin=np.sin(inner).astype(np.float32),
        anchors=anchors.astype(np.float32),
        perm=perm,
        mask1=mask1,
        mask4=mask4,
        mask16=mask16,
    )


def dot(a, b):
    return lax.dot_general(a, b, (((1,), (0,)), ((), ())), preferred_element_type=F32)


def dot_t(a, b):
    return lax.dot_general(a, b, (((1,), (1,)), ((), ())), preferred_element_type=F32)


def half(rows):
    return lax.broadcasted_iota(jnp.int32, (rows, 128), 1) < 64


def pack_kernel(
    index_ref, core_ref, q_hbm, k_hbm, v_hbm, perm_hbm, cos_hbm, sin_hbm, anchor_hbm, out_ref,
    q_ref, k_ref, v_ref, perm_ref, cos_ref, sin_ref, anchor_ref, sems,
):
    pairs = (
        (perm_hbm, perm_ref), (k_hbm, k_ref), (anchor_hbm, anchor_ref), (cos_hbm, cos_ref), (sin_hbm, sin_ref),
        (v_hbm, v_ref), (q_hbm, q_ref),
    )
    copies = [pltpu.make_async_copy(source, target, sems.at[n]) for n, (source, target) in enumerate(pairs)]
    for copy in copies:
        copy.start()
    for copy in copies[2:5]:
        copy.wait()
    block = index_ref[0]
    flip = 4 * ((block // GROUP) % 2)
    fine = anchor_ref[pl.ds(block % 16, 1), :]
    coarse = anchor_ref[pl.ds(16 + block // 16, 1), :]
    cos_a = fine[:, :128] * coarse[:, :128] - fine[:, 128:] * coarse[:, 128:]
    sin_a = fine[:, 128:] * coarse[:, :128] + fine[:, :128] * coarse[:, 128:]
    lane = lax.broadcasted_iota(jnp.int32, (TOK, 128), 1)
    low64 = lane < 64
    low32 = (lane & 63) < 32
    sign = jnp.where(low32[:1], -1.0, 1.0).astype(F32)
    cosine = cos_a * cos_ref[...] - sin_a * sin_ref[...]
    sine = (sin_a * sign) * cos_ref[...] + (cos_a * sign) * sin_ref[...]

    def turn(rows):
        other = jnp.where(low32, pltpu.roll(rows, 96, 1), pltpu.roll(rows, 32, 1))
        return rows * cosine + other * sine

    copies[0].wait()
    copies[1].wait()
    perm = perm_ref[...]
    keys = [turn(dot(perm, k_ref[:, 128 * j : 128 * j + 128])) for j in range(4)]
    copies[5].wait()
    for j in range(4):
        key = keys[j]
        value = dot(perm, v_ref[:, 128 * j : 128 * j + 128])
        even = (2 * j) ^ flip
        odd = even + 1
        out_ref[even, 0:TOK] = jnp.where(low64, key, pltpu.roll(value, 64, 1)).astype(BF)
        out_ref[odd, 0:TOK] = jnp.where(low64, pltpu.roll(key, 64, 1), value).astype(BF)
    copies[6].wait()
    for j in range(4):
        query = turn(dot(perm, q_ref[:, 128 * j : 128 * j + 128])) * (1.0 / math.sqrt(HD))
        even = (2 * j) ^ flip
        odd = even + 1
        first, second = query[:128], query[128:]
        out_ref[even, TOK : TOK + 128] = jnp.where(low64[:128], first, pltpu.roll(second, 64, 1)).astype(BF)
        out_ref[odd, TOK : TOK + 128] = jnp.where(low64[:128], pltpu.roll(first, 64, 1), second).astype(BF)


def wide(x, n):
    return jnp.concatenate([x] * n, axis=1) if n > 1 else x


def value_masks(rows):
    low = half(rows)
    return jnp.where(low, 1.0, 0.0).astype(BF), jnp.where(low, 0.0, 1.0).astype(BF)


def normal(total):
    return total / pltpu.roll(total, 64, 1)


def row_max(scores):
    return jnp.max(scores, axis=1, keepdims=True)


def weights(scores, peak):
    return jnp.exp(scores - wide(peak, scores.shape[1] // 128)).astype(BF)


def own_kernel(own_ref, mask1_ref, mask4_ref, mask16_ref, acc_ref, top_ref, qs_ref, vs, s16, s4, s1, p16, p4, p1):
    low256, high256 = value_masks(TOK)
    low_bf = low256[:128]
    for i in range(GROUP):
        packed = own_ref[i, TOK : TOK + 128]
        qs_ref[i, 0:128] = packed * low_bf
        qs_ref[i, 128:256] = pltpu.roll(packed.astype(F32), 64, 1).astype(BF) * low_bf
        vs[i, 0:TOK] = own_ref[i, 0:TOK] * high256 + low256

    def at4(n):
        b, r = n // 4, n % 4
        seen = slice(max(0, 2 * b - 2), 2 * b + 2)
        return slice(2 * b, 2 * b + 2), slice(64 * r, 64 * r + 64), seen, 64 * (seen.stop - seen.start)

    def at1(i):
        seen = slice(max(0, i - 1), i + 1)
        return seen, TOK * (seen.stop - seen.start)

    for r in range(16):
        rows = slice(16 * r, 16 * r + 16)
        scores = dot_t(qs_ref[:, rows].reshape(128, 128), own_ref[:, rows].reshape(128, 128)) + mask16_ref[:, 128:256]
        s16[r] = scores
        top_ref[:, rows] = jnp.broadcast_to(row_max(scores), (128, 128)).reshape(8, 16, 128)
    for n in range(16):
        at, rows, seen, width = at4(n)
        scores = dot_t(qs_ref[at, rows].reshape(128, 128), own_ref[seen, rows].reshape(width, 128))
        scores = scores + mask4_ref[:, 256 - width : 256]
        s4[n, :, 0:width] = scores
        top_ref[at, rows] = jnp.maximum(top_ref[at, rows].reshape(128, 128), row_max(scores)).reshape(2, 64, 128)
    for i in range(GROUP):
        seen, width = at1(i)
        scores = dot_t(qs_ref[i, 0:TOK], own_ref[seen, 0:TOK].reshape(width, 128)) + mask1_ref[:, 512 - width : 512]
        s1[i, :, 0:width] = scores
        top_ref[i, 0:TOK] = jnp.maximum(top_ref[i, 0:TOK], row_max(scores))
    for r in range(16):
        p16[r] = weights(s16[r], top_ref[:, 16 * r : 16 * r + 16].reshape(128, 128))
    for n in range(16):
        at, rows, seen, width = at4(n)
        p4[n, :, 0:width] = weights(s4[n, :, 0:width], top_ref[at, rows].reshape(128, 128))
    for i in range(GROUP):
        seen, width = at1(i)
        p1[i, :, 0:width] = weights(s1[i, :, 0:width], top_ref[i, 0:TOK])
    for r in range(16):
        rows = slice(16 * r, 16 * r + 16)
        acc_ref[:, rows] = dot(p16[r], vs[:, rows].reshape(128, 128)).reshape(8, 16, 128)
    for n in range(16):
        at, rows, seen, width = at4(n)
        acc_ref[at, rows] += dot(p4[n, :, 0:width], vs[seen, rows].reshape(width, 128)).reshape(2, 64, 128)
    for i in range(GROUP):
        seen, width = at1(i)
        acc_ref[i, 0:TOK] += dot(p1[i, :, 0:width], vs[seen, 0:TOK].reshape(width, 128))


def gather(ref, count, start, n, blocks):
    return jnp.concatenate([ref[count * i + start : count * i + start + n] for i in blocks], axis=0)


def halo_rows(index_ref, acc_ref, top_ref, qs_ref, masks, base, count, ks, vs, near, near_values, scratch):
    mask1_ref, mask4_ref, mask16_ref = masks
    new, peak, s16, s4, s1, p16, p4, p1 = scratch
    bias = jnp.where(index_ref[0] < GROUP, NEG, 0.0).astype(F32)
    span = slice(base, base + count)
    every, last_two = range(GROUP), (6, 7)

    mask16 = mask16_ref[:, 0:128] + bias
    for r in range(count // 16):
        rows = slice(16 * r, 16 * r + 16)
        full = slice(base + 16 * r, base + 16 * r + 16)
        scores = dot_t(qs_ref[:, full].reshape(128, 128), gather(ks, count, 16 * r, 16, every)) + mask16
        s16[r] = scores
        peak[:, rows] = jnp.maximum(top_ref[:, full].reshape(128, 128), row_max(scores)).reshape(8, 16, 128)
    mask4 = mask4_ref[:, 0:128] + bias
    for r in range(count // 64):
        rows = slice(64 * r, 64 * r + 64)
        full = slice(base + 64 * r, base + 64 * r + 64)
        scores = dot_t(qs_ref[0:2, full].reshape(128, 128), gather(ks, count, 64 * r, 64, last_two)) + mask4
        s4[r] = scores
        peak[0:2, rows] = jnp.maximum(peak[0:2, rows].reshape(128, 128), row_max(scores)).reshape(2, 64, 128)
    scores = dot_t(qs_ref[0, span], near) + (mask1_ref[span, 0:TOK] + bias)
    s1[...] = scores
    peak[0, 0:count] = jnp.maximum(peak[0, 0:count], row_max(scores))
    for r in range(count // 16):
        p16[r] = weights(s16[r], peak[:, 16 * r : 16 * r + 16].reshape(128, 128))
    for r in range(count // 64):
        p4[r] = weights(s4[r], peak[0:2, 64 * r : 64 * r + 64].reshape(128, 128))
    p1[...] = weights(s1[...], peak[0, 0:count])
    for i in range(GROUP):
        new[i, 0:count] = acc_ref[i, span] * jnp.exp(top_ref[i, span] - peak[i, 0:count])
    for r in range(count // 16):
        rows = slice(16 * r, 16 * r + 16)
        new[:, rows] += dot(p16[r], gather(vs, count, 16 * r, 16, every)).reshape(8, 16, 128)
    for r in range(count // 64):
        rows = slice(64 * r, 64 * r + 64)
        new[0:2, rows] += dot(p4[r], gather(vs, count, 64 * r, 64, last_two)).reshape(2, 64, 128)
    new[0, 0:count] += dot(p1[...], near_values)


def with_ones(keys_values):
    low, high = value_masks(keys_values.shape[0])
    return keys_values * high + low


def first_kernel(index_ref, acc_ref, top_ref, qs_ref, halo_ref, mask1_ref, mask4_ref, mask16_ref, lo_ref, vs, *scratch):
    for n in range(0, GROUP * FIRST + TOK - FIRST, 64):
        vs[n : n + 64] = with_ones(halo_ref[n : n + 64])
    near = slice(7 * FIRST, 7 * FIRST + TOK)
    halo_rows(
        index_ref, acc_ref, top_ref, qs_ref, (mask1_ref, mask4_ref, mask16_ref), 0, FIRST,
        halo_ref, vs, halo_ref[near], vs[near], scratch,
    )
    new = scratch[0]
    _, high = value_masks(FIRST)
    for i in range(GROUP):
        lo_ref[i] = normal(new[i, 0:FIRST]).astype(BF) * high


def last_kernel(
    index_ref, acc_ref, top_ref, qs_ref, lo_ref, before_ref, halo_ref, perm_ref, mask1_ref, mask4_ref, mask16_ref,
    out_ref, vs, *scratch,
):
    count = TOK - FIRST
    for n in range(0, GROUP * count, 64):
        vs[n : n + 64] = with_ones(halo_ref[n : n + 64])
    near = before_ref[7 * FIRST : 7 * FIRST + TOK]
    halo_rows(
        index_ref, acc_ref, top_ref, qs_ref, (mask1_ref, mask4_ref, mask16_ref), FIRST, count,
        halo_ref, vs, near, with_ones(near), scratch,
    )
    new = scratch[0]
    _, high = value_masks(count)
    low_rows = half(64)
    for i in range(GROUP):
        mixed = jnp.concatenate([lo_ref[i], normal(new[i, 0:count]).astype(BF) * high], axis=0)
        natural = dot(perm_ref[...], mixed)
        out_ref[2 * i] = jnp.where(low_rows, pltpu.roll(natural[0:64], 64, 1), natural[64:128]).astype(BF)
        out_ref[2 * i + 1] = jnp.where(low_rows, pltpu.roll(natural[128:192], 64, 1), natural[192:256]).astype(BF)


def project_kernel(index_ref, core_ref, rows_ref, own_ref, other_ref, out_hbm, mixed, out_ref, sems):
    low = half(64)
    flip = 4 * ((index_ref[0] // GROUP) % 2)
    for side in range(2):
        core = core_ref[0] if side == 0 else 1 - core_ref[0]
        for j in range(4):
            first = rows_ref[2 * ((2 * j) ^ flip) + core].astype(F32)
            second = rows_ref[2 * ((2 * j) ^ flip) + 2 + core].astype(F32)
            cols = slice(128 * j, 128 * j + 128)
            mixed[side, 0:64, cols] = jnp.where(low, first, pltpu.roll(second, 64, 1)).astype(BF)
            mixed[side, 64:128, cols] = jnp.where(low, pltpu.roll(first, 64, 1), second).astype(BF)
    copies = []
    for n in range(4):
        cols = slice(512 * n, 512 * n + 512)
        out_ref[:, cols] = (dot(mixed[0], own_ref[:, cols]) + dot(mixed[1], other_ref[:, cols])).astype(BF)
        copy = pltpu.make_async_copy(out_ref.at[:, cols], out_hbm.at[:, cols], sems.at[n])
        copy.start()
        copies.append(copy)
    for copy in copies:
        copy.wait()


def vmem():
    return pl.BlockSpec(memory_space=pltpu.VMEM)


def limit(mib):
    return pltpu.CompilerParams(vmem_limit_bytes=mib * 2**20)


def per_device(query_rows, key_rows, value_rows, out_weight, blocks):
    tables = make_tables(blocks)
    index = lax.axis_index(SP).astype(jnp.int32).reshape(1)
    core = lax.axis_index("tp").astype(jnp.int32).reshape(1)

    smem = pl.BlockSpec(memory_space=pltpu.SMEM)
    hbm = pl.BlockSpec(memory_space=pltpu.HBM)
    send = pl.pallas_call(
        pack_kernel,
        in_specs=[smem] * 2 + [hbm] * 7,
        out_specs=vmem(),
        out_shape=jax.ShapeDtypeStruct((GROUP, TOK + 128, 128), BF),
        scratch_shapes=[
            pltpu.VMEM((TOK, 512), BF),
            pltpu.VMEM((TOK, 512), BF),
            pltpu.VMEM((TOK, 512), BF),
            pltpu.VMEM((TOK, TOK), BF),
            pltpu.VMEM((TOK, 128), F32),
            pltpu.VMEM((TOK, 128), F32),
            pltpu.VMEM((16 + blocks // 16, 256), F32),
            pltpu.SemaphoreType.DMA((7,)),
        ],
        compiler_params=limit(12),
        name="pack",
    )(
        index,
        core,
        *(
            pltpu.with_memory_space_constraint(array, pltpu.HBM)
            for array in (
                query_rows,
                key_rows,
                value_rows,
                jnp.asarray(tables["perm"], BF),
                jnp.asarray(tables["cos"]),
                jnp.asarray(tables["sin"]),
                jnp.asarray(tables["anchors"]),
            )
        ),
    )
    own = lax.all_to_all(send, ("b", "x"), 0, 0, tiled=True)
    following = [(s, (s // GROUP + 1) * GROUP + ((s % GROUP) ^ 4)) for s in range(blocks - GROUP)]
    early = jnp.concatenate([own[:, 0:FIRST].reshape(GROUP * FIRST, 128), own[7, FIRST:TOK]], axis=0)
    halo_a = lax.ppermute(early, SP, following)
    halo_b = lax.ppermute(own[:, FIRST:TOK].reshape(GROUP * (TOK - FIRST), 128), SP, following)
    weight, _ = lax.optimization_barrier((out_weight, own))
    other_weight = lax.ppermute(weight, "tp", [(0, 1), (1, 0)])
    mask1, mask4, mask16 = (jnp.asarray(tables[name]) for name in ("mask1", "mask4", "mask16"))
    state = jax.ShapeDtypeStruct((GROUP, TOK + 8, 128), F32)
    acc, top, qs = pl.pallas_call(
        own_kernel,
        in_specs=[vmem()] * 4,
        out_specs=[vmem()] * 3,
        out_shape=[state, state, jax.ShapeDtypeStruct((GROUP, TOK + 16, 128), BF)],
        scratch_shapes=[
            pltpu.VMEM((GROUP, TOK + 16, 128), BF),
            pltpu.VMEM((16, 128, 128), F32),
            pltpu.VMEM((16, 128, 256), F32),
            pltpu.VMEM((GROUP, TOK, 512), F32),
            pltpu.VMEM((16, 128, 128), BF),
            pltpu.VMEM((16, 128, 256), BF),
            pltpu.VMEM((GROUP, TOK, 512), BF),
        ],
        compiler_params=limit(24),
        cost_estimate=pl.CostEstimate(flops=20 * 10**9, bytes_accessed=2 * 2**20, transcendentals=0),
        name="attend_own",
    )(own, mask1, mask4, mask16)

    def scratch(total, count):
        return [
            pltpu.VMEM((total, 128), BF),
            pltpu.VMEM((GROUP, count + 8, 128), F32),
            pltpu.VMEM((GROUP, count + 8, 128), F32),
            pltpu.VMEM((count // 16, 128, 128), F32),
            pltpu.VMEM((count // 64, 128, 128), F32),
            pltpu.VMEM((count, TOK), F32),
            pltpu.VMEM((count // 16, 128, 128), BF),
            pltpu.VMEM((count // 64, 128, 128), BF),
            pltpu.VMEM((count, TOK), BF),
        ]

    lo = pl.pallas_call(
        first_kernel,
        in_specs=[smem] + [vmem()] * 7,
        out_specs=vmem(),
        out_shape=jax.ShapeDtypeStruct((GROUP, FIRST, 128), BF),
        scratch_shapes=scratch(GROUP * FIRST + TOK - FIRST, FIRST),
        compiler_params=limit(16),
        cost_estimate=pl.CostEstimate(flops=4 * 10**9, bytes_accessed=2 * 2**20, transcendentals=0),
        name="attend_first",
    )(index, acc, top, qs, halo_a, mask1, mask4, mask16)
    back = pl.pallas_call(
        last_kernel,
        in_specs=[smem] + [vmem()] * 10,
        out_specs=vmem(),
        out_shape=jax.ShapeDtypeStruct((2 * GROUP, 64, 128), BF),
        scratch_shapes=scratch(GROUP * (TOK - FIRST), TOK - FIRST),
        compiler_params=limit(16),
        cost_estimate=pl.CostEstimate(flops=4 * 10**9, bytes_accessed=2 * 2**20, transcendentals=0),
        name="attend_last",
    )(index, acc, top, qs, lo, halo_a, halo_b, jnp.asarray(tables["perm"].T, BF), mask1, mask4, mask16)
    back, other_weight = lax.optimization_barrier((back, other_weight))
    rows = lax.all_to_all(back, ("b", "x", "tp"), 0, 0, tiled=True)
    return pl.pallas_call(
        project_kernel,
        in_specs=[smem] * 2 + [vmem()] * 3,
        out_specs=hbm,
        out_shape=pltpu.HBM((TOK // 2, 2048), BF),
        scratch_shapes=[
            pltpu.VMEM((2, TOK // 2, 512), BF),
            pltpu.VMEM((TOK // 2, 2048), BF),
            pltpu.SemaphoreType.DMA((4,)),
        ],
        compiler_params=limit(16),
        name="project",
    )(index, core, rows, out_weight, other_weight)


def solution(mesh):
    blocks = mesh.shape["sp"]
    fine = Mesh(mesh.devices.reshape(blocks // 16, 2, 2, 4, 2), SP + ("tp",))
    return jax.shard_map(
        functools.partial(per_device, blocks=blocks),
        mesh=fine,
        in_specs=(P(SP, "tp"), P(SP, "tp"), P(SP, "tp"), P("tp", None)),
        out_specs=P(SP + ("tp",), None),
        check_vma=False,
    )
```

```python
import functools
import math

import jax
import jax.numpy as jnp
import numpy as np
from jax import lax
from jax.experimental import pallas as pl
from jax.experimental.pallas import tpu as pltpu
from jax.sharding import Mesh, PartitionSpec as P


HD = 64
BACK = 128
THETA = 500000.0
TOK = 256
GROUP = 8
SP = ("z", "g", "b", "x")
NEG = -1e30
BF = jnp.bfloat16
F32 = jnp.float32


def row_tokens():
    p = np.arange(TOK)
    residue4, a, n = p // 64, (p % 64) // 16, p % 16
    return 16 * n + residue4 + 4 * a


def make_tables(blocks):
    t = row_tokens()
    inverse = np.float64(THETA) ** (-np.arange(32, dtype=np.float64) / 32)
    lanes = inverse[np.arange(128) % 32]
    inner = t[:, None] * lanes[None, :]
    fine = np.arange(16) * TOK
    coarse = np.arange(blocks // 16) * (16 * TOK)
    anchor = np.concatenate([fine, coarse])[:, None] * lanes[None, :]
    anchors = np.concatenate([np.cos(anchor), np.sin(anchor)], axis=1)
    perm = np.zeros((TOK, TOK), np.float32)
    perm[np.arange(TOK), t] = 1.0

    def band(query, key):
        distance = query[:, None] - key[None, :]
        return np.where((distance >= 0) & (distance <= BACK), 0.0, NEG).astype(np.float32)

    mask1 = band(t, np.concatenate([t - TOK, t]))
    row = np.arange(64)
    sub = 4 * (row % 16) + row // 16
    query4 = np.concatenate([sub, sub + 64])
    mask4 = band(query4, np.concatenate([query4 - 128, query4]))
    query16 = np.arange(128)
    mask16 = band(query16, np.concatenate([query16 - 128, query16]))
    return dict(
        cos=np.cos(inner).astype(np.float32),
        sin=np.sin(inner).astype(np.float32),
        anchors=anchors.astype(np.float32),
        perm=perm,
        masks=np.concatenate([mask1, np.concatenate([mask4, mask16], axis=0)], axis=1),
    )


def dot(a, b):
    return lax.dot_general(a, b, (((1,), (0,)), ((), ())), preferred_element_type=F32)


def dot_t(a, b):
    return lax.dot_general(a, b, (((1,), (1,)), ((), ())), preferred_element_type=F32)


def half(rows):
    return lax.broadcasted_iota(jnp.int32, (rows, 128), 1) < 64


def pack_kernel(
    index_ref, core_ref, q_hbm, k_hbm, v_hbm, perm_hbm, cos_hbm, sin_hbm, anchor_hbm, kv_ref, packed_ref,
    q_ref, k_ref, v_ref, perm_ref, cos_ref, sin_ref, anchor_ref, sems,
):
    pairs = (
        (anchor_hbm, anchor_ref), (cos_hbm, cos_ref), (sin_hbm, sin_ref), (perm_hbm, perm_ref),
        (k_hbm, k_ref), (v_hbm, v_ref), (q_hbm, q_ref),
    )
    copies = [pltpu.make_async_copy(source, target, sems.at[n]) for n, (source, target) in enumerate(pairs)]
    for copy in copies:
        copy.start()
    for copy in copies:
        copy.wait()
    block = index_ref[0]
    flip = 4 * ((block // GROUP) % 2)
    fine = anchor_ref[pl.ds(block % 16, 1), :]
    coarse = anchor_ref[pl.ds(16 + block // 16, 1), :]
    cos_a = fine[:, :128] * coarse[:, :128] - fine[:, 128:] * coarse[:, 128:]
    sin_a = fine[:, 128:] * coarse[:, :128] + fine[:, :128] * coarse[:, 128:]
    lane = lax.broadcasted_iota(jnp.int32, (TOK, 128), 1)
    low64 = lane < 64
    low32 = (lane & 63) < 32
    sign = jnp.where(low32[:1], -1.0, 1.0).astype(F32)
    cosine = cos_a * cos_ref[...] - sin_a * sin_ref[...]
    sine = (sin_a * sign) * cos_ref[...] + (cos_a * sign) * sin_ref[...]

    def turn(rows):
        other = jnp.where(low32, pltpu.roll(rows, 96, 1), pltpu.roll(rows, 32, 1))
        return rows * cosine + other * sine

    perm = perm_ref[...]
    for j in range(4):
        cols = slice(128 * j, 128 * j + 128)
        query = turn(dot(perm, q_ref[:, cols])) * (1.0 / math.sqrt(HD))
        key = turn(dot(perm, k_ref[:, cols]))
        value = dot(perm, v_ref[:, cols])
        even = (2 * j) ^ flip
        odd = even + 1
        kv_ref[even] = jnp.where(low64, key, pltpu.roll(value, 64, 1)).astype(BF)
        kv_ref[odd] = jnp.where(low64, pltpu.roll(key, 64, 1), value).astype(BF)
        first, second = query[:128], query[128:]
        packed_ref[even] = jnp.where(low64[:128], first, pltpu.roll(second, 64, 1)).astype(BF)
        packed_ref[odd] = jnp.where(low64[:128], pltpu.roll(first, 64, 1), second).astype(BF)


def wide(x, n):
    return jnp.concatenate([x] * n, axis=1) if n > 1 else x


def value_masks(rows):
    low = half(rows)
    return jnp.where(low, 1.0, 0.0).astype(BF), jnp.where(low, 0.0, 1.0).astype(BF)


def normal(total):
    return total / pltpu.roll(total, 64, 1)


def row_max(scores):
    return jnp.max(scores, axis=1, keepdims=True)


def weights(scores, peak):
    return jnp.exp(scores - wide(peak, scores.shape[1] // 128)).astype(BF)


def own_kernel(own_ref, packed_ref, mask_ref, acc_ref, top_ref, qs_ref, vs, s16, s4, s1, p16, p4, p1):
    mask1_ref, mask4_ref, mask16_ref = (
        mask_ref.at[:, 0:512], mask_ref.at[0:128, 512:768], mask_ref.at[128:256, 512:768]
    )
    low256, high256 = value_masks(TOK)
    low_bf = low256[:128]
    for i in range(GROUP):
        packed = packed_ref[i]
        qs_ref[i, 0:128] = packed * low_bf
        qs_ref[i, 128:256] = pltpu.roll(packed.astype(F32), 64, 1).astype(BF) * low_bf
        vs[i, 0:TOK] = own_ref[i, 0:TOK] * high256 + low256

    def at4(n):
        b, r = n // 4, n % 4
        seen = slice(max(0, 2 * b - 2), 2 * b + 2)
        return slice(2 * b, 2 * b + 2), slice(64 * r, 64 * r + 64), seen, 64 * (seen.stop - seen.start)

    def at1(i):
        seen = slice(max(0, i - 1), i + 1)
        return seen, TOK * (seen.stop - seen.start)

    for r in range(16):
        rows = slice(16 * r, 16 * r + 16)
        scores = dot_t(qs_ref[:, rows].reshape(128, 128), own_ref[:, rows].reshape(128, 128)) + mask16_ref[:, 128:256]
        s16[r] = scores
        top_ref[:, rows] = jnp.broadcast_to(row_max(scores), (128, 128)).reshape(8, 16, 128)
    for n in range(16):
        at, rows, seen, width = at4(n)
        scores = dot_t(qs_ref[at, rows].reshape(128, 128), own_ref[seen, rows].reshape(width, 128))
        scores = scores + mask4_ref[:, 256 - width : 256]
        s4[n, :, 0:width] = scores
        top_ref[at, rows] = jnp.maximum(top_ref[at, rows].reshape(128, 128), row_max(scores)).reshape(2, 64, 128)
    for i in range(GROUP):
        seen, width = at1(i)
        scores = dot_t(qs_ref[i, 0:TOK], own_ref[seen, 0:TOK].reshape(width, 128)) + mask1_ref[:, 512 - width : 512]
        s1[i, :, 0:width] = scores
        top_ref[i, 0:TOK] = jnp.maximum(top_ref[i, 0:TOK], row_max(scores))
    for r in range(16):
        p16[r] = weights(s16[r], top_ref[:, 16 * r : 16 * r + 16].reshape(128, 128))
    for n in range(16):
        at, rows, seen, width = at4(n)
        p4[n, :, 0:width] = weights(s4[n, :, 0:width], top_ref[at, rows].reshape(128, 128))
    for i in range(GROUP):
        seen, width = at1(i)
        p1[i, :, 0:width] = weights(s1[i, :, 0:width], top_ref[i, 0:TOK])
    for r in range(16):
        rows = slice(16 * r, 16 * r + 16)
        acc_ref[:, rows] = dot(p16[r], vs[:, rows].reshape(128, 128)).reshape(8, 16, 128)
    for n in range(16):
        at, rows, seen, width = at4(n)
        acc_ref[at, rows] += dot(p4[n, :, 0:width], vs[seen, rows].reshape(width, 128)).reshape(2, 64, 128)
    for i in range(GROUP):
        seen, width = at1(i)
        acc_ref[i, 0:TOK] += dot(p1[i, :, 0:width], vs[seen, 0:TOK].reshape(width, 128))


def halo_kernel(
    index_ref, halo_ref, acc_ref, top_ref, qs_ref, perm_ref, mask_ref,
    out_ref, vs, peak, s16, s4, s1, p16, p4, p1,
):
    mask1_ref, mask4_ref, mask16_ref = (
        mask_ref.at[:, 0:512], mask_ref.at[0:128, 512:768], mask_ref.at[128:256, 512:768]
    )
    bias = jnp.where(index_ref[0] < GROUP, NEG, 0.0).astype(F32)
    low256, high256 = value_masks(TOK)
    for i in range(GROUP):
        vs[i, 0:TOK] = halo_ref[i] * high256 + low256

    def blocks(ref, rows):
        return ref[:, rows].reshape(128, 128)

    def last_two(ref, rows):
        return ref[6:8, rows].reshape(128, 128)

    mask16 = mask16_ref[:, 0:128] + bias
    for r in range(16):
        rows = slice(16 * r, 16 * r + 16)
        scores = dot_t(qs_ref[:, rows].reshape(128, 128), blocks(halo_ref, rows)) + mask16
        s16[r] = scores
        peak[:, rows] = jnp.maximum(top_ref[:, rows].reshape(128, 128), row_max(scores)).reshape(8, 16, 128)
    mask4 = mask4_ref[:, 0:128] + bias
    for r in range(4):
        rows = slice(64 * r, 64 * r + 64)
        scores = dot_t(qs_ref[0:2, rows].reshape(128, 128), last_two(halo_ref, rows)) + mask4
        s4[r] = scores
        peak[0:2, rows] = jnp.maximum(peak[0:2, rows].reshape(128, 128), row_max(scores)).reshape(2, 64, 128)
    scores = dot_t(qs_ref[0, 0:TOK], halo_ref[7]) + (mask1_ref[:, 0:TOK] + bias)
    s1[...] = scores
    peak[0, 0:TOK] = jnp.maximum(peak[0, 0:TOK], row_max(scores))
    for r in range(16):
        p16[r] = weights(s16[r], peak[:, 16 * r : 16 * r + 16].reshape(128, 128))
    for r in range(4):
        p4[r] = weights(s4[r], peak[0:2, 64 * r : 64 * r + 64].reshape(128, 128))
    p1[...] = weights(s1[...], peak[0, 0:TOK])
    for i in range(GROUP):
        peak[i, 0:TOK] = acc_ref[i, 0:TOK] * jnp.exp(top_ref[i, 0:TOK] - peak[i, 0:TOK])
    new = peak
    for r in range(16):
        rows = slice(16 * r, 16 * r + 16)
        new[:, rows] += dot(p16[r], blocks(vs, rows)).reshape(8, 16, 128)
    for r in range(4):
        rows = slice(64 * r, 64 * r + 64)
        new[0:2, rows] += dot(p4[r], last_two(vs, rows)).reshape(2, 64, 128)
    new[0, 0:TOK] += dot(p1[...], vs[7, 0:TOK])
    low_rows = half(64)
    for i in range(GROUP):
        mixed = normal(new[i, 0:TOK]).astype(BF) * high256
        natural = dot(perm_ref[...], mixed)
        out_ref[2 * i] = jnp.where(low_rows, pltpu.roll(natural[0:64], 64, 1), natural[64:128]).astype(BF)
        out_ref[2 * i + 1] = jnp.where(low_rows, pltpu.roll(natural[128:192], 64, 1), natural[192:256]).astype(BF)


def project_kernel(index_ref, core_ref, rows_ref, own_ref, other_ref, out_hbm, mixed, out_ref, sems):
    low = half(64)
    flip = 4 * ((index_ref[0] // GROUP) % 2)
    for side in range(2):
        core = core_ref[0] if side == 0 else 1 - core_ref[0]
        for j in range(4):
            first = rows_ref[2 * ((2 * j) ^ flip) + core].astype(F32)
            second = rows_ref[2 * ((2 * j) ^ flip) + 2 + core].astype(F32)
            cols = slice(128 * j, 128 * j + 128)
            mixed[side, 0:64, cols] = jnp.where(low, first, pltpu.roll(second, 64, 1)).astype(BF)
            mixed[side, 64:128, cols] = jnp.where(low, pltpu.roll(first, 64, 1), second).astype(BF)
    copies = []
    for n in range(4):
        cols = slice(512 * n, 512 * n + 512)
        out_ref[:, cols] = (dot(mixed[0], own_ref[:, cols]) + dot(mixed[1], other_ref[:, cols])).astype(BF)
        copy = pltpu.make_async_copy(out_ref.at[:, cols], out_hbm.at[:, cols], sems.at[n])
        copy.start()
        copies.append(copy)
    for copy in copies:
        copy.wait()


def vmem():
    return pl.BlockSpec(memory_space=pltpu.VMEM)


def limit(mib):
    return pltpu.CompilerParams(vmem_limit_bytes=mib * 2**20)


def per_device(query_rows, key_rows, value_rows, out_weight, blocks):
    tables = make_tables(blocks)
    index = lax.axis_index(SP).astype(jnp.int32).reshape(1)
    core = lax.axis_index("tp").astype(jnp.int32).reshape(1)

    smem = pl.BlockSpec(memory_space=pltpu.SMEM)
    hbm = pl.BlockSpec(memory_space=pltpu.HBM)
    send_kv, send_q = pl.pallas_call(
        pack_kernel,
        in_specs=[smem] * 2 + [hbm] * 7,
        out_specs=[vmem()] * 2,
        out_shape=[
            jax.ShapeDtypeStruct((GROUP, TOK, 128), BF),
            jax.ShapeDtypeStruct((GROUP, 128, 128), BF),
        ],
        scratch_shapes=[
            pltpu.VMEM((TOK, 512), BF),
            pltpu.VMEM((TOK, 512), BF),
            pltpu.VMEM((TOK, 512), BF),
            pltpu.VMEM((TOK, TOK), BF),
            pltpu.VMEM((TOK, 128), F32),
            pltpu.VMEM((TOK, 128), F32),
            pltpu.VMEM((16 + blocks // 16, 256), F32),
            pltpu.SemaphoreType.DMA((7,)),
        ],
        compiler_params=limit(12),
        name="pack",
    )(
        index,
        core,
        *(
            pltpu.with_memory_space_constraint(array, pltpu.HBM)
            for array in (
                query_rows,
                key_rows,
                value_rows,
                jnp.asarray(tables["perm"], BF),
                jnp.asarray(tables["cos"]),
                jnp.asarray(tables["sin"]),
                jnp.asarray(tables["anchors"]),
            )
        ),
    )
    following = [(s, (s // GROUP + 1) * GROUP + ((s % GROUP) ^ 4)) for s in range(blocks - GROUP)]
    own = lax.all_to_all(send_kv, ("b", "x"), 0, 0, tiled=True)
    halo = lax.ppermute(own, SP, following)
    send_q, _ = lax.optimization_barrier((send_q, own))
    packed = lax.all_to_all(send_q, ("b", "x"), 0, 0, tiled=True)
    weight, _ = lax.optimization_barrier((out_weight, packed))
    other_weight = lax.ppermute(weight, "tp", [(0, 1), (1, 0)])
    masks = jnp.asarray(tables["masks"])
    state = jax.ShapeDtypeStruct((GROUP, TOK + 8, 128), F32)
    acc, top, qs = pl.pallas_call(
        own_kernel,
        in_specs=[vmem()] * 3,
        out_specs=[vmem()] * 3,
        out_shape=[state, state, jax.ShapeDtypeStruct((GROUP, TOK + 16, 128), BF)],
        scratch_shapes=[
            pltpu.VMEM((GROUP, TOK + 16, 128), BF),
            pltpu.VMEM((16, 128, 128), F32),
            pltpu.VMEM((16, 128, 256), F32),
            pltpu.VMEM((GROUP, TOK, 512), F32),
            pltpu.VMEM((16, 128, 128), BF),
            pltpu.VMEM((16, 128, 256), BF),
            pltpu.VMEM((GROUP, TOK, 512), BF),
        ],
        compiler_params=limit(24),
        cost_estimate=pl.CostEstimate(flops=20 * 10**9, bytes_accessed=2 * 2**20, transcendentals=0),
        name="attend_own",
    )(own, packed, masks)
    back = pl.pallas_call(
        halo_kernel,
        in_specs=[smem] + [vmem()] * 6,
        out_specs=vmem(),
        out_shape=jax.ShapeDtypeStruct((2 * GROUP, 64, 128), BF),
        scratch_shapes=[
            pltpu.VMEM((GROUP, TOK + 16, 128), BF),
            pltpu.VMEM((GROUP, TOK + 8, 128), F32),
            pltpu.VMEM((16, 128, 128), F32),
            pltpu.VMEM((4, 128, 128), F32),
            pltpu.VMEM((TOK, TOK), F32),
            pltpu.VMEM((16, 128, 128), BF),
            pltpu.VMEM((4, 128, 128), BF),
            pltpu.VMEM((TOK, TOK), BF),
        ],
        compiler_params=limit(16),
        cost_estimate=pl.CostEstimate(flops=4 * 10**9, bytes_accessed=2 * 2**20, transcendentals=0),
        name="attend_halo",
    )(index, halo, acc, top, qs, jnp.asarray(tables["perm"].T, BF), masks)
    back, other_weight = lax.optimization_barrier((back, other_weight))
    rows = lax.all_to_all(back, ("b", "x", "tp"), 0, 0, tiled=True)
    return pl.pallas_call(
        project_kernel,
        in_specs=[smem] * 2 + [vmem()] * 3,
        out_specs=hbm,
        out_shape=pltpu.HBM((TOK // 2, 2048), BF),
        scratch_shapes=[
            pltpu.VMEM((2, TOK // 2, 512), BF),
            pltpu.VMEM((TOK // 2, 2048), BF),
            pltpu.SemaphoreType.DMA((4,)),
        ],
        compiler_params=limit(16),
        name="project",
    )(index, core, rows, out_weight, other_weight)


def solution(mesh):
    blocks = mesh.shape["sp"]
    fine = Mesh(mesh.devices.reshape(blocks // 16, 2, 2, 4, 2), SP + ("tp",))
    return jax.shard_map(
        functools.partial(per_device, blocks=blocks),
        mesh=fine,
        in_specs=(P(SP, "tp"), P(SP, "tp"), P(SP, "tp"), P("tp", None)),
        out_specs=P(SP + ("tp",), None),
        check_vma=False,
    )
```

```python
import functools
import math

import jax
import jax.numpy as jnp
import numpy as np
from jax import lax
from jax.experimental import pallas as pl
from jax.experimental.pallas import tpu as pltpu
from jax.sharding import Mesh, PartitionSpec as P


HD = 64
BACK = 128
THETA = 500000.0
TOK = 256
HALF = 128
GROUP = 8
SP = ("z", "g", "b", "x")
NEG = -1e30
BF = jnp.bfloat16
F32 = jnp.float32


def make_tables(blocks):
    p = np.arange(HALF)
    t = 16 * (p % 8) + p // 32 + 4 * ((p % 32) // 8)
    perm = np.zeros((HALF, HALF), np.float32)
    perm[p, t] = 1.0
    inverse = np.float64(THETA) ** (-np.arange(32, dtype=np.float64) / 32)
    lanes = inverse[np.arange(128) % 32]
    inner = t[:, None] * lanes[None, :]
    anchor = np.concatenate([np.arange(32) * HALF, np.arange(blocks // 16) * (16 * TOK)])[:, None] * lanes[None, :]
    return dict(
        cos=np.cos(inner).astype(np.float32),
        sin=np.sin(inner).astype(np.float32),
        anchors=np.concatenate([np.cos(anchor), np.sin(anchor)], axis=1).astype(np.float32),
        perm=perm,
    )


def dot(a, b):
    return lax.dot_general(a, b, (((1,), (0,)), ((), ())), preferred_element_type=F32)


def dot_t(a, b):
    return lax.dot_general(a, b, (((1,), (1,)), ((), ())), preferred_element_type=F32)


def half(rows):
    return lax.broadcasted_iota(jnp.int32, (rows, 128), 1) < 64


def pack_kernel(
    index_ref, core_ref, q_hbm, k_hbm, v_hbm, perm_hbm, cos_hbm, sin_hbm, anchor_hbm, kv_ref, packed_ref,
    q_ref, k_ref, v_ref, perm_ref, cos_ref, sin_ref, anchor_ref, kf, vf, qf, sems,
):
    pairs = (
        (anchor_hbm, anchor_ref), (cos_hbm, cos_ref), (sin_hbm, sin_ref), (perm_hbm, perm_ref),
        (k_hbm, k_ref), (v_hbm, v_ref), (q_hbm, q_ref),
    )
    copies = [pltpu.make_async_copy(source, target, sems.at[n]) for n, (source, target) in enumerate(pairs)]
    for copy in copies:
        copy.start()
    for copy in copies:
        copy.wait()
    block = index_ref[0]
    flip = 4 * ((block // GROUP) % 2)
    coarse = anchor_ref[pl.ds(32 + block // 16, 1), :]
    lane = lax.broadcasted_iota(jnp.int32, (HALF, 128), 1)
    low64 = lane < 64
    low32 = (lane & 63) < 32
    sign = jnp.where(low32[:1], -1.0, 1.0).astype(F32)

    def turn(rows, cosine, sine):
        other = jnp.where(low32, pltpu.roll(rows, 96, 1), pltpu.roll(rows, 32, 1))
        return rows * cosine + other * sine

    perm = perm_ref[...]
    for side in range(2):
        rows = slice(HALF * side, HALF * side + HALF)
        for source, target in ((k_ref, kf), (v_ref, vf), (q_ref, qf)):
            target[rows] = dot(perm, source[rows])
    for side in range(2):
        rows = slice(HALF * side, HALF * side + HALF)
        fine = anchor_ref[pl.ds(2 * (block % 16) + side, 1), :]
        cos_a = fine[:, :128] * coarse[:, :128] - fine[:, 128:] * coarse[:, 128:]
        sin_a = fine[:, 128:] * coarse[:, :128] + fine[:, :128] * coarse[:, 128:]
        cosine = cos_a * cos_ref[...] - sin_a * sin_ref[...]
        sine = (sin_a * sign) * cos_ref[...] + (cos_a * sign) * sin_ref[...]
        for j in range(4):
            cols = slice(128 * j, 128 * j + 128)
            key = turn(kf[rows, cols], cosine, sine)
            value = vf[rows, cols]
            even = (2 * j) ^ flip
            odd = even + 1
            kv_ref[even, rows] = jnp.where(low64, key, pltpu.roll(value, 64, 1)).astype(BF)
            kv_ref[odd, rows] = jnp.where(low64, pltpu.roll(key, 64, 1), value).astype(BF)
            qf[rows, cols] = turn(qf[rows, cols], cosine, sine) * (1.0 / math.sqrt(HD))
    for j in range(4):
        cols = slice(128 * j, 128 * j + 128)
        even = (2 * j) ^ flip
        odd = even + 1
        first, second = qf[0:HALF, cols], qf[HALF:TOK, cols]
        packed_ref[even] = jnp.where(low64, first, pltpu.roll(second, 64, 1)).astype(BF)
        packed_ref[odd] = jnp.where(low64, pltpu.roll(first, 64, 1), second).astype(BF)


def wide(x, n):
    return jnp.concatenate([x] * n, axis=1) if n > 1 else x


def value_masks(rows):
    low = half(rows)
    return jnp.where(low, 1.0, 0.0).astype(BF), jnp.where(low, 0.0, 1.0).astype(BF)


def normal(total):
    return total / pltpu.roll(total, 64, 1)


def row_max(scores):
    return jnp.max(scores, axis=1, keepdims=True)


def weights(scores, peak):
    return jnp.exp(scores - wide(peak, scores.shape[1] // 128)).astype(BF)


def band(query, key):
    distance = query - key
    return jnp.where((distance >= 0) & (distance <= BACK), 0.0, NEG).astype(F32)


def positions(rows, axis):
    shape = (rows, 128) if axis == 0 else (1, rows)
    p = lax.broadcasted_iota(jnp.int32, shape, axis)
    one = 16 * (p & 7) + (p >> 5) + 4 * ((p >> 3) & 3)
    four = 32 * (p >> 5) + 4 * (p & 7) + ((p >> 3) & 3)
    return one, four, p


def make_masks(before_ref, same_ref, bias):
    for n, (query, key) in enumerate(zip(positions(128, 0), positions(128, 1), strict=True)):
        before_ref[n] = band(query, key - 128) + bias
        if same_ref is not None:
            same_ref[n] = band(query, key)


def pieces16(ref, r):
    return ref[:, 8 * r : 8 * r + 8].reshape(128, 128)


def pieces4(ref, b, r):
    return ref[4 * b : 4 * b + 4, 32 * r : 32 * r + 32].reshape(128, 128)


def own_kernel(own_ref, packed_ref, acc_ref, top_ref, qs_ref, before, same, ks, vs, s16, s4, s1, p16, p4, p1):
    low, high = value_masks(128)
    for i in range(GROUP):
        packed = packed_ref[i]
        qs_ref[2 * i] = packed * low
        qs_ref[2 * i + 1] = pltpu.roll(packed.astype(F32), 64, 1).astype(BF) * low
        for side in range(2):
            key = own_ref[i, HALF * side : HALF * side + HALF]
            ks[2 * i + side] = key
            vs[2 * i + side] = key * high + low
    make_masks(before, same, 0.0)
    pair = lambda n: jnp.concatenate([before[n], same[n]], axis=1)

    def keys4(ref, b, r):
        return pieces4(ref, b, r) if b == 0 else jnp.concatenate([pieces4(ref, b - 1, r), pieces4(ref, b, r)], axis=0)

    def keys1(ref, i):
        return ref[0] if i == 0 else ref[i - 1 : i + 1].reshape(256, 128)

    for r in range(16):
        scores = dot_t(pieces16(qs_ref, r), pieces16(ks, r)) + same[2]
        s16[r] = scores
        top_ref[:, 8 * r : 8 * r + 8] = jnp.broadcast_to(row_max(scores), (128, 128)).reshape(16, 8, 128)
    for n in range(16):
        b, r = n // 4, n % 4
        scores = dot_t(pieces4(qs_ref, b, r), keys4(ks, b, r)) + (same[1] if b == 0 else pair(1))
        s4[n, :, 0 : scores.shape[1]] = scores
        peak = jnp.maximum(pieces4(top_ref, b, r), row_max(scores))
        top_ref[4 * b : 4 * b + 4, 32 * r : 32 * r + 32] = peak.reshape(4, 32, 128)
    for i in range(16):
        scores = dot_t(qs_ref[i], keys1(ks, i)) + (same[0] if i == 0 else pair(0))
        s1[i, :, 0 : scores.shape[1]] = scores
        top_ref[i] = jnp.maximum(top_ref[i], row_max(scores))
    for r in range(16):
        p16[r] = weights(s16[r], pieces16(top_ref, r))
    for n in range(16):
        width = 128 if n < 4 else 256
        p4[n, :, 0:width] = weights(s4[n, :, 0:width], pieces4(top_ref, n // 4, n % 4))
    for i in range(16):
        width = 128 if i == 0 else 256
        p1[i, :, 0:width] = weights(s1[i, :, 0:width], top_ref[i])
    for r in range(16):
        acc_ref[:, 8 * r : 8 * r + 8] = dot(p16[r], pieces16(vs, r)).reshape(16, 8, 128)
    for n in range(16):
        b, r = n // 4, n % 4
        width = 128 if n < 4 else 256
        acc_ref[4 * b : 4 * b + 4, 32 * r : 32 * r + 32] += dot(p4[n, :, 0:width], keys4(vs, b, r)).reshape(4, 32, 128)
    for i in range(16):
        width = 128 if i == 0 else 256
        acc_ref[i] += dot(p1[i, :, 0:width], keys1(vs, i))


def halo_kernel(
    index_ref, halo_ref, acc_ref, top_ref, qs_ref, perm_ref, out_ref, before, ks, vs, peak, s16, s4, s1, p16, p4, p1
):
    low, high = value_masks(128)
    for i in range(GROUP):
        for side in range(2):
            key = halo_ref[i, HALF * side : HALF * side + HALF]
            ks[2 * i + side] = key
            vs[2 * i + side] = key * high + low
    make_masks(before, None, jnp.where(index_ref[0] < GROUP, NEG, 0.0).astype(F32))
    for r in range(16):
        scores = dot_t(pieces16(qs_ref, r), pieces16(ks, r)) + before[2]
        s16[r] = scores
        peak[:, 8 * r : 8 * r + 8] = jnp.maximum(pieces16(top_ref, r), row_max(scores)).reshape(16, 8, 128)
    for r in range(4):
        scores = dot_t(pieces4(qs_ref, 0, r), pieces4(ks, 3, r)) + before[1]
        s4[r] = scores
        best = jnp.maximum(pieces4(peak, 0, r), row_max(scores))
        peak[0:4, 32 * r : 32 * r + 32] = best.reshape(4, 32, 128)
    scores = dot_t(qs_ref[0], ks[15]) + before[0]
    s1[...] = scores
    peak[0] = jnp.maximum(peak[0], row_max(scores))
    for r in range(16):
        p16[r] = weights(s16[r], pieces16(peak, r))
    for r in range(4):
        p4[r] = weights(s4[r], pieces4(peak, 0, r))
    p1[...] = weights(s1[...], peak[0])
    new = peak
    for i in range(16):
        new[i] = acc_ref[i] * jnp.exp(top_ref[i] - peak[i])
    for r in range(16):
        new[:, 8 * r : 8 * r + 8] += dot(p16[r], pieces16(vs, r)).reshape(16, 8, 128)
    for r in range(4):
        new[0:4, 32 * r : 32 * r + 32] += dot(p4[r], pieces4(vs, 3, r)).reshape(4, 32, 128)
    new[0] += dot(p1[...], vs[15])
    low_rows = half(64)
    for i in range(16):
        natural = dot(perm_ref[...], normal(new[i]).astype(BF) * high)
        out_ref[i] = jnp.where(low_rows, pltpu.roll(natural[0:64], 64, 1), natural[64:128]).astype(BF)


def project_kernel(index_ref, core_ref, rows_ref, own_ref, other_ref, out_hbm, mixed, out_ref, sems):
    low = half(64)
    flip = 4 * ((index_ref[0] // GROUP) % 2)
    for side in range(2):
        core = core_ref[0] if side == 0 else 1 - core_ref[0]
        for j in range(4):
            first = rows_ref[2 * ((2 * j) ^ flip) + core].astype(F32)
            second = rows_ref[2 * ((2 * j) ^ flip) + 2 + core].astype(F32)
            cols = slice(128 * j, 128 * j + 128)
            mixed[side, 0:64, cols] = jnp.where(low, first, pltpu.roll(second, 64, 1)).astype(BF)
            mixed[side, 64:128, cols] = jnp.where(low, pltpu.roll(first, 64, 1), second).astype(BF)
    copies = []
    for n in range(4):
        cols = slice(512 * n, 512 * n + 512)
        out_ref[:, cols] = (dot(mixed[0], own_ref[:, cols]) + dot(mixed[1], other_ref[:, cols])).astype(BF)
        copy = pltpu.make_async_copy(out_ref.at[:, cols], out_hbm.at[:, cols], sems.at[n])
        copy.start()
        copies.append(copy)
    for copy in copies:
        copy.wait()


def vmem():
    return pl.BlockSpec(memory_space=pltpu.VMEM)


def limit(mib):
    return pltpu.CompilerParams(vmem_limit_bytes=mib * 2**20)


def per_device(query_rows, key_rows, value_rows, out_weight, blocks):
    tables = make_tables(blocks)
    index = lax.axis_index(SP).astype(jnp.int32).reshape(1)
    core = lax.axis_index("tp").astype(jnp.int32).reshape(1)

    smem = pl.BlockSpec(memory_space=pltpu.SMEM)
    hbm = pl.BlockSpec(memory_space=pltpu.HBM)
    send_kv, send_q = pl.pallas_call(
        pack_kernel,
        in_specs=[smem] * 2 + [hbm] * 7,
        out_specs=[vmem()] * 2,
        out_shape=[
            jax.ShapeDtypeStruct((GROUP, TOK, 128), BF),
            jax.ShapeDtypeStruct((GROUP, 128, 128), BF),
        ],
        scratch_shapes=[
            pltpu.VMEM((TOK, 512), BF),
            pltpu.VMEM((TOK, 512), BF),
            pltpu.VMEM((TOK, 512), BF),
            pltpu.VMEM((HALF, HALF), BF),
            pltpu.VMEM((HALF, 128), F32),
            pltpu.VMEM((HALF, 128), F32),
            pltpu.VMEM((32 + blocks // 16, 256), F32),
            pltpu.VMEM((TOK, 512), F32),
            pltpu.VMEM((TOK, 512), F32),
            pltpu.VMEM((TOK, 512), F32),
            pltpu.SemaphoreType.DMA((7,)),
        ],
        compiler_params=limit(12),
        name="pack",
    )(
        index,
        core,
        *(
            pltpu.with_memory_space_constraint(array, pltpu.HBM)
            for array in (
                query_rows,
                key_rows,
                value_rows,
                jnp.asarray(tables["perm"], BF),
                jnp.asarray(tables["cos"]),
                jnp.asarray(tables["sin"]),
                jnp.asarray(tables["anchors"]),
            )
        ),
    )
    following = [(s, (s // GROUP + 1) * GROUP + ((s % GROUP) ^ 4)) for s in range(blocks - GROUP)]
    own = lax.all_to_all(send_kv, ("b", "x"), 0, 0, tiled=True)
    halo = lax.ppermute(own, SP, following)
    send_q, _ = lax.optimization_barrier((send_q, own))
    packed = lax.all_to_all(send_q, ("b", "x"), 0, 0, tiled=True)
    weight, _ = lax.optimization_barrier((out_weight, packed))
    other_weight = lax.ppermute(weight, "tp", [(0, 1), (1, 0)])
    state = jax.ShapeDtypeStruct((16, HALF, 128), F32)
    rows16 = pltpu.VMEM((16, HALF, 128), BF)
    acc, top, qs = pl.pallas_call(
        own_kernel,
        in_specs=[vmem()] * 2,
        out_specs=[vmem()] * 3,
        out_shape=[state, state, jax.ShapeDtypeStruct((16, HALF, 128), BF)],
        scratch_shapes=[
            pltpu.VMEM((3, 128, 128), F32),
            pltpu.VMEM((3, 128, 128), F32),
            rows16,
            rows16,
            pltpu.VMEM((16, 128, 128), F32),
            pltpu.VMEM((16, 128, 256), F32),
            pltpu.VMEM((16, 128, 256), F32),
            pltpu.VMEM((16, 128, 128), BF),
            pltpu.VMEM((16, 128, 256), BF),
            pltpu.VMEM((16, 128, 256), BF),
        ],
        compiler_params=limit(24),
        cost_estimate=pl.CostEstimate(flops=20 * 10**9, bytes_accessed=2 * 2**20, transcendentals=0),
        name="attend_own",
    )(own, packed)
    back = pl.pallas_call(
        halo_kernel,
        in_specs=[smem] + [vmem()] * 5,
        out_specs=vmem(),
        out_shape=jax.ShapeDtypeStruct((2 * GROUP, 64, 128), BF),
        scratch_shapes=[
            pltpu.VMEM((3, 128, 128), F32),
            rows16,
            rows16,
            pltpu.VMEM((16, HALF, 128), F32),
            pltpu.VMEM((16, 128, 128), F32),
            pltpu.VMEM((4, 128, 128), F32),
            pltpu.VMEM((128, 128), F32),
            pltpu.VMEM((16, 128, 128), BF),
            pltpu.VMEM((4, 128, 128), BF),
            pltpu.VMEM((128, 128), BF),
        ],
        compiler_params=limit(16),
        cost_estimate=pl.CostEstimate(flops=4 * 10**9, bytes_accessed=2 * 2**20, transcendentals=0),
        name="attend_halo",
    )(index, halo, acc, top, qs, jnp.asarray(tables["perm"].T, BF))
    back, other_weight = lax.optimization_barrier((back, other_weight))
    rows = lax.all_to_all(back, ("b", "x", "tp"), 0, 0, tiled=True)
    return pl.pallas_call(
        project_kernel,
        in_specs=[smem] * 2 + [vmem()] * 3,
        out_specs=hbm,
        out_shape=pltpu.HBM((TOK // 2, 2048), BF),
        scratch_shapes=[
            pltpu.VMEM((2, TOK // 2, 512), BF),
            pltpu.VMEM((TOK // 2, 2048), BF),
            pltpu.SemaphoreType.DMA((4,)),
        ],
        compiler_params=limit(16),
        name="project",
    )(index, core, rows, out_weight, other_weight)


def solution(mesh):
    blocks = mesh.shape["sp"]
    fine = Mesh(mesh.devices.reshape(blocks // 16, 2, 2, 4, 2), SP + ("tp",))
    return jax.shard_map(
        functools.partial(per_device, blocks=blocks),
        mesh=fine,
        in_specs=(P(SP, "tp"), P(SP, "tp"), P(SP, "tp"), P("tp", None)),
        out_specs=P(SP + ("tp",), None),
        check_vma=False,
    )
```

```python
import functools
import math

import jax
import jax.numpy as jnp
import numpy as np
from jax import lax
from jax.experimental import pallas as pl
from jax.experimental.pallas import tpu as pltpu
from jax.sharding import Mesh, PartitionSpec as P


HD = 64
BACK = 128
THETA = 500000.0
TOK = 256
HALF = 128
GROUP = 8
SP = ("z", "g", "b", "x")
NEG = -1e30
BF = jnp.bfloat16
F32 = jnp.float32


def make_tables(blocks):
    p = np.arange(HALF)
    t = 16 * (p % 8) + p // 32 + 4 * ((p % 32) // 8)
    perm = np.zeros((HALF, HALF), np.float32)
    perm[p, t] = 1.0
    inverse = np.float64(THETA) ** (-np.arange(32, dtype=np.float64) / 32)
    lanes = inverse[np.arange(128) % 32]
    inner = t[:, None] * lanes[None, :]
    anchor = np.concatenate([np.arange(32) * HALF, np.arange(blocks // 16) * (16 * TOK)])[:, None] * lanes[None, :]
    return dict(
        cos=np.cos(inner).astype(np.float32),
        sin=np.sin(inner).astype(np.float32),
        anchors=np.concatenate([np.cos(anchor), np.sin(anchor)], axis=1).astype(np.float32),
        perm=perm,
    )


def dot(a, b):
    return lax.dot_general(a, b, (((1,), (0,)), ((), ())), preferred_element_type=F32)


def dot_t(a, b):
    return lax.dot_general(a, b, (((1,), (1,)), ((), ())), preferred_element_type=F32)


def half(rows):
    return lax.broadcasted_iota(jnp.int32, (rows, 128), 1) < 64


def pack_kernel(
    index_ref, core_ref, q_hbm, k_hbm, v_hbm, perm_hbm, cos_hbm, sin_hbm, anchor_hbm, kv_ref, packed_ref,
    q_ref, k_ref, v_ref, perm_ref, cos_ref, sin_ref, anchor_ref, kf, vf, qf, sems,
):
    pairs = (
        (anchor_hbm, anchor_ref), (cos_hbm, cos_ref), (sin_hbm, sin_ref), (perm_hbm, perm_ref),
        (k_hbm, k_ref), (v_hbm, v_ref), (q_hbm, q_ref),
    )
    copies = [pltpu.make_async_copy(source, target, sems.at[n]) for n, (source, target) in enumerate(pairs)]
    for copy in copies:
        copy.start()
    for copy in copies:
        copy.wait()
    block = index_ref[0]
    flip = 4 * ((block // GROUP) % 2)
    coarse = anchor_ref[pl.ds(32 + block // 16, 1), :]
    lane = lax.broadcasted_iota(jnp.int32, (HALF, 128), 1)
    low64 = lane < 64
    low32 = (lane & 63) < 32
    sign = jnp.where(low32[:1], -1.0, 1.0).astype(F32)

    def turn(rows, cosine, sine):
        other = jnp.where(low32, pltpu.roll(rows, 96, 1), pltpu.roll(rows, 32, 1))
        return rows * cosine + other * sine

    perm = perm_ref[...]
    for side in range(2):
        rows = slice(HALF * side, HALF * side + HALF)
        for source, target in ((k_ref, kf), (v_ref, vf), (q_ref, qf)):
            target[rows] = dot(perm, source[rows])
    for side in range(2):
        rows = slice(HALF * side, HALF * side + HALF)
        fine = anchor_ref[pl.ds(2 * (block % 16) + side, 1), :]
        cos_a = fine[:, :128] * coarse[:, :128] - fine[:, 128:] * coarse[:, 128:]
        sin_a = fine[:, 128:] * coarse[:, :128] + fine[:, :128] * coarse[:, 128:]
        cosine = cos_a * cos_ref[...] - sin_a * sin_ref[...]
        sine = (sin_a * sign) * cos_ref[...] + (cos_a * sign) * sin_ref[...]
        for j in range(4):
            cols = slice(128 * j, 128 * j + 128)
            key = turn(kf[rows, cols], cosine, sine)
            value = vf[rows, cols]
            even = (2 * j) ^ flip
            odd = even + 1
            kv_ref[2 * even + side] = jnp.where(low64, key, pltpu.roll(value, 64, 1)).astype(BF)
            kv_ref[2 * odd + side] = jnp.where(low64, pltpu.roll(key, 64, 1), value).astype(BF)
            qf[rows, cols] = turn(qf[rows, cols], cosine, sine) * (1.0 / math.sqrt(HD))
    for j in range(4):
        cols = slice(128 * j, 128 * j + 128)
        even = (2 * j) ^ flip
        odd = even + 1
        first, second = qf[0:HALF, cols], qf[HALF:TOK, cols]
        packed_ref[even] = jnp.where(low64, first, pltpu.roll(second, 64, 1)).astype(BF)
        packed_ref[odd] = jnp.where(low64, pltpu.roll(first, 64, 1), second).astype(BF)


def wide(x, n):
    return jnp.concatenate([x] * n, axis=1) if n > 1 else x


def value_masks(rows):
    low = half(rows)
    return jnp.where(low, 1.0, 0.0).astype(BF), jnp.where(low, 0.0, 1.0).astype(BF)


def normal(total):
    return total / pltpu.roll(total, 64, 1)


def scored(query, keys, mask):
    return dot_t(query, keys) * math.log2(math.e) + mask


def row_max(scores):
    return jnp.max(scores, axis=1, keepdims=True)


def weights(scores, peak):
    return jnp.exp2(scores - wide(peak, scores.shape[1] // 128)).astype(BF)


def band(query, key):
    distance = query - key
    return jnp.where((distance >= 0) & (distance <= BACK), 0.0, NEG).astype(F32)


def positions(rows, axis):
    shape = (rows, 128) if axis == 0 else (1, rows)
    p = lax.broadcasted_iota(jnp.int32, shape, axis)
    one = 16 * (p & 7) + (p >> 5) + 4 * ((p >> 3) & 3)
    four = 32 * (p >> 5) + 4 * (p & 7) + ((p >> 3) & 3)
    return one, four, p


def make_masks(before_ref, same_ref, bias):
    for n, (query, key) in enumerate(zip(positions(128, 0), positions(128, 1), strict=True)):
        before_ref[n] = band(query, key - 128) + bias
        if same_ref is not None:
            same_ref[n] = band(query, key)


def pieces16(ref, r):
    return ref[:, 8 * r : 8 * r + 8].reshape(128, 128)


def pieces4(ref, b, r):
    return ref[4 * b : 4 * b + 4, 32 * r : 32 * r + 32].reshape(128, 128)


def own_kernel(ks, packed_ref, acc_ref, top_ref, qs_ref, before, same, vs, s16, s4, s1, p16, p4, p1):
    low, high = value_masks(128)
    for i in range(GROUP):
        packed = packed_ref[i]
        qs_ref[2 * i] = packed * low
        qs_ref[2 * i + 1] = pltpu.roll(packed.astype(F32), 64, 1).astype(BF) * low
        for n in (2 * i, 2 * i + 1):
            vs[n] = ks[n] * high + low
    make_masks(before, same, 0.0)
    pair = lambda n: jnp.concatenate([before[n], same[n]], axis=1)

    def keys4(ref, b, r):
        return pieces4(ref, b, r) if b == 0 else jnp.concatenate([pieces4(ref, b - 1, r), pieces4(ref, b, r)], axis=0)

    def keys1(ref, i):
        return ref[0] if i == 0 else ref[i - 1 : i + 1].reshape(256, 128)

    for r in range(16):
        scores = scored(pieces16(qs_ref, r), pieces16(ks, r), same[2])
        s16[r] = scores
        top_ref[:, 8 * r : 8 * r + 8] = jnp.broadcast_to(row_max(scores), (128, 128)).reshape(16, 8, 128)
    for n in range(16):
        b, r = n // 4, n % 4
        scores = scored(pieces4(qs_ref, b, r), keys4(ks, b, r), same[1] if b == 0 else pair(1))
        s4[n, :, 0 : scores.shape[1]] = scores
        peak = jnp.maximum(pieces4(top_ref, b, r), row_max(scores))
        top_ref[4 * b : 4 * b + 4, 32 * r : 32 * r + 32] = peak.reshape(4, 32, 128)
    for i in range(16):
        scores = scored(qs_ref[i], keys1(ks, i), same[0] if i == 0 else pair(0))
        s1[i, :, 0 : scores.shape[1]] = scores
        top_ref[i] = jnp.maximum(top_ref[i], row_max(scores))
    for r in range(16):
        p16[r] = weights(s16[r], pieces16(top_ref, r))
    for n in range(16):
        width = 128 if n < 4 else 256
        p4[n, :, 0:width] = weights(s4[n, :, 0:width], pieces4(top_ref, n // 4, n % 4))
    for i in range(16):
        width = 128 if i == 0 else 256
        p1[i, :, 0:width] = weights(s1[i, :, 0:width], top_ref[i])
    for r in range(16):
        acc_ref[:, 8 * r : 8 * r + 8] = dot(p16[r], pieces16(vs, r)).reshape(16, 8, 128)
    for n in range(16):
        b, r = n // 4, n % 4
        width = 128 if n < 4 else 256
        acc_ref[4 * b : 4 * b + 4, 32 * r : 32 * r + 32] += dot(p4[n, :, 0:width], keys4(vs, b, r)).reshape(4, 32, 128)
    for i in range(16):
        width = 128 if i == 0 else 256
        acc_ref[i] += dot(p1[i, :, 0:width], keys1(vs, i))


def halo_kernel(
    index_ref, ks, acc_ref, top_ref, qs_ref, perm_ref, out_ref, before, vs, peak, s16, s4, s1, p16, p4, p1
):
    low, high = value_masks(128)
    for n in range(16):
        vs[n] = ks[n] * high + low
    make_masks(before, None, jnp.where(index_ref[0] < GROUP, NEG, 0.0).astype(F32))
    for r in range(16):
        scores = scored(pieces16(qs_ref, r), pieces16(ks, r), before[2])
        s16[r] = scores
        peak[:, 8 * r : 8 * r + 8] = jnp.maximum(pieces16(top_ref, r), row_max(scores)).reshape(16, 8, 128)
    for r in range(4):
        scores = scored(pieces4(qs_ref, 0, r), pieces4(ks, 3, r), before[1])
        s4[r] = scores
        best = jnp.maximum(pieces4(peak, 0, r), row_max(scores))
        peak[0:4, 32 * r : 32 * r + 32] = best.reshape(4, 32, 128)
    scores = scored(qs_ref[0], ks[15], before[0])
    s1[...] = scores
    peak[0] = jnp.maximum(peak[0], row_max(scores))
    for r in range(16):
        p16[r] = weights(s16[r], pieces16(peak, r))
    for r in range(4):
        p4[r] = weights(s4[r], pieces4(peak, 0, r))
    p1[...] = weights(s1[...], peak[0])
    new = peak
    for i in range(16):
        new[i] = acc_ref[i] * jnp.exp2(top_ref[i] - peak[i])
    for r in range(16):
        new[:, 8 * r : 8 * r + 8] += dot(p16[r], pieces16(vs, r)).reshape(16, 8, 128)
    for r in range(4):
        new[0:4, 32 * r : 32 * r + 32] += dot(p4[r], pieces4(vs, 3, r)).reshape(4, 32, 128)
    new[0] += dot(p1[...], vs[15])
    low_rows = half(64)
    for i in range(16):
        natural = dot(perm_ref[...], normal(new[i]).astype(BF) * high)
        out_ref[i] = jnp.where(low_rows, pltpu.roll(natural[0:64], 64, 1), natural[64:128]).astype(BF)


def project_kernel(index_ref, core_ref, rows_ref, own_ref, other_hbm, out_hbm, mixed, out_ref, partial, other_ref, load_sems, sems):
    loads = []
    for n in range(4):
        cols = slice(512 * n, 512 * n + 512)
        load = pltpu.make_async_copy(other_hbm.at[:, cols], other_ref.at[:, cols], load_sems.at[n])
        load.start()
        loads.append(load)
    low = half(64)
    flip = 4 * ((index_ref[0] // GROUP) % 2)
    for side in range(2):
        core = core_ref[0] if side == 0 else 1 - core_ref[0]
        for j in range(4):
            first = rows_ref[2 * ((2 * j) ^ flip) + core].astype(F32)
            second = rows_ref[2 * ((2 * j) ^ flip) + 2 + core].astype(F32)
            cols = slice(128 * j, 128 * j + 128)
            mixed[side, 0:64, cols] = jnp.where(low, first, pltpu.roll(second, 64, 1)).astype(BF)
            mixed[side, 64:128, cols] = jnp.where(low, pltpu.roll(first, 64, 1), second).astype(BF)
    for n in range(4):
        cols = slice(512 * n, 512 * n + 512)
        partial[:, cols] = dot(mixed[0], own_ref[:, cols])
    copies = []
    for n in range(4):
        cols = slice(512 * n, 512 * n + 512)
        loads[n].wait()
        out_ref[:, cols] = (partial[:, cols] + dot(mixed[1], other_ref[:, cols])).astype(BF)
        copy = pltpu.make_async_copy(out_ref.at[:, cols], out_hbm.at[:, cols], sems.at[n])
        copy.start()
        copies.append(copy)
    for copy in copies:
        copy.wait()


def vmem():
    return pl.BlockSpec(memory_space=pltpu.VMEM)


def limit(mib):
    return pltpu.CompilerParams(vmem_limit_bytes=mib * 2**20)


def per_device(query_rows, key_rows, value_rows, out_weight, blocks):
    tables = make_tables(blocks)
    index = lax.axis_index(SP).astype(jnp.int32).reshape(1)
    core = lax.axis_index("tp").astype(jnp.int32).reshape(1)

    smem = pl.BlockSpec(memory_space=pltpu.SMEM)
    hbm = pl.BlockSpec(memory_space=pltpu.HBM)
    send_kv, send_q = pl.pallas_call(
        pack_kernel,
        in_specs=[smem] * 2 + [hbm] * 7,
        out_specs=[vmem()] * 2,
        out_shape=[
            jax.ShapeDtypeStruct((2 * GROUP, HALF, 128), BF),
            jax.ShapeDtypeStruct((GROUP, 128, 128), BF),
        ],
        scratch_shapes=[
            pltpu.VMEM((TOK, 512), BF),
            pltpu.VMEM((TOK, 512), BF),
            pltpu.VMEM((TOK, 512), BF),
            pltpu.VMEM((HALF, HALF), BF),
            pltpu.VMEM((HALF, 128), F32),
            pltpu.VMEM((HALF, 128), F32),
            pltpu.VMEM((32 + blocks // 16, 256), F32),
            pltpu.VMEM((TOK, 512), F32),
            pltpu.VMEM((TOK, 512), F32),
            pltpu.VMEM((TOK, 512), F32),
            pltpu.SemaphoreType.DMA((7,)),
        ],
        compiler_params=limit(12),
        name="pack",
    )(
        index,
        core,
        *(
            pltpu.with_memory_space_constraint(array, pltpu.HBM)
            for array in (
                query_rows,
                key_rows,
                value_rows,
                jnp.asarray(tables["perm"], BF),
                jnp.asarray(tables["cos"]),
                jnp.asarray(tables["sin"]),
                jnp.asarray(tables["anchors"]),
            )
        ),
    )
    following = [(s, (s // GROUP + 1) * GROUP + ((s % GROUP) ^ 4)) for s in range(blocks - GROUP)]
    own = lax.all_to_all(send_kv, ("b", "x"), 0, 0, tiled=True)
    halo = lax.ppermute(own, SP, following)
    send_q, _ = lax.optimization_barrier((send_q, own))
    packed = lax.all_to_all(send_q, ("b", "x"), 0, 0, tiled=True)
    state = jax.ShapeDtypeStruct((16, HALF, 128), F32)
    rows16 = pltpu.VMEM((16, HALF, 128), BF)
    acc, top, qs = pl.pallas_call(
        own_kernel,
        in_specs=[vmem()] * 2,
        out_specs=[vmem()] * 3,
        out_shape=[state, state, jax.ShapeDtypeStruct((16, HALF, 128), BF)],
        scratch_shapes=[
            pltpu.VMEM((3, 128, 128), F32),
            pltpu.VMEM((3, 128, 128), F32),
            rows16,
            pltpu.VMEM((16, 128, 128), F32),
            pltpu.VMEM((16, 128, 256), F32),
            pltpu.VMEM((16, 128, 256), F32),
            pltpu.VMEM((16, 128, 128), BF),
            pltpu.VMEM((16, 128, 256), BF),
            pltpu.VMEM((16, 128, 256), BF),
        ],
        compiler_params=limit(24),
        cost_estimate=pl.CostEstimate(flops=20 * 10**9, bytes_accessed=2 * 2**20, transcendentals=0),
        name="attend_own",
    )(own, packed)
    back = pl.pallas_call(
        halo_kernel,
        in_specs=[smem] + [vmem()] * 5,
        out_specs=vmem(),
        out_shape=jax.ShapeDtypeStruct((2 * GROUP, 64, 128), BF),
        scratch_shapes=[
            pltpu.VMEM((3, 128, 128), F32),
            rows16,
            pltpu.VMEM((16, HALF, 128), F32),
            pltpu.VMEM((16, 128, 128), F32),
            pltpu.VMEM((4, 128, 128), F32),
            pltpu.VMEM((128, 128), F32),
            pltpu.VMEM((16, 128, 128), BF),
            pltpu.VMEM((4, 128, 128), BF),
            pltpu.VMEM((128, 128), BF),
        ],
        compiler_params=limit(16),
        cost_estimate=pl.CostEstimate(flops=4 * 10**9, bytes_accessed=2 * 2**20, transcendentals=0),
        name="attend_halo",
    )(index, halo, acc, top, qs, jnp.asarray(tables["perm"].T, BF))
    weight, _ = lax.optimization_barrier((out_weight, back))
    rows = lax.all_to_all(back, ("b", "x", "tp"), 0, 0, tiled=True)
    other_weight = lax.ppermute(weight, "tp", [(0, 1), (1, 0)])
    return pl.pallas_call(
        project_kernel,
        in_specs=[smem] * 2 + [vmem()] * 2 + [hbm],
        out_specs=hbm,
        out_shape=pltpu.HBM((TOK // 2, 2048), BF),
        scratch_shapes=[
            pltpu.VMEM((2, TOK // 2, 512), BF),
            pltpu.VMEM((TOK // 2, 2048), BF),
            pltpu.VMEM((TOK // 2, 2048), F32),
            pltpu.VMEM((512, 2048), BF),
            pltpu.SemaphoreType.DMA((4,)),
            pltpu.SemaphoreType.DMA((4,)),
        ],
        compiler_params=limit(16),
        name="project",
    )(index, core, rows, out_weight, pltpu.with_memory_space_constraint(other_weight, pltpu.HBM))


def solution(mesh):
    blocks = mesh.shape["sp"]
    fine = Mesh(mesh.devices.reshape(blocks // 16, 2, 2, 4, 2), SP + ("tp",))
    return jax.shard_map(
        functools.partial(per_device, blocks=blocks),
        mesh=fine,
        in_specs=(P(SP, "tp"), P(SP, "tp"), P(SP, "tp"), P("tp", None)),
        out_specs=P(SP + ("tp",), None),
        check_vma=False,
    )
```

```python
import functools
import math

import jax
import jax.numpy as jnp
import numpy as np
from jax import lax
from jax.experimental import pallas as pl
from jax.experimental.pallas import tpu as pltpu
from jax.sharding import Mesh, PartitionSpec as P


HD = 64
BACK = 128
THETA = 500000.0
TOK = 256
HALF = 128
GROUP = 8
SP = ("z", "g", "b", "x")
NEG = -1e30
BF = jnp.bfloat16
F32 = jnp.float32


def make_tables(blocks):
    p = np.arange(HALF)
    t = 16 * (p % 8) + p // 32 + 4 * ((p % 32) // 8)
    perm = np.zeros((HALF, HALF), np.float32)
    perm[p, t] = 1.0
    inverse = np.float64(THETA) ** (-np.arange(32, dtype=np.float64) / 32)
    lanes = inverse[np.arange(128) % 32]
    inner = t[:, None] * lanes[None, :]
    anchor = np.concatenate([np.arange(32) * HALF, np.arange(blocks // 16) * (16 * TOK)])[:, None] * lanes[None, :]
    return dict(
        cos=np.cos(inner).astype(np.float32),
        sin=np.sin(inner).astype(np.float32),
        anchors=np.concatenate([np.cos(anchor), np.sin(anchor)], axis=1).astype(np.float32),
        perm=perm,
    )


def dot(a, b):
    return lax.dot_general(a, b, (((1,), (0,)), ((), ())), preferred_element_type=F32)


def dot_t(a, b):
    return lax.dot_general(a, b, (((1,), (1,)), ((), ())), preferred_element_type=F32)


def half(rows):
    return lax.broadcasted_iota(jnp.int32, (rows, 128), 1) < 64


def pack_kernel(
    index_ref, core_ref, q_hbm, k_hbm, v_hbm, perm_hbm, cos_hbm, sin_hbm, anchor_hbm, out_ref,
    q_ref, k_ref, v_ref, perm_ref, cos_ref, sin_ref, anchor_ref, kf, vf, qf, sems,
):
    pairs = (
        (anchor_hbm, anchor_ref), (cos_hbm, cos_ref), (sin_hbm, sin_ref), (perm_hbm, perm_ref),
        (k_hbm, k_ref), (v_hbm, v_ref), (q_hbm, q_ref),
    )
    copies = [pltpu.make_async_copy(source, target, sems.at[n]) for n, (source, target) in enumerate(pairs)]
    for copy in copies:
        copy.start()
    for copy in copies:
        copy.wait()
    block = index_ref[0]
    flip = 4 * ((block // GROUP) % 2)
    coarse = anchor_ref[pl.ds(32 + block // 16, 1), :]
    lane = lax.broadcasted_iota(jnp.int32, (HALF, 128), 1)
    low64 = lane < 64
    low32 = (lane & 63) < 32
    sign = jnp.where(low32[:1], -1.0, 1.0).astype(F32)

    def turn(rows, cosine, sine):
        other = jnp.where(low32, pltpu.roll(rows, 96, 1), pltpu.roll(rows, 32, 1))
        return rows * cosine + other * sine

    perm = perm_ref[...]
    for side in range(2):
        rows = slice(HALF * side, HALF * side + HALF)
        for source, target in ((k_ref, kf), (v_ref, vf), (q_ref, qf)):
            target[rows] = dot(perm, source[rows])
    for side in range(2):
        rows = slice(HALF * side, HALF * side + HALF)
        fine = anchor_ref[pl.ds(2 * (block % 16) + side, 1), :]
        cos_a = fine[:, :128] * coarse[:, :128] - fine[:, 128:] * coarse[:, 128:]
        sin_a = fine[:, 128:] * coarse[:, :128] + fine[:, :128] * coarse[:, 128:]
        cosine = cos_a * cos_ref[...] - sin_a * sin_ref[...]
        sine = (sin_a * sign) * cos_ref[...] + (cos_a * sign) * sin_ref[...]
        for j in range(4):
            cols = slice(128 * j, 128 * j + 128)
            key = turn(kf[rows, cols], cosine, sine)
            value = vf[rows, cols]
            even = (2 * j) ^ flip
            odd = even + 1
            out_ref[3 * even + side] = jnp.where(low64, key, pltpu.roll(value, 64, 1)).astype(BF)
            out_ref[3 * odd + side] = jnp.where(low64, pltpu.roll(key, 64, 1), value).astype(BF)
            qf[rows, cols] = turn(qf[rows, cols], cosine, sine) * (1.0 / math.sqrt(HD))
    for j in range(4):
        cols = slice(128 * j, 128 * j + 128)
        even = (2 * j) ^ flip
        odd = even + 1
        first, second = qf[0:HALF, cols], qf[HALF:TOK, cols]
        out_ref[3 * even + 2] = jnp.where(low64, first, pltpu.roll(second, 64, 1)).astype(BF)
        out_ref[3 * odd + 2] = jnp.where(low64, pltpu.roll(first, 64, 1), second).astype(BF)


def wide(x, n):
    return jnp.concatenate([x] * n, axis=1) if n > 1 else x


def value_masks(rows):
    low = half(rows)
    return jnp.where(low, 1.0, 0.0).astype(BF), jnp.where(low, 0.0, 1.0).astype(BF)


def normal(total):
    return total / pltpu.roll(total, 64, 1)


def scored(query, keys, mask):
    return dot_t(query, keys) * math.log2(math.e) + mask


def row_max(scores):
    return jnp.max(scores, axis=1, keepdims=True)


def weights(scores, peak):
    return jnp.exp2(scores - wide(peak, scores.shape[1] // 128)).astype(BF)


def band(query, key):
    distance = query - key
    return jnp.where((distance >= 0) & (distance <= BACK), 0.0, NEG).astype(F32)


def positions(rows, axis):
    shape = (rows, 128) if axis == 0 else (1, rows)
    p = lax.broadcasted_iota(jnp.int32, shape, axis)
    one = 16 * (p & 7) + (p >> 5) + 4 * ((p >> 3) & 3)
    four = 32 * (p >> 5) + 4 * (p & 7) + ((p >> 3) & 3)
    return one, four, p


def make_masks(before_ref, same_ref, bias):
    for n, (query, key) in enumerate(zip(positions(128, 0), positions(128, 1), strict=True)):
        before_ref[n] = band(query, key - 128) + bias
        if same_ref is not None:
            same_ref[n] = band(query, key)


def pieces16(ref, r):
    return ref[:, 8 * r : 8 * r + 8].reshape(128, 128)


def pieces4(ref, b, r):
    return ref[4 * b : 4 * b + 4, 32 * r : 32 * r + 32].reshape(128, 128)


def own_kernel(ks, packed_ref, acc_ref, top_ref, qs_ref, before, same, vs, s16, s4, s1, p16, p4, p1):
    low, high = value_masks(128)
    for i in range(GROUP):
        packed = packed_ref[3 * i + 2]
        qs_ref[2 * i] = packed * low
        qs_ref[2 * i + 1] = pltpu.roll(packed.astype(F32), 64, 1).astype(BF) * low
        for n in (2 * i, 2 * i + 1):
            vs[n] = ks[n] * high + low
    make_masks(before, same, 0.0)
    pair = lambda n: jnp.concatenate([before[n], same[n]], axis=1)

    def keys4(ref, b, r):
        return pieces4(ref, b, r) if b == 0 else jnp.concatenate([pieces4(ref, b - 1, r), pieces4(ref, b, r)], axis=0)

    def keys1(ref, i):
        return ref[0] if i == 0 else ref[i - 1 : i + 1].reshape(256, 128)

    for r in range(16):
        scores = scored(pieces16(qs_ref, r), pieces16(ks, r), same[2])
        s16[r] = scores
        top_ref[:, 8 * r : 8 * r + 8] = jnp.broadcast_to(row_max(scores), (128, 128)).reshape(16, 8, 128)
    for n in range(16):
        b, r = n // 4, n % 4
        scores = scored(pieces4(qs_ref, b, r), keys4(ks, b, r), same[1] if b == 0 else pair(1))
        s4[n, :, 0 : scores.shape[1]] = scores
        peak = jnp.maximum(pieces4(top_ref, b, r), row_max(scores))
        top_ref[4 * b : 4 * b + 4, 32 * r : 32 * r + 32] = peak.reshape(4, 32, 128)
    for i in range(16):
        scores = scored(qs_ref[i], keys1(ks, i), same[0] if i == 0 else pair(0))
        s1[i, :, 0 : scores.shape[1]] = scores
        top_ref[i] = jnp.maximum(top_ref[i], row_max(scores))
    for r in range(16):
        p16[r] = weights(s16[r], pieces16(top_ref, r))
    for n in range(16):
        width = 128 if n < 4 else 256
        p4[n, :, 0:width] = weights(s4[n, :, 0:width], pieces4(top_ref, n // 4, n % 4))
    for i in range(16):
        width = 128 if i == 0 else 256
        p1[i, :, 0:width] = weights(s1[i, :, 0:width], top_ref[i])
    for r in range(16):
        acc_ref[:, 8 * r : 8 * r + 8] = dot(p16[r], pieces16(vs, r)).reshape(16, 8, 128)
    for n in range(16):
        b, r = n // 4, n % 4
        width = 128 if n < 4 else 256
        acc_ref[4 * b : 4 * b + 4, 32 * r : 32 * r + 32] += dot(p4[n, :, 0:width], keys4(vs, b, r)).reshape(4, 32, 128)
    for i in range(16):
        width = 128 if i == 0 else 256
        acc_ref[i] += dot(p1[i, :, 0:width], keys1(vs, i))


def halo_kernel(
    index_ref, ks, acc_ref, top_ref, qs_ref, perm_ref, out_ref, before, vs, peak, s16, s4, s1, p16, p4, p1
):
    low, high = value_masks(128)
    for n in range(16):
        vs[n] = ks[n] * high + low
    make_masks(before, None, jnp.where(index_ref[0] < GROUP, NEG, 0.0).astype(F32))
    for r in range(16):
        scores = scored(pieces16(qs_ref, r), pieces16(ks, r), before[2])
        s16[r] = scores
        peak[:, 8 * r : 8 * r + 8] = jnp.maximum(pieces16(top_ref, r), row_max(scores)).reshape(16, 8, 128)
    for r in range(4):
        scores = scored(pieces4(qs_ref, 0, r), pieces4(ks, 3, r), before[1])
        s4[r] = scores
        best = jnp.maximum(pieces4(peak, 0, r), row_max(scores))
        peak[0:4, 32 * r : 32 * r + 32] = best.reshape(4, 32, 128)
    scores = scored(qs_ref[0], ks[15], before[0])
    s1[...] = scores
    peak[0] = jnp.maximum(peak[0], row_max(scores))
    for r in range(16):
        p16[r] = weights(s16[r], pieces16(peak, r))
    for r in range(4):
        p4[r] = weights(s4[r], pieces4(peak, 0, r))
    p1[...] = weights(s1[...], peak[0])
    new = peak
    for i in range(16):
        new[i] = acc_ref[i] * jnp.exp2(top_ref[i] - peak[i])
    for r in range(16):
        new[:, 8 * r : 8 * r + 8] += dot(p16[r], pieces16(vs, r)).reshape(16, 8, 128)
    for r in range(4):
        new[0:4, 32 * r : 32 * r + 32] += dot(p4[r], pieces4(vs, 3, r)).reshape(4, 32, 128)
    new[0] += dot(p1[...], vs[15])
    low_rows = half(64)
    for i in range(16):
        natural = dot(perm_ref[...], normal(new[i]).astype(BF) * high)
        out_ref[i] = jnp.where(low_rows, pltpu.roll(natural[0:64], 64, 1), natural[64:128]).astype(BF)


def project_kernel(index_ref, core_ref, rows_ref, own_ref, other_ref, out_hbm, mixed, out_ref, sems):
    low = half(64)
    flip = 4 * ((index_ref[0] // GROUP) % 2)
    for side in range(2):
        core = core_ref[0] if side == 0 else 1 - core_ref[0]
        for j in range(4):
            first = rows_ref[2 * ((2 * j) ^ flip) + core].astype(F32)
            second = rows_ref[2 * ((2 * j) ^ flip) + 2 + core].astype(F32)
            cols = slice(128 * j, 128 * j + 128)
            mixed[side, 0:64, cols] = jnp.where(low, first, pltpu.roll(second, 64, 1)).astype(BF)
            mixed[side, 64:128, cols] = jnp.where(low, pltpu.roll(first, 64, 1), second).astype(BF)
    copies = []
    for n in range(4):
        cols = slice(512 * n, 512 * n + 512)
        out_ref[:, cols] = (dot(mixed[0], own_ref[:, cols]) + dot(mixed[1], other_ref[:, cols])).astype(BF)
        copy = pltpu.make_async_copy(out_ref.at[:, cols], out_hbm.at[:, cols], sems.at[n])
        copy.start()
        copies.append(copy)
    for copy in copies:
        copy.wait()


def vmem():
    return pl.BlockSpec(memory_space=pltpu.VMEM)


def limit(mib):
    return pltpu.CompilerParams(vmem_limit_bytes=mib * 2**20)


def per_device(query_rows, key_rows, value_rows, out_weight, blocks):
    tables = make_tables(blocks)
    index = lax.axis_index(SP).astype(jnp.int32).reshape(1)
    core = lax.axis_index("tp").astype(jnp.int32).reshape(1)

    smem = pl.BlockSpec(memory_space=pltpu.SMEM)
    hbm = pl.BlockSpec(memory_space=pltpu.HBM)
    send = pl.pallas_call(
        pack_kernel,
        in_specs=[smem] * 2 + [hbm] * 7,
        out_specs=vmem(),
        out_shape=jax.ShapeDtypeStruct((3 * GROUP, HALF, 128), BF),
        scratch_shapes=[
            pltpu.VMEM((TOK, 512), BF),
            pltpu.VMEM((TOK, 512), BF),
            pltpu.VMEM((TOK, 512), BF),
            pltpu.VMEM((HALF, HALF), BF),
            pltpu.VMEM((HALF, 128), F32),
            pltpu.VMEM((HALF, 128), F32),
            pltpu.VMEM((32 + blocks // 16, 256), F32),
            pltpu.VMEM((TOK, 512), F32),
            pltpu.VMEM((TOK, 512), F32),
            pltpu.VMEM((TOK, 512), F32),
            pltpu.SemaphoreType.DMA((7,)),
        ],
        compiler_params=limit(12),
        name="pack",
    )(
        index,
        core,
        *(
            pltpu.with_memory_space_constraint(array, pltpu.HBM)
            for array in (
                query_rows,
                key_rows,
                value_rows,
                jnp.asarray(tables["perm"], BF),
                jnp.asarray(tables["cos"]),
                jnp.asarray(tables["sin"]),
                jnp.asarray(tables["anchors"]),
            )
        ),
    )
    following = [(s, (s // GROUP + 1) * GROUP + ((s % GROUP) ^ 4)) for s in range(blocks - GROUP)]
    both = lax.all_to_all(send, ("b", "x"), 0, 0, tiled=True)
    own = both.reshape(GROUP, 3, HALF, 128)[:, 0:2].reshape(2 * GROUP, HALF, 128)
    halo = lax.ppermute(own, SP, following)
    weight, _ = lax.optimization_barrier((out_weight, own))
    other_weight = lax.ppermute(weight, "tp", [(0, 1), (1, 0)])
    state = jax.ShapeDtypeStruct((16, HALF, 128), F32)
    rows16 = pltpu.VMEM((16, HALF, 128), BF)
    acc, top, qs = pl.pallas_call(
        own_kernel,
        in_specs=[vmem()] * 2,
        out_specs=[vmem()] * 3,
        out_shape=[state, state, jax.ShapeDtypeStruct((16, HALF, 128), BF)],
        scratch_shapes=[
            pltpu.VMEM((3, 128, 128), F32),
            pltpu.VMEM((3, 128, 128), F32),
            rows16,
            pltpu.VMEM((16, 128, 128), F32),
            pltpu.VMEM((16, 128, 256), F32),
            pltpu.VMEM((16, 128, 256), F32),
            pltpu.VMEM((16, 128, 128), BF),
            pltpu.VMEM((16, 128, 256), BF),
            pltpu.VMEM((16, 128, 256), BF),
        ],
        compiler_params=limit(24),
        cost_estimate=pl.CostEstimate(flops=20 * 10**9, bytes_accessed=2 * 2**20, transcendentals=0),
        name="attend_own",
    )(own, both)
    back = pl.pallas_call(
        halo_kernel,
        in_specs=[smem] + [vmem()] * 5,
        out_specs=vmem(),
        out_shape=jax.ShapeDtypeStruct((2 * GROUP, 64, 128), BF),
        scratch_shapes=[
            pltpu.VMEM((3, 128, 128), F32),
            rows16,
            pltpu.VMEM((16, HALF, 128), F32),
            pltpu.VMEM((16, 128, 128), F32),
            pltpu.VMEM((4, 128, 128), F32),
            pltpu.VMEM((128, 128), F32),
            pltpu.VMEM((16, 128, 128), BF),
            pltpu.VMEM((4, 128, 128), BF),
            pltpu.VMEM((128, 128), BF),
        ],
        compiler_params=limit(16),
        cost_estimate=pl.CostEstimate(flops=4 * 10**9, bytes_accessed=2 * 2**20, transcendentals=0),
        name="attend_halo",
    )(index, halo, acc, top, qs, jnp.asarray(tables["perm"].T, BF))
    back, other_weight = lax.optimization_barrier((back, other_weight))
    rows = lax.all_to_all(back, ("b", "x", "tp"), 0, 0, tiled=True)
    return pl.pallas_call(
        project_kernel,
        in_specs=[smem] * 2 + [vmem()] * 3,
        out_specs=hbm,
        out_shape=pltpu.HBM((TOK // 2, 2048), BF),
        scratch_shapes=[
            pltpu.VMEM((2, TOK // 2, 512), BF),
            pltpu.VMEM((TOK // 2, 2048), BF),
            pltpu.SemaphoreType.DMA((4,)),
        ],
        compiler_params=limit(16),
        name="project",
    )(index, core, rows, out_weight, other_weight)


def solution(mesh):
    blocks = mesh.shape["sp"]
    fine = Mesh(mesh.devices.reshape(blocks // 16, 2, 2, 4, 2), SP + ("tp",))
    return jax.shard_map(
        functools.partial(per_device, blocks=blocks),
        mesh=fine,
        in_specs=(P(SP, "tp"), P(SP, "tp"), P(SP, "tp"), P("tp", None)),
        out_specs=P(SP + ("tp",), None),
        check_vma=False,
    )
```

```python
import functools
import math

import jax
import jax.numpy as jnp
import numpy as np
from jax import lax
from jax.experimental import pallas as pl
from jax.experimental.pallas import tpu as pltpu
from jax.sharding import Mesh, PartitionSpec as P


HD = 64
BACK = 128
THETA = 500000.0
TOK = 256
HALF = 128
GROUP = 8
SP = ("z", "g", "b", "x")
NEG = -1e30
BF = jnp.bfloat16
F32 = jnp.float32


def make_tables(blocks):
    p = np.arange(HALF)
    t = 16 * (p % 8) + p // 32 + 4 * ((p % 32) // 8)
    perm = np.zeros((HALF, HALF), np.float32)
    perm[p, t] = 1.0
    inverse = np.float64(THETA) ** (-np.arange(32, dtype=np.float64) / 32)
    lanes = inverse[np.arange(128) % 32]
    inner = t[:, None] * lanes[None, :]
    anchor = np.concatenate([np.arange(32) * HALF, np.arange(blocks // 16) * (16 * TOK)])[:, None] * lanes[None, :]
    return dict(
        cos=np.cos(inner).astype(np.float32),
        sin=np.sin(inner).astype(np.float32),
        anchors=np.concatenate([np.cos(anchor), np.sin(anchor)], axis=1).astype(np.float32),
        perm=perm,
    )


def dot(a, b):
    return lax.dot_general(a, b, (((1,), (0,)), ((), ())), preferred_element_type=F32)


def dot_t(a, b):
    return lax.dot_general(a, b, (((1,), (1,)), ((), ())), preferred_element_type=F32)


def half(rows):
    return lax.broadcasted_iota(jnp.int32, (rows, 128), 1) < 64


def pack_kernel(
    index_ref, core_ref, q_hbm, k_hbm, v_hbm, perm_hbm, cos_hbm, sin_hbm, anchor_hbm, kv_ref, packed_ref,
    q_ref, k_ref, v_ref, perm_ref, cos_ref, sin_ref, anchor_ref, kf, vf, qf, sems,
):
    pairs = (
        (anchor_hbm, anchor_ref), (cos_hbm, cos_ref), (sin_hbm, sin_ref), (perm_hbm, perm_ref),
        (k_hbm, k_ref), (v_hbm, v_ref), (q_hbm, q_ref),
    )
    copies = [pltpu.make_async_copy(source, target, sems.at[n]) for n, (source, target) in enumerate(pairs)]
    for copy in copies:
        copy.start()
    for copy in copies:
        copy.wait()
    block = index_ref[0]
    flip = 4 * ((block // GROUP) % 2)
    coarse = anchor_ref[pl.ds(32 + block // 16, 1), :]
    lane = lax.broadcasted_iota(jnp.int32, (HALF, 128), 1)
    low64 = lane < 64
    low32 = (lane & 63) < 32
    sign = jnp.where(low32[:1], -1.0, 1.0).astype(F32)

    def turn(rows, cosine, sine):
        other = jnp.where(low32, pltpu.roll(rows, 96, 1), pltpu.roll(rows, 32, 1))
        return rows * cosine + other * sine

    perm = perm_ref[...]
    for side in range(2):
        rows = slice(HALF * side, HALF * side + HALF)
        for source, target in ((k_ref, kf), (v_ref, vf), (q_ref, qf)):
            target[rows] = dot(perm, source[rows])
    for side in range(2):
        rows = slice(HALF * side, HALF * side + HALF)
        fine = anchor_ref[pl.ds(2 * (block % 16) + side, 1), :]
        cos_a = fine[:, :128] * coarse[:, :128] - fine[:, 128:] * coarse[:, 128:]
        sin_a = fine[:, 128:] * coarse[:, :128] + fine[:, :128] * coarse[:, 128:]
        cosine = cos_a * cos_ref[...] - sin_a * sin_ref[...]
        sine = (sin_a * sign) * cos_ref[...] + (cos_a * sign) * sin_ref[...]
        for j in range(4):
            cols = slice(128 * j, 128 * j + 128)
            key = turn(kf[rows, cols], cosine, sine)
            value = vf[rows, cols]
            even = (2 * j) ^ flip
            odd = even + 1
            kv_ref[2 * even + side] = jnp.where(low64, key, pltpu.roll(value, 64, 1)).astype(BF)
            kv_ref[2 * odd + side] = jnp.where(low64, pltpu.roll(key, 64, 1), value).astype(BF)
            qf[rows, cols] = turn(qf[rows, cols], cosine, sine) * (1.0 / math.sqrt(HD))
    for j in range(4):
        cols = slice(128 * j, 128 * j + 128)
        even = (2 * j) ^ flip
        odd = even + 1
        first, second = qf[0:HALF, cols], qf[HALF:TOK, cols]
        packed_ref[even] = jnp.where(low64, first, pltpu.roll(second, 64, 1)).astype(BF)
        packed_ref[odd] = jnp.where(low64, pltpu.roll(first, 64, 1), second).astype(BF)


def wide(x, n):
    return jnp.concatenate([x] * n, axis=1) if n > 1 else x


def value_masks(rows):
    low = half(rows)
    return jnp.where(low, 1.0, 0.0).astype(BF), jnp.where(low, 0.0, 1.0).astype(BF)


def normal(total):
    return total / pltpu.roll(total, 64, 1)


def scored(query, keys, mask):
    return dot_t(query, keys) * math.log2(math.e) + mask


def row_max(scores):
    return jnp.max(scores, axis=1, keepdims=True)


def weights(scores, peak):
    return jnp.exp2(scores - wide(peak, scores.shape[1] // 128)).astype(BF)


def band(query, key):
    distance = query - key
    return jnp.where((distance >= 0) & (distance <= BACK), 0.0, NEG).astype(F32)


def positions(rows, axis):
    shape = (rows, 128) if axis == 0 else (1, rows)
    p = lax.broadcasted_iota(jnp.int32, shape, axis)
    one = 16 * (p & 7) + (p >> 5) + 4 * ((p >> 3) & 3)
    four = 32 * (p >> 5) + 4 * (p & 7) + ((p >> 3) & 3)
    return one, four, p


def make_masks(before_ref, same_ref, bias):
    for n, (query, key) in enumerate(zip(positions(128, 0), positions(128, 1), strict=True)):
        before_ref[n] = band(query, key - 128) + bias
        if same_ref is not None:
            same_ref[n] = band(query, key)


def pieces16(ref, r):
    return ref[:, 8 * r : 8 * r + 8].reshape(128, 128)


def pieces4(ref, b, r):
    return ref[4 * b : 4 * b + 4, 32 * r : 32 * r + 32].reshape(128, 128)


def own_kernel(ks, packed_ref, acc_ref, top_ref, qs_ref, before, same, vs, s16, s4, s1, p16, p4, p1):
    low, high = value_masks(128)
    for i in range(GROUP):
        packed = packed_ref[i]
        qs_ref[2 * i] = packed * low
        qs_ref[2 * i + 1] = pltpu.roll(packed.astype(F32), 64, 1).astype(BF) * low
        for n in (2 * i, 2 * i + 1):
            vs[n] = ks[n] * high + low
    make_masks(before, same, 0.0)
    pair = lambda n: jnp.concatenate([before[n], same[n]], axis=1)

    def keys4(ref, b, r):
        return pieces4(ref, b, r) if b == 0 else jnp.concatenate([pieces4(ref, b - 1, r), pieces4(ref, b, r)], axis=0)

    def keys1(ref, i):
        return ref[0] if i == 0 else ref[i - 1 : i + 1].reshape(256, 128)

    for r in range(16):
        scores = scored(pieces16(qs_ref, r), pieces16(ks, r), same[2])
        s16[r] = scores
        top_ref[:, 8 * r : 8 * r + 8] = jnp.broadcast_to(row_max(scores), (128, 128)).reshape(16, 8, 128)
    for n in range(16):
        b, r = n // 4, n % 4
        scores = scored(pieces4(qs_ref, b, r), keys4(ks, b, r), same[1] if b == 0 else pair(1))
        s4[n, :, 0 : scores.shape[1]] = scores
        peak = jnp.maximum(pieces4(top_ref, b, r), row_max(scores))
        top_ref[4 * b : 4 * b + 4, 32 * r : 32 * r + 32] = peak.reshape(4, 32, 128)
    for i in range(16):
        scores = scored(qs_ref[i], keys1(ks, i), same[0] if i == 0 else pair(0))
        s1[i, :, 0 : scores.shape[1]] = scores
        top_ref[i] = jnp.maximum(top_ref[i], row_max(scores))
    for r in range(16):
        p16[r] = weights(s16[r], pieces16(top_ref, r))
    for n in range(16):
        width = 128 if n < 4 else 256
        p4[n, :, 0:width] = weights(s4[n, :, 0:width], pieces4(top_ref, n // 4, n % 4))
    for i in range(16):
        width = 128 if i == 0 else 256
        p1[i, :, 0:width] = weights(s1[i, :, 0:width], top_ref[i])
    for r in range(16):
        acc_ref[:, 8 * r : 8 * r + 8] = dot(p16[r], pieces16(vs, r)).reshape(16, 8, 128)
    for n in range(16):
        b, r = n // 4, n % 4
        width = 128 if n < 4 else 256
        acc_ref[4 * b : 4 * b + 4, 32 * r : 32 * r + 32] += dot(p4[n, :, 0:width], keys4(vs, b, r)).reshape(4, 32, 128)
    for i in range(16):
        width = 128 if i == 0 else 256
        acc_ref[i] += dot(p1[i, :, 0:width], keys1(vs, i))


def halo_kernel(
    index_ref, ks, acc_ref, top_ref, qs_ref, perm_ref, out_ref, before, vs, peak, s16, s4, s1, p16, p4, p1
):
    low, high = value_masks(128)
    for n in range(16):
        vs[n] = ks[n] * high + low
    make_masks(before, None, jnp.where(index_ref[0] < GROUP, NEG, 0.0).astype(F32))
    for r in range(16):
        scores = scored(pieces16(qs_ref, r), pieces16(ks, r), before[2])
        s16[r] = scores
        peak[:, 8 * r : 8 * r + 8] = jnp.maximum(pieces16(top_ref, r), row_max(scores)).reshape(16, 8, 128)
    for r in range(4):
        scores = scored(pieces4(qs_ref, 0, r), pieces4(ks, 3, r), before[1])
        s4[r] = scores
        best = jnp.maximum(pieces4(peak, 0, r), row_max(scores))
        peak[0:4, 32 * r : 32 * r + 32] = best.reshape(4, 32, 128)
    scores = scored(qs_ref[0], ks[15], before[0])
    s1[...] = scores
    peak[0] = jnp.maximum(peak[0], row_max(scores))
    for r in range(16):
        p16[r] = weights(s16[r], pieces16(peak, r))
    for r in range(4):
        p4[r] = weights(s4[r], pieces4(peak, 0, r))
    p1[...] = weights(s1[...], peak[0])
    new = peak
    for i in range(16):
        new[i] = acc_ref[i] * jnp.exp2(top_ref[i] - peak[i])
    for r in range(16):
        new[:, 8 * r : 8 * r + 8] += dot(p16[r], pieces16(vs, r)).reshape(16, 8, 128)
    for r in range(4):
        new[0:4, 32 * r : 32 * r + 32] += dot(p4[r], pieces4(vs, 3, r)).reshape(4, 32, 128)
    new[0] += dot(p1[...], vs[15])
    low_rows = half(64)
    for i in range(16):
        natural = dot(perm_ref[...], normal(new[i]).astype(BF) * high)
        out_ref[i] = jnp.where(low_rows, pltpu.roll(natural[0:64], 64, 1), natural[64:128]).astype(BF)


def project_kernel(index_ref, core_ref, rows_ref, own_ref, other_ref, out_hbm, mixed, out_ref, sems):
    low = half(64)
    flip = 4 * ((index_ref[0] // GROUP) % 2)
    for side in range(2):
        core = core_ref[0] if side == 0 else 1 - core_ref[0]
        for j in range(4):
            first = rows_ref[2 * ((2 * j) ^ flip) + core].astype(F32)
            second = rows_ref[2 * ((2 * j) ^ flip) + 2 + core].astype(F32)
            cols = slice(128 * j, 128 * j + 128)
            mixed[side, 0:64, cols] = jnp.where(low, first, pltpu.roll(second, 64, 1)).astype(BF)
            mixed[side, 64:128, cols] = jnp.where(low, pltpu.roll(first, 64, 1), second).astype(BF)
    copies = []
    for n in range(4):
        cols = slice(512 * n, 512 * n + 512)
        out_ref[:, cols] = (dot(mixed[0], own_ref[:, cols]) + dot(mixed[1], other_ref[:, cols])).astype(BF)
        copy = pltpu.make_async_copy(out_ref.at[:, cols], out_hbm.at[:, cols], sems.at[n])
        copy.start()
        copies.append(copy)
    for copy in copies:
        copy.wait()


def vmem():
    return pl.BlockSpec(memory_space=pltpu.VMEM)


def limit(mib):
    return pltpu.CompilerParams(vmem_limit_bytes=mib * 2**20)


def per_device(query_rows, key_rows, value_rows, out_weight, blocks):
    tables = make_tables(blocks)
    index = lax.axis_index(SP).astype(jnp.int32).reshape(1)
    core = lax.axis_index("tp").astype(jnp.int32).reshape(1)

    smem = pl.BlockSpec(memory_space=pltpu.SMEM)
    hbm = pl.BlockSpec(memory_space=pltpu.HBM)
    send_kv, send_q = pl.pallas_call(
        pack_kernel,
        in_specs=[smem] * 2 + [hbm] * 7,
        out_specs=[vmem()] * 2,
        out_shape=[
            jax.ShapeDtypeStruct((2 * GROUP, HALF, 128), BF),
            jax.ShapeDtypeStruct((GROUP, 128, 128), BF),
        ],
        scratch_shapes=[
            pltpu.VMEM((TOK, 512), BF),
            pltpu.VMEM((TOK, 512), BF),
            pltpu.VMEM((TOK, 512), BF),
            pltpu.VMEM((HALF, HALF), BF),
            pltpu.VMEM((HALF, 128), F32),
            pltpu.VMEM((HALF, 128), F32),
            pltpu.VMEM((32 + blocks // 16, 256), F32),
            pltpu.VMEM((TOK, 512), F32),
            pltpu.VMEM((TOK, 512), F32),
            pltpu.VMEM((TOK, 512), F32),
            pltpu.SemaphoreType.DMA((7,)),
        ],
        compiler_params=limit(12),
        name="pack",
    )(
        index,
        core,
        *(
            pltpu.with_memory_space_constraint(array, pltpu.HBM)
            for array in (
                query_rows,
                key_rows,
                value_rows,
                jnp.asarray(tables["perm"], BF),
                jnp.asarray(tables["cos"]),
                jnp.asarray(tables["sin"]),
                jnp.asarray(tables["anchors"]),
            )
        ),
    )
    following = [(s, (s // GROUP + 1) * GROUP + ((s % GROUP) ^ 4)) for s in range(blocks - GROUP)]
    own = lax.all_to_all(send_kv, ("b", "x"), 0, 0, tiled=True)
    halo = lax.ppermute(own, SP, following)
    send_q, _ = lax.optimization_barrier((send_q, own))
    packed = lax.all_to_all(send_q, ("b", "x"), 0, 0, tiled=True)
    state = jax.ShapeDtypeStruct((16, HALF, 128), F32)
    rows16 = pltpu.VMEM((16, HALF, 128), BF)
    acc, top, qs = pl.pallas_call(
        own_kernel,
        in_specs=[vmem()] * 2,
        out_specs=[vmem()] * 3,
        out_shape=[state, state, jax.ShapeDtypeStruct((16, HALF, 128), BF)],
        scratch_shapes=[
            pltpu.VMEM((3, 128, 128), F32),
            pltpu.VMEM((3, 128, 128), F32),
            rows16,
            pltpu.VMEM((16, 128, 128), F32),
            pltpu.VMEM((16, 128, 256), F32),
            pltpu.VMEM((16, 128, 256), F32),
            pltpu.VMEM((16, 128, 128), BF),
            pltpu.VMEM((16, 128, 256), BF),
            pltpu.VMEM((16, 128, 256), BF),
        ],
        compiler_params=limit(24),
        cost_estimate=pl.CostEstimate(flops=20 * 10**9, bytes_accessed=2 * 2**20, transcendentals=0),
        name="attend_own",
    )(own, packed)
    weight, acc = lax.optimization_barrier((out_weight, acc))
    other_weight = lax.ppermute(weight, "tp", [(0, 1), (1, 0)])
    back = pl.pallas_call(
        halo_kernel,
        in_specs=[smem] + [vmem()] * 5,
        out_specs=vmem(),
        out_shape=jax.ShapeDtypeStruct((2 * GROUP, 64, 128), BF),
        scratch_shapes=[
            pltpu.VMEM((3, 128, 128), F32),
            rows16,
            pltpu.VMEM((16, HALF, 128), F32),
            pltpu.VMEM((16, 128, 128), F32),
            pltpu.VMEM((4, 128, 128), F32),
            pltpu.VMEM((128, 128), F32),
            pltpu.VMEM((16, 128, 128), BF),
            pltpu.VMEM((4, 128, 128), BF),
            pltpu.VMEM((128, 128), BF),
        ],
        compiler_params=limit(16),
        cost_estimate=pl.CostEstimate(flops=4 * 10**9, bytes_accessed=2 * 2**20, transcendentals=0),
        name="attend_halo",
    )(index, halo, acc, top, qs, jnp.asarray(tables["perm"].T, BF))
    back, other_weight = lax.optimization_barrier((back, other_weight))
    rows = lax.all_to_all(back, ("b", "x", "tp"), 0, 0, tiled=True)
    return pl.pallas_call(
        project_kernel,
        in_specs=[smem] * 2 + [vmem()] * 3,
        out_specs=hbm,
        out_shape=pltpu.HBM((TOK // 2, 2048), BF),
        scratch_shapes=[
            pltpu.VMEM((2, TOK // 2, 512), BF),
            pltpu.VMEM((TOK // 2, 2048), BF),
            pltpu.SemaphoreType.DMA((4,)),
        ],
        compiler_params=limit(16),
        name="project",
    )(index, core, rows, out_weight, other_weight)


def solution(mesh):
    blocks = mesh.shape["sp"]
    fine = Mesh(mesh.devices.reshape(blocks // 16, 2, 2, 4, 2), SP + ("tp",))
    return jax.shard_map(
        functools.partial(per_device, blocks=blocks),
        mesh=fine,
        in_specs=(P(SP, "tp"), P(SP, "tp"), P(SP, "tp"), P("tp", None)),
        out_specs=P(SP + ("tp",), None),
        check_vma=False,
    )
```
